32 devices in a mesh: sp: 4 (over z), fs: 4 (over y, x), tp: 2 (over core).
Axes of the slice: x: 2, y: 2, z: 4, core: 2. Of those that a mesh axis runs over, the one named last changes fastest.
Arguments:
- inputs: bfloat16 [4, 512, 2048], P('fs', 'sp', 'tp'), may hold values from -1000 to 1000
- input_norm_gain: float32 [2048], replicated, may hold values from 0.1 to 1.9
- receptance_weight: bfloat16 [2048, 1024], P(('sp', 'fs'), 'tp'), may hold values from -0.125 to 0.125
- linear_key_weight: bfloat16 [2048, 1024], P(('sp', 'fs'), 'tp'), may hold values from -0.125 to 0.125
- linear_value_weight: bfloat16 [2048, 1024], P(('sp', 'fs'), 'tp'), may hold values from -0.125 to 0.125
- window_query_weight: bfloat16 [2048, 1024], P(('sp', 'fs'), 'tp'), may hold values from -1 to 1
- window_key_weight: bfloat16 [2048, 256], P(('sp', 'fs'), 'tp'), may hold values from -1 to 1
- window_value_weight: bfloat16 [2048, 256], P(('sp', 'fs'), 'tp'), may hold values from -0.125 to 0.125
- decay_down_weight: bfloat16 [2048, 96], replicated, may hold values from -0.125 to 0.125
- decay_up_weight: bfloat16 [2, 96, 1024], replicated, may hold values from -1 to 1
- decay_offset: float32 [2, 1024], replicated, may hold values from -13 to -3
- decay_log_extra: float32 [4, 16, 512], P('fs', 'tp', 'sp'), may hold values from -1.4 to 0
- erasure_down_weight: bfloat16 [2048, 96], replicated, may hold values from -0.125 to 0.125
- erasure_up_weight: bfloat16 [2, 96, 1024], replicated, may hold values from -0.625 to 0.625
- erasure_offset: float32 [2, 1024], replicated, may hold values from -9.5 to 1
- initial_state: float32 [2, 16, 64, 64], replicated, may hold values from -128 to 128
- head_norm_gain: float32 [1024], replicated, may hold values from 0.1 to 1.9
- query_sink_logit: float32 [16], replicated, may hold values from 2 to 7
- linear_output_weight: bfloat16 [1024, 2048], P('tp', ('sp', 'fs')), may hold values from -0.1875 to 0.1875
- window_output_weight: bfloat16 [1024, 2048], P('tp', ('sp', 'fs')), may hold values from -1.5 to 1.5
Outputs:
- layer_out: bfloat16 [4, 512, 2048], P('fs', ('sp', 'tp'))
The draws below stay inside these ranges and needn't reach their ends.
All inputs are finite; a program needn't handle non-finite values.
Results may differ from the reference program's by a relative error of at most 0.006.
The reference program's roundings to bfloat16 on the way count: a program that leaves them out, or rounds other values in their place, can miss the bound.
Values may be sent and summed in bfloat16 or wider, within the bound.
A program may use at most 128 MiB of HBM per device.

```python
import math
import jax
import jax.numpy as jnp
from jax import lax

MODEL_DIM = 2048
RH = 16
HD = 64
AH = 16
AKV = 4
LOW_RANK_WIDTH = 96
WINDOW = 128
GRID_W = 64
ATT_BLOCK = 128
SPAN = 8
TOK_DEV = 128
SEQS = 4
LENGTH = 512
LINEAR_WIDTH = 1024
AW = 1024
KVW = 256


def slow_flags(key):
    share = 0.5
    flags = jax.random.bernoulli(jax.random.fold_in(key, 103), share, (RH,))
    return jnp.repeat(flags, HD)


def draw_inputs(key, part):
    shape = (SEQS, LENGTH, MODEL_DIM)
    noise_key = jax.random.fold_in(key, 1)
    return jax.random.normal(noise_key, shape, jnp.float32).astype(jnp.bfloat16)


def drawn_weight(key, salt, head_count):
    shape = (MODEL_DIM, head_count * HD)
    scale = MODEL_DIM ** (-0.5)
    noise_key = jax.random.fold_in(key, salt)
    return jax.random.normal(noise_key, shape, jnp.float32) * scale


def draw_window_query_weight(key, part):
    return drawn_weight(key, 5, AH).astype(jnp.bfloat16)


def draw_window_key_weight(key, part):
    return drawn_weight(key, 6, AKV).astype(jnp.bfloat16)


def draw_decay_offset(key, part):
    slow = slow_flags(key)[None, :]
    spread = jax.random.uniform(jax.random.fold_in(key, 7), (2, LINEAR_WIDTH), jnp.float32, 0.0, 1.0)
    slow_value = -math.log(LENGTH) - 2.0 + spread
    fast_value = -4.2 + spread
    return jnp.where(slow, slow_value, fast_value)


def draw_erasure_offset(key, part):
    slow = slow_flags(key)[None, :]
    spread = jax.random.uniform(jax.random.fold_in(key, 8), (2, LINEAR_WIDTH), jnp.float32, 0.0, 1.0)
    return jnp.where(slow, -9.5 + spread, -1.0 + 2.0 * spread)


def draw_decay_log_extra(key, part):
    span_len = TOK_DEV // 2
    span_count = LENGTH // span_len
    factor = jax.random.uniform(jax.random.fold_in(key, 9), (SEQS, RH, span_count, 1), jnp.float32, 0.0, 0.8)
    steady = -jnp.broadcast_to(factor, (SEQS, RH, span_count, span_len)).reshape(SEQS, RH, LENGTH) / LENGTH
    places = jax.random.randint(jax.random.fold_in(key, 10), (SEQS, RH, 2, 1), 0, LENGTH)
    depths = jax.random.uniform(jax.random.fold_in(key, 11), (SEQS, RH, 2, 1), jnp.float32, 0.22, 0.69)
    hits = jnp.sum(depths * (jnp.arange(LENGTH)[None, None, None, :] == places).astype(jnp.float32), axis=2)
    return steady - hits


def steps_of(rng, extent, cuts, smallest, high):
    gain, own = 1.0, jax.random.fold_in(rng, 6)
    for dim, blocks in cuts:
        draws = jnp.exp(jax.random.uniform(jax.random.fold_in(own, dim), (blocks,), jnp.float32, smallest / len(cuts), high / len(cuts)))
        gain = gain * jnp.repeat(draws, extent[dim] // blocks).reshape([-1 if axis == dim else 1 for axis in range(len(extent))])
    return gain


def scatter_about(own_key, shape, scale, limit, cuts=(), kind=jnp.bfloat16):
    factor_of = steps_of(own_key, shape, cuts, -0.22, 0.18) if cuts else 1.0
    drawn = jax.random.normal(own_key, shape, jnp.float32) * scale * factor_of
    return jnp.minimum(jnp.maximum(drawn, -limit), limit).astype(kind)


def setup_inputs(seed: int = 0) -> dict:
    key_of = jax.random.split(jax.random.key(seed), 21)
    return {
        "inputs": draw_inputs(jax.random.fold_in(key_of[20], 71), 0),
        "input_norm_gain": jnp.clip(1.0 + 0.18 * jax.random.normal(key_of[1], (MODEL_DIM,), jnp.float32), 0.1, 1.9),
        "receptance_weight": scatter_about(key_of[2], (MODEL_DIM, LINEAR_WIDTH), MODEL_DIM ** -0.5, 0.125, ((0, 16), (1, 2))),
        "linear_key_weight": scatter_about(key_of[3], (MODEL_DIM, LINEAR_WIDTH), MODEL_DIM ** -0.5, 0.125, ((0, 16), (1, 2))),
        "linear_value_weight": scatter_about(key_of[4], (MODEL_DIM, LINEAR_WIDTH), MODEL_DIM ** -0.5, 0.125, ((0, 16), (1, 2))),
        "window_query_weight": draw_window_query_weight(jax.random.fold_in(key_of[20], 71), 0),
        "window_key_weight": draw_window_key_weight(jax.random.fold_in(key_of[20], 71), 0),
        "window_value_weight": scatter_about(key_of[7], (MODEL_DIM, KVW), MODEL_DIM ** -0.5, 0.125, ((0, 16), (1, 2))),
        "decay_down_weight": scatter_about(key_of[8], (MODEL_DIM, LOW_RANK_WIDTH), MODEL_DIM ** -0.5, 0.125),
        "decay_up_weight": scatter_about(key_of[9], (2, LOW_RANK_WIDTH, LINEAR_WIDTH), 36 ** -0.5, 1.0),
        "decay_offset": draw_decay_offset(jax.random.fold_in(key_of[20], 71), 0),
        "decay_log_extra": draw_decay_log_extra(jax.random.fold_in(key_of[20], 71), 0),
        "erasure_down_weight": scatter_about(key_of[12], (MODEL_DIM, LOW_RANK_WIDTH), MODEL_DIM ** -0.5, 0.125),
        "erasure_up_weight": scatter_about(key_of[13], (2, LOW_RANK_WIDTH, LINEAR_WIDTH), LOW_RANK_WIDTH ** -0.5, 0.625),
        "erasure_offset": draw_erasure_offset(jax.random.fold_in(key_of[20], 71), 0),
        "initial_state": scatter_about(key_of[15], (2, RH, HD, HD), (LENGTH ** 0.5), 128.0, (), jnp.float32),
        "head_norm_gain": jnp.clip(1.0 + 0.18 * jax.random.normal(key_of[16], (LINEAR_WIDTH,), jnp.float32), 0.1, 1.9),
        "query_sink_logit": jnp.clip(jax.random.uniform(key_of[17], (AH,), jnp.float32, 2.0, 7.0), 2.0, 7.0),
        "linear_output_weight": scatter_about(key_of[18], (LINEAR_WIDTH, MODEL_DIM), LINEAR_WIDTH ** -0.5, 0.1875, ((0, 2), (1, 16))),
        "window_output_weight": scatter_about(key_of[19], (AW, MODEL_DIM), (AW // 64) ** -0.5, 1.5, ((0, 2), (1, 16))),
    }


NORM_EPS = 1e-06
GROUP_EPS = 0.00064
ROPE_BASE = 10000.0
HIGHEST = lax.Precision.HIGHEST

def to_bf16(array):
    return lax.optimization_barrier(array.astype(jnp.bfloat16))

def rope_axial(values, positions):
    quarter = values.shape[-1] // 4
    inverse = ROPE_BASE ** (-jnp.arange(quarter, dtype=jnp.float32) / quarter)
    grid_rows = (positions // GRID_W).astype(jnp.float32)
    grid_cols = (positions % GRID_W).astype(jnp.float32)
    pieces = []
    for which_half, coordinate in ((0, grid_rows), (1, grid_cols)):
        angles = coordinate[:, None] * inverse[None, :]
        cosine = jnp.cos(angles)[:, None, :]
        sine_part = jnp.sin(angles)[:, None, :]
        front_part = values[..., 2 * which_half * quarter:(2 * which_half + 1) * quarter]
        back_part = values[..., (2 * which_half + 1) * quarter:(2 * which_half + 2) * quarter]
        pieces.append(front_part * cosine - back_part * sine_part)
        pieces.append(front_part * sine_part + back_part * cosine)
    return jnp.concatenate(pieces, axis=-1)

def run_chain(initial, recept, decay_factor, keys, values, unit, erase, backward):
    seq_count, length = (recept.shape[0], recept.shape[1])
    segments = length // SPAN

    def blocked(array):
        return jnp.moveaxis(array.reshape(seq_count, segments, SPAN, RH, HD), 1, 0)
    streams = tuple((blocked(array) for array in (recept, decay_factor, keys, values, unit, erase)))
    visits = list(range(SPAN))[::-1] if backward else list(range(SPAN))

    def advance(memory, segment):
        results = [None] * SPAN
        for position in visits:
            read_now, decay_now, key_now, value_now, unit_now, erase_now = (array[:, position] for array in segment)
            erased = jnp.einsum('bhvk,bhk->bhv', memory, unit_now, precision=HIGHEST)
            memory = memory * decay_now[:, :, None, :] - erased[..., None] * erase_now[:, :, None, :] + value_now[..., None] * key_now[:, :, None, :]
            results[position] = jnp.einsum('bhvk,bhk->bhv', memory, read_now, precision=HIGHEST)
        return (memory, jnp.stack(results, axis=1))
    memory_init = jnp.broadcast_to(initial[None], (seq_count,) + initial.shape)
    _, outputs = lax.scan(advance, memory_init, streams, reverse=backward)
    return jnp.moveaxis(outputs, 0, 1).reshape(seq_count, length, RH, HD)

def window_attention(queries, keys, values, query_sink_logit):
    seq_count, length = (queries.shape[0], queries.shape[1])
    group_size = AH // AKV
    grouped = queries.reshape(seq_count, length, AKV, group_size, HD).astype(jnp.float32)
    padding = ((0, 0), (WINDOW, WINDOW), (0, 0), (0, 0))
    key_pad = jnp.pad(keys, padding).astype(jnp.float32)
    value_pad = jnp.pad(values, padding).astype(jnp.float32)
    sink_local = query_sink_logit.reshape(AKV, group_size)[None, :, :, None, None]
    reach = ATT_BLOCK + 2 * WINDOW

    def one_block(block_idx):
        query_rows = lax.dynamic_slice_in_dim(grouped, block_idx * ATT_BLOCK, ATT_BLOCK, 1)
        key_rows = lax.dynamic_slice_in_dim(key_pad, block_idx * ATT_BLOCK, reach, 1)
        value_rows = lax.dynamic_slice_in_dim(value_pad, block_idx * ATT_BLOCK, reach, 1)
        scores = jnp.einsum('sqgrd,skgd->sgrqk', query_rows, key_rows) * HD ** (-0.5)
        query_pos = block_idx * ATT_BLOCK + jnp.arange(ATT_BLOCK, dtype=jnp.int32)
        key_pos = block_idx * ATT_BLOCK - WINDOW + jnp.arange(reach, dtype=jnp.int32)
        allowed = (jnp.abs(query_pos[:, None] - key_pos[None, :]) <= WINDOW) & (key_pos[None, :] >= 0) & (key_pos[None, :] < length)
        scores = jnp.where(allowed, scores, -jnp.inf)
        top_score = jnp.maximum(lax.optimization_barrier(jnp.max(scores, axis=-1, keepdims=True)), sink_local)
        raised = jnp.exp(scores - top_score)
        denominator = jnp.exp(sink_local - top_score) + lax.optimization_barrier(jnp.sum(raised, axis=-1, keepdims=True))
        weights = to_bf16(raised / denominator).astype(jnp.float32)
        mixed = jnp.einsum('sgrqk,skgd->sqgrd', weights, value_rows)
        return mixed.astype(jnp.bfloat16)
    blocks = lax.map(one_block, jnp.arange(length // ATT_BLOCK, dtype=jnp.int32))
    return jnp.moveaxis(blocks, 0, 1).reshape(seq_count, length, AH * HD)

def reference(inputs, input_norm_gain, receptance_weight, linear_key_weight, linear_value_weight, window_query_weight, window_key_weight, window_value_weight, decay_down_weight, decay_up_weight, decay_offset, decay_log_extra, erasure_down_weight, erasure_up_weight, erasure_offset, initial_state, head_norm_gain, query_sink_logit, linear_output_weight, window_output_weight):
    seq_count, length, model_width = inputs.shape
    widened = inputs.astype(jnp.float32)
    hidden = to_bf16(widened * lax.rsqrt(lax.optimization_barrier(jnp.mean(widened * widened, axis=-1, keepdims=True)) + NORM_EPS) * input_norm_gain).reshape(seq_count * length, model_width)

    def project(weight):
        return to_bf16(jnp.dot(hidden, weight, preferred_element_type=jnp.float32))

    def lin_heads(array):
        return array.astype(jnp.float32).reshape(seq_count, length, RH, HD)
    recept = lin_heads(project(receptance_weight))
    keys = lin_heads(project(linear_key_weight))
    values = lin_heads(project(linear_value_weight))
    unit = keys * lax.rsqrt(lax.optimization_barrier(jnp.sum(keys * keys, axis=-1, keepdims=True)) + NORM_EPS)
    decay_act = to_bf16(jnp.tanh(project(decay_down_weight).astype(jnp.float32)))
    learn_low = project(erasure_down_weight)
    decay_spikes = jnp.transpose(decay_log_extra, (0, 2, 1))[..., None]
    lin_sum = jnp.zeros((seq_count, length, RH, HD), jnp.float32)
    for direction in range(2):
        pre_decay = decay_offset[direction] + jnp.dot(decay_act, decay_up_weight[direction], preferred_element_type=jnp.float32)
        erasure_rate = lin_heads(jnp.exp(-jax.nn.softplus(-pre_decay) - 0.5))
        decay_factor = jnp.exp(decay_spikes - erasure_rate)
        learn = lin_heads(jax.nn.sigmoid(erasure_offset[direction] + jnp.dot(learn_low, erasure_up_weight[direction], preferred_element_type=jnp.float32)))
        lin_sum = lin_sum + run_chain(initial_state[direction], recept, decay_factor, keys, values, unit, unit * learn, direction == 1)
    centred = lin_sum - lax.optimization_barrier(jnp.mean(lin_sum, axis=-1, keepdims=True))
    normed = centred * lax.rsqrt(lax.optimization_barrier(jnp.mean(centred * centred, axis=-1, keepdims=True)) + GROUP_EPS)
    lin_mix = (normed.reshape(seq_count * length, RH * HD) * head_norm_gain).astype(jnp.bfloat16)
    positions = jnp.arange(length, dtype=jnp.int32)
    queries = to_bf16(rope_axial(project(window_query_weight).astype(jnp.float32).reshape(seq_count, length, AH, HD), positions))
    att_keys = to_bf16(rope_axial(project(window_key_weight).astype(jnp.float32).reshape(seq_count, length, AKV, HD), positions))
    att_values = project(window_value_weight).reshape(seq_count, length, AKV, HD)
    att_mix = window_attention(queries, att_keys, att_values, query_sink_logit).reshape(seq_count * length, AH * HD)
    result = jnp.dot(lin_mix, linear_output_weight, preferred_element_type=jnp.float32) + jnp.dot(att_mix, window_output_weight, preferred_element_type=jnp.float32)
    return result.astype(jnp.bfloat16).reshape(seq_count, length, model_width)
```

```python
import jax
import jax.numpy as jnp
import numpy as np
from jax import lax
from jax.experimental import pallas as pl
from jax.experimental.pallas import tpu as pltpu
from jax.sharding import PartitionSpec as P

HD = 64
WINDOW = 128
GRID_W = 64
ATT_BLOCK = 128


NORM_EPS = 1e-06
GROUP_EPS = 0.00064
ROPE_BASE = 10000.0
HIGHEST = lax.Precision.HIGHEST


def padded(block, sides, width):
    for axis, dim in sides:
        count = lax.axis_size(axis)
        forward = [(i, i + 1) for i in range(count - 1)]
        backward = [(target, source) for source, target in forward]
        low = lax.ppermute(
            lax.slice_in_dim(block, block.shape[dim] - width, None, axis=dim), axis, forward
        )
        high = lax.ppermute(lax.slice_in_dim(block, 0, width, axis=dim), axis, backward)
        block = jnp.concatenate([low, block, high], axis=dim)
    return block


def to_bf16(array):
    return lax.optimization_barrier(array.astype(jnp.bfloat16))


def rope_axial(values, positions):
    quarter = values.shape[-1] // 4
    inverse = ROPE_BASE ** (-jnp.arange(quarter, dtype=jnp.float32) / quarter)
    grid_rows = (positions // GRID_W).astype(jnp.float32)
    grid_cols = (positions % GRID_W).astype(jnp.float32)
    pieces = []
    for which_half, coordinate in ((0, grid_rows), (1, grid_cols)):
        angles = coordinate[:, None] * inverse[None, :]
        cosine = jnp.cos(angles)[:, None, :]
        sine_part = jnp.sin(angles)[:, None, :]
        front_part = values[..., 2 * which_half * quarter : (2 * which_half + 1) * quarter]
        back_part = values[..., (2 * which_half + 1) * quarter : (2 * which_half + 2) * quarter]
        pieces.append(front_part * cosine - back_part * sine_part)
        pieces.append(front_part * sine_part + back_part * cosine)
    return jnp.concatenate(pieces, axis=-1)


CHUNK = 32
PAIR = 2 * HD
F32 = jnp.float32
BF16 = jnp.bfloat16
NN = (((1,), (0,)), ((), ()))
NT = (((1,), (1,)), ((), ()))


def dot1(left, right, dims=NN):
    return lax.dot_general(
        left.astype(jnp.bfloat16), right.astype(jnp.bfloat16), dims, preferred_element_type=F32
    )


def halves(value):
    high = value.astype(jnp.bfloat16)
    return high, (value - high.astype(F32)).astype(jnp.bfloat16)


def dot3(left, right, dims=NN):
    left_high, left_low = halves(left)
    right_high, right_low = halves(right)

    def product(one, other):
        return lax.dot_general(one, other, dims, preferred_element_type=F32)

    return product(left_high, right_high) + (
        product(left_high, right_low) + product(left_low, right_high)
    )


def full_dot(left, right):
    return lax.dot_general(left, right, NN, precision=HIGHEST, preferred_element_type=F32)


def chunk_kernel(read_ref, key_ref, value_ref, log_ref, learn_ref, out_ref, end_ref):
    tokens = read_ref.shape[0]
    read = read_ref[...].astype(F32)
    key = key_ref[...].astype(F32)
    value = value_ref[...].astype(F32)
    first = lax.broadcasted_iota(jnp.int32, (tokens, PAIR), 1) < HD
    pair_i = lax.broadcasted_iota(jnp.int32, (PAIR, PAIR), 0)
    pair_j = lax.broadcasted_iota(jnp.int32, (PAIR, PAIR), 1)
    same_head = jnp.where(pair_i // HD == pair_j // HD, 1.0, 0.0)
    row = lax.broadcasted_iota(jnp.int32, (tokens, tokens), 0)
    col = lax.broadcasted_iota(jnp.int32, (tokens, tokens), 1)
    same_chunk = row // CHUNK == col // CHUNK
    eye = jnp.where(row == col, 1.0, 0.0)
    unit = key * lax.rsqrt(full_dot(key * key, same_head) + NORM_EPS)
    own = (first, jnp.logical_not(first))
    values = (
        jnp.where(first, value, 0.0),
        jnp.where(first, pltpu.roll(value, HD, 1), 0.0),
    )
    all_chunk = jnp.where(same_chunk, 1.0, 0.0)
    for direction in range(2):
        before = (col < row) if direction == 0 else (col > row)
        strict = same_chunk & before
        upto = same_chunk & (before | (col == row))
        log_decay = log_ref[direction]
        erase = unit * learn_ref[direction]
        total_log = full_dot(jnp.where(upto, 1.0, 0.0), log_decay)
        chunk_log = full_dot(all_chunk, log_decay)
        prior_log = total_log - log_decay
        middle = 0.5 * chunk_log
        unit_start = jnp.exp(prior_log) * unit
        unit_mid = jnp.exp(prior_log - middle) * unit
        read_start = jnp.exp(total_log) * read
        read_mid = jnp.exp(total_log - middle) * read
        inverse = jnp.exp(middle - total_log)
        sources = jnp.concatenate([erase * inverse, key * inverse], axis=0)
        rest = jnp.exp(chunk_log - total_log)
        key_rest = key * rest
        erase_rest = erase * rest
        chunk_decay = jnp.exp(chunk_log).T
        solved, offsets, mixes = [], [], []
        for head in range(2):
            readers = jnp.concatenate(
                [jnp.where(own[head], unit_mid, 0.0), jnp.where(own[head], read_mid, 0.0)], axis=0
            )
            meets = dot3(readers, sources, NT)
            erased = jnp.where(strict, meets[:tokens, :tokens], 0.0)
            seen = jnp.where(strict, meets[:tokens, tokens:], 0.0)
            read_erased = jnp.where(upto, meets[tokens:, :tokens], 0.0)
            read_seen = jnp.where(upto, meets[tokens:, tokens:], 0.0)
            solve = eye - jnp.where(row // 2 == col // 2, erased, 0.0)
            size = 2
            while size < CHUNK:
                level = (row // (2 * size) == col // (2 * size)) & (row // size != col // size)
                solve = solve - dot1(dot1(solve, jnp.where(level, erased, 0.0)), solve)
                size *= 2
            solve = solve + dot1(solve, eye - solve - dot3(erased, solve))
            both = dot3(
                solve,
                jnp.concatenate(
                    [jnp.where(own[head], unit_start, 0.0), dot3(seen, values[head])], axis=1
                ),
            )
            solved.append(both[:, :PAIR])
            offsets.append(both[:, PAIR:])
            mixes.append(jnp.concatenate([read_seen, -read_erased], axis=1))
        state = jnp.where(pair_j == HD + pair_i % HD, 1.0, 0.0)
        count = tokens // CHUNK
        drops = [[None] * count, [None] * count]
        reads = [[None] * count, [None] * count]
        for step in range(count):
            place = step if direction == 0 else count - 1 - step
            rows = slice(place * CHUNK, (place + 1) * CHUNK)
            lefts = jnp.concatenate(
                [solved[0][rows], solved[1][rows]]
                + [jnp.where(own[head], read_start, 0.0)[rows] for head in range(2)],
                axis=0,
            )
            seen_state = dot3(lefts, state)
            for head in range(2):
                drops[head][place] = (
                    seen_state[head * CHUNK : (head + 1) * CHUNK] + offsets[head][rows]
                )
                reads[head][place] = seen_state[(2 + head) * CHUNK : (3 + head) * CHUNK]
            adders = jnp.concatenate(
                [jnp.where(own[head], key_rest, 0.0)[rows] for head in range(2)]
                + [jnp.where(own[head], -erase_rest, 0.0)[rows] for head in range(2)],
                axis=0,
            ).T
            added = jnp.concatenate(
                [values[0][rows], values[1][rows], drops[0][place], drops[1][place]], axis=0
            )
            first_col = place * CHUNK
            state = chunk_decay[:, first_col : first_col + 1] * state + dot3(adders, added)
        for head in range(2):
            dropped = jnp.concatenate(drops[head], axis=0)
            out_ref[direction, head] = jnp.concatenate(reads[head], axis=0) + dot3(
                mixes[head], jnp.concatenate([values[head], dropped], axis=0)
            )
        end_ref[direction] = state


def chunked(returned, log_decay, learn, head_width):
    tokens = returned.shape[0]
    pairs = head_width // PAIR

    def role(which):
        return pl.BlockSpec((tokens, PAIR), lambda p: (0, which * pairs + p))

    wide = pl.BlockSpec((2, tokens, PAIR), lambda p: (0, 0, p))
    return pl.pallas_call(
        chunk_kernel,
        grid=(pairs,),
        in_specs=[role(0), role(1), role(2), wide, wide],
        out_specs=[
            pl.BlockSpec((2, 2, tokens, PAIR), lambda p: (0, p, 0, 0)),
            pl.BlockSpec((2, PAIR, PAIR), lambda p: (0, p, 0)),
        ],
        out_shape=[
            jax.ShapeDtypeStruct((2, 2 * pairs, tokens, PAIR), F32),
            jax.ShapeDtypeStruct((2, pairs * PAIR, PAIR), F32),
        ],
        cost_estimate=pl.CostEstimate(
            flops=pairs * 400 * PAIR**3, bytes_accessed=8 * tokens * head_width * 4, transcendentals=0
        ),
        name="chunked_state",
    )(returned, returned, returned, log_decay, learn)


def merge_kernel(local_ref, state_ref, gain_ref, out_ref):
    pair_i = lax.broadcasted_iota(jnp.int32, (PAIR, PAIR), 0)
    pair_j = lax.broadcasted_iota(jnp.int32, (PAIR, PAIR), 1)
    average = jnp.where(pair_i // HD == pair_j // HD, 1.0 / HD, 0.0)
    sums = []
    for head in range(2):
        total = 0.0
        for direction in range(2):
            block = local_ref[direction, head]
            total = total + (
                block[:, :HD] + dot3(block[:, HD:], state_ref[direction, head])
            )
        sums.append(total)
    lin_sum = jnp.concatenate(sums, axis=1)
    centred = lin_sum - full_dot(lin_sum, average)
    normed = centred * lax.rsqrt(full_dot(centred * centred, average) + GROUP_EPS)
    out_ref[...] = (normed * gain_ref[...]).astype(jnp.bfloat16)


def merged(local_out, entry, gain):
    _, head_count, tokens, _ = local_out.shape
    pairs = head_count // 2
    return pl.pallas_call(
        merge_kernel,
        grid=(pairs,),
        in_specs=[
            pl.BlockSpec((2, 2, tokens, PAIR), lambda p: (0, p, 0, 0)),
            pl.BlockSpec((2, 2, HD, HD), lambda p: (0, p, 0, 0)),
            pl.BlockSpec((1, PAIR), lambda p: (0, p)),
        ],
        out_specs=pl.BlockSpec((tokens, PAIR), lambda p: (0, p)),
        out_shape=jax.ShapeDtypeStruct((tokens, head_count * HD), jnp.bfloat16),
        cost_estimate=pl.CostEstimate(
            flops=pairs * 30 * PAIR**3, bytes_accessed=4 * tokens * head_count * PAIR * 4, transcendentals=0
        ),
        name="merged_norm",
    )(local_out, entry, gain[None, :])


def entering_states(ends, initial):
    count = lax.axis_size("sp")
    place = lax.axis_index("sp")
    ups = [(i, i + 1) for i in range(count - 1)]
    downs = [(i + 1, i) for i in range(count - 1)]
    adds, maps = ends[..., :HD], ends[..., HD:]

    def hop(_, states):
        later = jnp.einsum("dhkj,dhjv->dhkv", maps, states, precision=HIGHEST) + adds
        forward = lax.ppermute(later[0], "sp", ups)
        backward = lax.ppermute(later[1], "sp", downs)
        return jnp.stack(
            [
                jnp.where(place == 0, initial[0], forward),
                jnp.where(place == count - 1, initial[1], backward),
            ]
        )

    states = initial
    if count > 8:
        return lax.fori_loop(0, count - 1, hop, states)
    for _ in range(count - 1):
        states = hop(0, states)
    return states


def swapped(block, axis):
    count = lax.axis_size(axis)
    return [block] + [
        lax.ppermute(block, axis, [(i, i ^ flip) for i in range(count)]) for flip in range(1, count)
    ]


def in_order(pieces, axis):
    me = lax.axis_index(axis)
    stacked = jnp.stack(pieces)
    return [
        lax.dynamic_index_in_dim(stacked, me ^ place, 0, False) for place in range(len(pieces))
    ]


def local(
    inputs,
    input_norm_gain,
    receptance_weight,
    linear_key_weight,
    linear_value_weight,
    window_query_weight,
    window_key_weight,
    window_value_weight,
    decay_down_weight,
    decay_up_weight,
    decay_offset,
    decay_log_extra,
    erasure_down_weight,
    erasure_up_weight,
    erasure_offset,
    initial_state,
    head_norm_gain,
    query_sink_logit,
    linear_output_weight,
    window_output_weight,
):
    tokens = inputs.shape[1]
    tp_index = lax.axis_index("tp")
    length = tokens * lax.axis_size("sp")
    offset = lax.axis_index("sp") * tokens
    gathered = lax.all_gather(inputs, "tp", axis=2, tiled=True)[0]
    widened = gathered.astype(jnp.float32)
    hidden = to_bf16(
        widened
        * lax.rsqrt(jnp.mean(widened * widened, axis=-1, keepdims=True) + NORM_EPS)
        * input_norm_gain
    )
    weights = (
        receptance_weight,
        linear_key_weight,
        linear_value_weight,
        window_query_weight,
        window_key_weight,
        window_value_weight,
    )
    widths = [weight.shape[1] for weight in weights]
    joined = jnp.concatenate(weights, axis=1)
    regrouped = lax.all_to_all(joined, "fs", split_axis=1, concat_axis=0, tiled=True)
    every_seq = jnp.concatenate(swapped(hidden, "fs"), axis=0)
    near_cols = jnp.concatenate(in_order(swapped(window_output_weight, "fs"), "fs"), axis=1)
    whole_cols = lax.all_gather(regrouped, "sp", axis=0, tiled=True)
    partial_cols = jnp.dot(every_seq, whole_cols, preferred_element_type=jnp.float32)
    by_seq = to_bf16(partial_cols).reshape(-1, tokens, partial_cols.shape[1])
    outgoing = jnp.concatenate(in_order(list(by_seq), "fs"), axis=0)
    returned = lax.all_to_all(outgoing, "fs", split_axis=0, concat_axis=1, tiled=True)
    bounds = [0]
    for col_width in widths:
        bounds.append(bounds[-1] + col_width)
    projected = [returned[:, bounds[role_idx] : bounds[role_idx + 1]] for role_idx in range(6)]
    recept, lin_keys, lin_values, queries, att_keys, att_values = projected
    head_width = recept.shape[1]
    head_count = head_width // HD
    first_col = tp_index * head_width
    up_decay = lax.dynamic_slice_in_dim(decay_up_weight, first_col, head_width, 2)
    up_learn = lax.dynamic_slice_in_dim(erasure_up_weight, first_col, head_width, 2)
    base_decay = lax.dynamic_slice_in_dim(decay_offset, first_col, head_width, 1)
    base_learn = lax.dynamic_slice_in_dim(erasure_offset, first_col, head_width, 1)
    gain_local = lax.dynamic_slice_in_dim(head_norm_gain, first_col, head_width, 0)
    state_local = lax.dynamic_slice_in_dim(initial_state, tp_index * head_count, head_count, 1)
    spread = (
        jnp.arange(head_count)[:, None] == jnp.arange(head_width)[None, :] // HD
    ).astype(jnp.float32)
    decay_spikes = jnp.einsum("ht,hc->tc", decay_log_extra[0], spread, precision=HIGHEST)
    decay_low = to_bf16(jnp.dot(hidden, decay_down_weight, preferred_element_type=jnp.float32))
    decay_act = to_bf16(jnp.tanh(decay_low.astype(jnp.float32)))
    learn_low = to_bf16(jnp.dot(hidden, erasure_down_weight, preferred_element_type=jnp.float32))
    pre_decay = base_decay[:, None, :] + jnp.einsum(
        "tl,dlc->dtc", decay_act, up_decay, preferred_element_type=jnp.float32
    )
    log_decay = decay_spikes[None] - jnp.exp(-jax.nn.softplus(-pre_decay) - 0.5)
    learn = jax.nn.sigmoid(
        base_learn[:, None, :]
        + jnp.einsum("tl,dlc->dtc", learn_low, up_learn, preferred_element_type=jnp.float32)
    )
    local_out, ends = chunked(returned, log_decay, learn, head_width)
    entry = entering_states(
        ends.reshape(2, head_count, HD, PAIR), jnp.swapaxes(state_local, -1, -2)
    )
    lin_mix = merged(local_out, entry, gain_local)
    positions = offset + jnp.arange(tokens, dtype=jnp.int32)
    query_count = queries.shape[1] // HD
    group_count = att_keys.shape[1] // HD
    group_size = query_count // group_count
    roped_q = rope_axial(
        queries.astype(jnp.float32).reshape(tokens, query_count, HD), positions
    ).astype(jnp.bfloat16)
    roped_k = rope_axial(
        att_keys.astype(jnp.float32).reshape(tokens, group_count, HD), positions
    ).astype(jnp.bfloat16)
    kv_width = group_count * HD
    packed = jnp.concatenate([roped_k.reshape(tokens, kv_width), att_values], axis=1)
    bordered = padded(packed, (("sp", 0),), WINDOW)
    sink_local = lax.dynamic_slice_in_dim(
        query_sink_logit, tp_index * query_count, query_count, 0
    ).reshape(group_count, group_size)[:, :, None, None]
    reach = ATT_BLOCK + 2 * WINDOW
    query_rows = roped_q.reshape(ATT_BLOCK, group_count, group_size, HD)
    key_rows = bordered[:, :kv_width].reshape(reach, group_count, HD)
    value_rows = bordered[:, kv_width:].reshape(reach, group_count, HD)
    scores = jnp.einsum(
        "qgrd,kgd->grqk", query_rows, key_rows, preferred_element_type=jnp.float32
    ) * HD ** (-0.5)
    query_pos = offset + 0 + jnp.arange(ATT_BLOCK, dtype=jnp.int32)
    key_pos = offset + 0 - WINDOW + jnp.arange(reach, dtype=jnp.int32)
    allowed = (
        (jnp.abs(query_pos[:, None] - key_pos[None, :]) <= WINDOW)
        & (key_pos[None, :] >= 0)
        & (key_pos[None, :] < length)
    )
    scores = jnp.where(allowed, scores, -jnp.inf)
    top_score = jnp.maximum(jnp.max(scores, axis=-1, keepdims=True), sink_local)
    raised = jnp.exp(scores - top_score)
    denominator = jnp.exp(sink_local - top_score) + jnp.sum(raised, axis=-1, keepdims=True)
    weights_bf = (raised / denominator).astype(jnp.bfloat16)
    mixed = jnp.einsum("grqk,kgd->qgrd", weights_bf, value_rows, preferred_element_type=jnp.float32)
    outputs = mixed.astype(jnp.bfloat16).reshape(ATT_BLOCK, query_count * HD)
    lin_weight = lax.all_gather(linear_output_weight, ("sp", "fs"), axis=1, tiled=True)
    if lax.axis_size("sp") > 8:
        att_out = jnp.dot(
            outputs,
            lax.all_gather(near_cols, "sp", axis=1, tiled=True),
            preferred_element_type=jnp.float32,
        )
    else:
        att_parts = [
            jnp.dot(outputs, part, preferred_element_type=jnp.float32)
            for part in swapped(near_cols, "sp")
        ]
        att_out = jnp.concatenate(in_order(att_parts, "sp"), axis=1)
    layer_out = lax.psum_scatter(
        jnp.dot(lin_mix, lin_weight, preferred_element_type=jnp.float32) + att_out,
        "tp",
        scatter_dimension=0,
        tiled=True,
    )
    return layer_out.astype(jnp.bfloat16)[None]

MESH_IDS = pl.DeviceIdType.MESH


def flipped(index, bits):
    result = index
    for bit in (1, 2):
        if bits & bit:
            result = result + bit - 2 * bit * lax.rem(lax.div(index, bit), 2)
    return result


def front_kernel(
    x_ref,
    wr_ref,
    wk_ref,
    wv_ref,
    wq_ref,
    kv_ref,
    extra_ref,
    dup_ref,
    eup_ref,
    gain_ref,
    ddown_ref,
    edown_ref,
    doff_ref,
    eoff_ref,
    proj_ref,
    log_ref,
    learn_ref,
    xbuf,
    wbuf,
    ebuf,
    dup,
    eup,
    local_sem,
    wlocal_sem,
    up_send,
    up_recv,
    dn_send,
    dn_recv,
    sib_send,
    sib_recv,
    wz_send,
    wz_recv,
    e_send,
    e_recv,
    p_send,
    p_recv,
    f_send,
    f_recv,
):
    sp, fs, tp = lax.axis_index("sp"), lax.axis_index("fs"), lax.axis_index("tp")
    depth = lax.axis_size("sp")
    width = lax.axis_size("fs")
    tokens = x_ref.shape[1]
    rows = wr_ref.shape[0]
    sibling = {"tp": 1 - tp}
    plane = ({"fs": flipped(fs, 1)}, {"fs": flipped(fs, 2)})

    def remote(src, dst, send, recv, device):
        return pltpu.make_async_remote_copy(
            src_ref=src,
            dst_ref=dst,
            send_sem=send,
            recv_sem=recv,
            device_id=device,
            device_id_type=MESH_IDS,
        )

    def rows_of(z, f):
        return pl.ds(pl.multiple_of((z * width + f) * rows, rows), rows)

    def pieces(z):
        low = pl.ds(pl.multiple_of(z * PAIR, PAIR), PAIR)
        shared = pl.ds(pl.multiple_of(lax.div(z, 2) * PAIR, PAIR), PAIR)
        return [ref.at[:, low] for ref in (wr_ref, wk_ref, wv_ref, wq_ref)] + [
            kv_ref.at[:, shared]
        ]

    def lanes(place):
        return slice(place * PAIR, (place + 1) * PAIR)

    cols = pl.ds(pl.multiple_of((tp * depth + sp) * PAIR, PAIR), PAIR)
    own_x = pltpu.make_async_copy(x_ref.at[0], xbuf.at[sp, tp], local_sem.at[0])
    own_x.start()
    own_w = [
        pltpu.make_async_copy(
            piece, wbuf.at[rows_of(sp, fs), lanes(place)], wlocal_sem.at[place]
        )
        for place, piece in enumerate(pieces(sp))
    ]
    for copy in own_w:
        copy.start()
    small = [
        pltpu.make_async_copy(extra_ref.at[0], ebuf.at[sp], local_sem.at[1]),
        pltpu.make_async_copy(dup_ref.at[:, :, cols], dup, local_sem.at[2]),
        pltpu.make_async_copy(eup_ref.at[:, :, cols], eup, local_sem.at[3]),
    ]
    for copy in small:
        copy.start()

    barrier = pltpu.get_barrier_semaphore()
    peers = [{"sp": flipped(sp, k)} for k in range(1, depth)] + [sibling, *plane]
    for peer in peers:
        pl.semaphore_signal(barrier, inc=1, device_id=peer, device_id_type=MESH_IDS)
    pl.semaphore_wait(barrier, len(peers))

    def x_move(src_z, send, recv, device, src=None):
        there = xbuf.at[src_z, tp]
        return remote(there if src is None else src, there, send, recv, device)

    up_to, dn_to = {"sp": sp + 1}, {"sp": sp - 1}

    @pl.when(sp < depth - 1)
    def _():
        x_move(sp, up_send.at[0], up_recv.at[0], up_to, x_ref.at[0]).start()

    @pl.when(sp > 0)
    def _():
        x_move(sp, dn_send.at[0], dn_recv.at[0], dn_to, x_ref.at[0]).start()

    def wz_block(k):
        there = wbuf.at[rows_of(sp, fs)]
        return remote(there, there, wz_send.at[k - 1], wz_recv.at[k - 1], {"sp": flipped(sp, k)})

    def e_block(k):
        return remote(
            extra_ref.at[0],
            ebuf.at[sp],
            e_send.at[k - 1],
            e_recv.at[k - 1],
            {"sp": flipped(sp, k)},
        )

    for k in range(1, depth):
        target = flipped(sp, k)
        for place, piece in enumerate(pieces(target)):
            remote(
                piece,
                wbuf.at[rows_of(sp, fs), lanes(place)],
                wz_send.at[k - 1],
                wz_recv.at[k - 1],
                {"sp": target},
            ).start()
        e_block(k).start()

    own_x.wait()
    sib = [x_move(sp, sib_send.at[0], sib_recv.at[0], sibling)]
    sib[0].start()
    for copy in own_w:
        copy.wait()

    def p_block(k, side):
        there = wbuf.at[rows_of(flipped(sp, k), fs)]
        return remote(there, there, p_send.at[k, side], p_recv.at[k, side], plane[side])

    def f_block(k):
        side = k % 2
        there = wbuf.at[rows_of(flipped(sp, k), flipped(fs, 2 if side == 0 else 1))]
        return remote(there, there, f_send.at[k], f_recv.at[k], plane[side])

    def x_step(k):
        @pl.when(sp >= k)
        def _():
            x_move(sp, up_send.at[k - 1], up_recv.at[k - 1], up_to).wait_recv()
            if k < depth - 1:

                @pl.when(sp < depth - 1)
                def _():
                    x_move(sp - k, up_send.at[k], up_recv.at[k], up_to).start()

            x_move(sp - k, sib_send.at[k], sib_recv.at[k], sibling).start()

        @pl.when(sp < depth - k)
        def _():
            x_move(sp, dn_send.at[k - 1], dn_recv.at[k - 1], dn_to).wait_recv()
            if k < depth - 1:

                @pl.when(sp > 0)
                def _():
                    x_move(sp + k, dn_send.at[k], dn_recv.at[k], dn_to).start()

            x_move(sp + k, sib_send.at[depth + k - 1], sib_recv.at[depth + k - 1], sibling).start()

    def w_step(k):
        wz_block(k).wait_recv()
        for side in range(2):
            p_block(k, side).start()

    def f_step(k):
        for side in range(2):
            p_block(k, side).wait_recv()
        f_block(k).start()

    for side in range(2):
        p_block(0, side).start()
    f_step(0)
    x_step(1)
    w_step(1)
    w_step(2)
    f_step(1)
    x_step(2)
    w_step(3)
    f_step(2)
    f_step(3)
    x_step(3)
    for k in range(depth):
        f_block(k).wait_recv()
    for k in range(1, depth):
        e_block(k).wait_recv()
    x_move(sp, sib_send.at[0], sib_recv.at[0], sibling).wait_recv()
    for k in range(1, depth):

        @pl.when(sp >= k)
        def _():
            x_move(sp, sib_send.at[k], sib_recv.at[k], sibling).wait_recv()

        @pl.when(sp < depth - k)
        def _():
            place = depth + k - 1
            x_move(sp, sib_send.at[place], sib_recv.at[place], sibling).wait_recv()

    for copy in small:
        copy.wait()

    gain = gain_ref[...]
    half = gain.shape[1] // 2
    doff = doff_ref[:, cols]
    eoff = eoff_ref[:, cols]

    def block(z, carry):
        parts = [xbuf[z, side].astype(F32) for side in range(2)]
        total = sum(jnp.sum(part * part, axis=1, keepdims=True) for part in parts)
        scale = lax.rsqrt(total / (2 * half) + NORM_EPS)
        hidden = jnp.concatenate(
            [
                (part * scale * gain[:, side * half : (side + 1) * half]).astype(BF16)
                for side, part in enumerate(parts)
            ],
            axis=1,
        )
        where = pl.ds(pl.multiple_of(z * tokens, tokens), tokens)

        def dot(left, right):
            return jnp.dot(left, right, preferred_element_type=F32)

        proj_ref[where, :] = dot(hidden, wbuf[...]).astype(BF16)
        decay_act = jnp.tanh(dot(hidden, ddown_ref[...]).astype(BF16).astype(F32)).astype(BF16)
        learn_low = dot(hidden, edown_ref[...]).astype(BF16)
        first_head = 2 * sp
        spikes = jnp.concatenate(
            [
                jnp.broadcast_to(ebuf[z, pl.ds(first_head + head, 1), :], (HD, tokens))
                for head in range(2)
            ],
            axis=0,
        ).T
        for direction in range(2):
            pre = doff[direction : direction + 1] + dot(decay_act, dup[direction])
            softplus = jnp.maximum(-pre, 0.0) + jnp.log1p(jnp.exp(-jnp.abs(pre)))
            log_ref[direction, where, :] = spikes - jnp.exp(-softplus - 0.5)
            learn = eoff[direction : direction + 1] + dot(learn_low, eup[direction])
            learn_ref[direction, where, :] = jax.nn.sigmoid(learn)
        return carry

    lax.fori_loop(0, depth, block, 0)

    @pl.when(sp < depth - 1)
    def _():
        x_move(sp, up_send.at[0], up_recv.at[0], up_to, x_ref.at[0]).wait_send()

    @pl.when(sp > 0)
    def _():
        x_move(sp, dn_send.at[0], dn_recv.at[0], dn_to, x_ref.at[0]).wait_send()

    x_move(sp, sib_send.at[0], sib_recv.at[0], sibling).wait_send()
    for k in range(1, depth):

        @pl.when(sp >= k)
        def _():
            x_move(sp, sib_send.at[k], sib_recv.at[k], sibling).wait_send()
            if k < depth - 1:

                @pl.when(sp < depth - 1)
                def _():
                    x_move(sp, up_send.at[k], up_recv.at[k], up_to).wait_send()

        @pl.when(sp < depth - k)
        def _():
            place = depth + k - 1
            x_move(sp, sib_send.at[place], sib_recv.at[place], sibling).wait_send()
            if k < depth - 1:

                @pl.when(sp > 0)
                def _():
                    x_move(sp, dn_send.at[k], dn_recv.at[k], dn_to).wait_send()

        wz_block(k).wait_send()
        e_block(k).wait_send()
    for k in range(depth):
        for side in range(2):
            p_block(k, side).wait_send()
        f_block(k).wait_send()


def front(inputs, gain, weights, kv, extra, ddown, dup, doff, edown, eup, eoff):
    depth = lax.axis_size("sp")
    width = lax.axis_size("fs")
    _, tokens, half = inputs.shape
    total = tokens * depth
    dma = pltpu.SemaphoreType.DMA
    any_spec = pl.BlockSpec(memory_space=pl.ANY)
    vmem_spec = pl.BlockSpec(memory_space=pltpu.VMEM)
    low = ddown.shape[1]
    return pl.pallas_call(
        front_kernel,
        in_specs=[any_spec] * 9 + [vmem_spec] * 5,
        out_specs=[vmem_spec] * 3,
        out_shape=[
            jax.ShapeDtypeStruct((total, 5 * PAIR), BF16),
            jax.ShapeDtypeStruct((2, total, PAIR), F32),
            jax.ShapeDtypeStruct((2, total, PAIR), F32),
        ],
        scratch_shapes=[
            pltpu.VMEM((depth, 2, tokens, half), BF16),
            pltpu.VMEM((2 * half, 5 * PAIR), BF16),
            pltpu.VMEM((depth, extra.shape[1], tokens), F32),
            pltpu.VMEM((2, low, PAIR), BF16),
            pltpu.VMEM((2, low, PAIR), BF16),
            dma((4,)),
            dma((5,)),
            dma((depth,)),
            dma((depth,)),
            dma((depth,)),
            dma((depth,)),
            dma((2 * depth,)),
            dma((2 * depth,)),
            dma((depth - 1,)),
            dma((depth - 1,)),
            dma((depth - 1,)),
            dma((depth - 1,)),
            dma((width, 2)),
            dma((width, 2)),
            dma((width,)),
            dma((width,)),
        ],
        compiler_params=pltpu.CompilerParams(collective_id=0, has_side_effects=True),
        name="front",
    )(
        inputs,
        *weights,
        kv,
        extra,
        dup,
        eup,
        gain[None, :],
        ddown,
        edown,
        doff,
        eoff,
    )


SPAN = HD
BATCH = 4
QUAD = 4 * HD
TN = (((0,), (0,)), ((), ()))


def mm(left, right, dims=NN):
    return lax.dot_general(left, right, dims, preferred_element_type=F32)


def rope_tables(total):
    quarter = HD // 4
    inverse = ROPE_BASE ** (-np.arange(quarter, dtype=np.float32) / np.float32(quarter))
    inverse = inverse.astype(np.float32)
    lane = np.arange(PAIR) % HD
    rates = inverse[lane % quarter]
    sign = np.where(lane % (2 * quarter) < quarter, -1.0, 1.0)
    coords = np.concatenate([np.arange(total // GRID_W), np.arange(GRID_W)])
    angles = (coords.astype(np.float32)[:, None] * rates[None, :]).astype(np.float64)
    return np.stack([np.cos(angles), np.sin(angles) * sign]).astype(np.float32)


def mix_body(
    hook, proj_ref, log_ref, learn_ref, table_ref, gain, sinks, states, mix_ref, s_w, s_read, s_m, s_a, s_local, s_re, s_lin, kpad, vpad, s_q
):
    total = proj_ref.shape[0]
    count = total // SPAN
    lane = lax.broadcasted_iota(jnp.int32, (SPAN, PAIR), 1)
    first = lane < HD
    ones = (
        jnp.where(first, 1.0, 0.0).astype(BF16),
        jnp.where(first, 0.0, 1.0).astype(BF16),
    )
    nothing = jnp.zeros((SPAN, PAIR), BF16)
    quad_row = lax.broadcasted_iota(jnp.int32, (SPAN, QUAD), 0)
    quad_lane = lax.broadcasted_iota(jnp.int32, (SPAN, QUAD), 1)
    quad_col = lax.rem(quad_lane, HD)
    ahead = quad_lane < PAIR
    before = jnp.where(ahead, quad_col - quad_row, quad_row - quad_col)
    strict, upto = before < 0, before <= 0
    eye = jnp.where(before == 0, 1.0, 0.0)

    def level(size):
        return (lax.div(quad_row, 2 * size) == lax.div(quad_col, 2 * size)) & (
            lax.div(quad_row, size) != lax.div(quad_col, size)
        )

    square_i = lax.broadcasted_iota(jnp.int32, (QUAD, QUAD), 0)
    square_j = lax.broadcasted_iota(jnp.int32, (QUAD, QUAD), 1)
    same_unit = lax.div(square_i, HD) == lax.div(square_j, HD)
    square_eye = square_i == square_j
    tri_i = lax.broadcasted_iota(jnp.int32, (SPAN, SPAN), 0)
    tri_j = lax.broadcasted_iota(jnp.int32, (SPAN, SPAN), 1)
    tri = [
        jnp.where(tri_j <= tri_i, 1.0, 0.0).astype(BF16),
        jnp.where(tri_j >= tri_i, 1.0, 0.0).astype(BF16),
    ]
    tri = [jnp.concatenate([one] * 3, axis=1) for one in tri]

    def diagonal(quad):
        left, right = quad[:, :PAIR], quad[:, PAIR:]
        return jnp.concatenate(
            [jnp.concatenate([left * one, nothing], axis=1) for one in ones]
            + [jnp.concatenate([nothing, right * one], axis=1) for one in ones],
            axis=0,
        )

    def quad_dot(lefts, right, dims=NN):
        highs, lows = zip(*[halves(left) for left in lefts])
        right_high, right_low = halves(right)
        count_left = len(lefts)
        outer = mm(jnp.concatenate(highs + lows, axis=0), diagonal(right_high), dims)
        inner = mm(jnp.concatenate(highs, axis=0), diagonal(right_low), dims)
        return [
            outer[k * SPAN : (k + 1) * SPAN]
            + (
                outer[(count_left + k) * SPAN : (count_left + k + 1) * SPAN]
                + inner[k * SPAN : (k + 1) * SPAN]
            )
            for k in range(count_left)
        ]

    def single(left, right):
        return mm(left.astype(BF16), diagonal(right.astype(BF16)))

    def rows_at(place):
        return pl.ds(pl.multiple_of(place * SPAN, SPAN), SPAN)

    def head_sum(value):
        low = jnp.sum(jnp.where(first, value, 0.0), axis=1, keepdims=True)
        high = jnp.sum(jnp.where(first, 0.0, value), axis=1, keepdims=True)
        return jnp.where(first, low, high)

    def prepare(direction, rows):
        read = proj_ref[rows, :PAIR].astype(F32)
        key = proj_ref[rows, PAIR : 2 * PAIR].astype(F32)
        log_decay = log_ref[direction, rows, :]
        unit = key * lax.rsqrt(head_sum(key * key) + NORM_EPS)
        erase = unit * learn_ref[direction, rows, :]
        high = log_decay.astype(BF16)
        rest = log_decay - high.astype(F32)
        middle_part = rest.astype(BF16)
        low = (rest - middle_part.astype(F32)).astype(BF16)
        total_log = mm(tri[direction], jnp.concatenate([high, middle_part, low], axis=0))
        end = SPAN - 1 if direction == 0 else 0
        span_log = total_log[end : end + 1, :]
        middle = 0.5 * span_log
        prior_log = total_log - log_decay
        inverse = jnp.exp(middle - total_log)
        left = jnp.exp(span_log - total_log)
        readers = jnp.concatenate(
            [jnp.exp(prior_log - middle) * unit, jnp.exp(total_log - middle) * read], axis=0
        )
        sources = jnp.concatenate([erase * inverse, key * inverse], axis=0)
        high_r, low_r = halves(readers)
        high_s, low_s = halves(sources)

        def spread(value):
            top, bottom = value[:SPAN], value[SPAN:]
            return jnp.concatenate([top * one for one in ones] + [bottom * one for one in ones], axis=0)

        high_s, low_s = spread(high_s), spread(low_s)
        meets = mm(
            jnp.concatenate([high_r, low_r, high_r], axis=1),
            jnp.concatenate([high_s, high_s, low_s], axis=1),
            NT,
        )
        return (
            meets,
            jnp.exp(prior_log) * unit,
            jnp.exp(total_log) * read,
            key * left,
            erase * left,
            jnp.exp(span_log),
        )

    def both(one, other):
        return jnp.concatenate([one, other], axis=1)

    def batch(index, carry, size):
        groups = [index * size + k for k in range(size)]
        erased, seens, read_eraseds, starts, lefts, finals, spans, values = [], [], [], [], [], [], [], []
        for group in groups:
            rows = (rows_at(group), rows_at(count - 1 - group))
            parts = [prepare(direction, rows[direction]) for direction in range(2)]
            meets = [part[0] for part in parts]
            value = both(*[proj_ref[row, 2 * PAIR : 3 * PAIR] for row in rows])
            erased.append(
                jnp.where(strict, both(meets[0][:SPAN, :PAIR], meets[1][:SPAN, :PAIR]), 0.0)
            )
            seen = jnp.where(strict, both(meets[0][:SPAN, PAIR:], meets[1][:SPAN, PAIR:]), 0.0)
            s_re[group] = jnp.where(
                upto, both(meets[0][SPAN:, :PAIR], meets[1][SPAN:, :PAIR]), 0.0
            )
            read_seen = jnp.where(upto, both(meets[0][SPAN:, PAIR:], meets[1][SPAN:, PAIR:]), 0.0)
            starts.append(both(parts[0][1], parts[1][1]))
            s_read[group] = both(parts[0][2], parts[1][2])
            lefts.append((both(parts[0][3], parts[1][3]), both(parts[0][4], parts[1][4])))
            spans.append(both(parts[0][5], parts[1][5]))
            values.append(value)
            pieces = jnp.concatenate([*halves(seen), *halves(read_seen)], axis=0)
            met = mm(pieces, diagonal(value))
            seens.append(met[:SPAN] + met[SPAN : 2 * SPAN])
            s_local[group] = met[2 * SPAN : 3 * SPAN] + met[3 * SPAN :]
        solves = [eye - jnp.where(level(1), one, 0.0) for one in erased]
        width = 2
        while width < SPAN:
            at = level(width)
            firsts = [single(solve, jnp.where(at, one, 0.0)) for solve, one in zip(solves, erased)]
            solves = [solve - single(one, solve) for solve, one in zip(solves, firsts)]
            width *= 2
        misses = [
            eye - solve - quad_dot([one], solve)[0] for solve, one in zip(solves, erased)
        ]
        solves = [solve + single(solve, miss) for solve, miss in zip(solves, misses)]
        maps = [quad_dot([solve], start)[0] for solve, start in zip(solves, starts)]
        shifts = [quad_dot([solve], seen)[0] for solve, seen in zip(solves, seens)]
        for place, group in enumerate(groups):
            key_left, erase_left = lefts[place]
            s_w[group] = jnp.concatenate([maps[place], shifts[place]], axis=1)
            map_high, map_low = halves(maps[place])
            left_high, left_low = halves(erase_left)
            fade = mm(
                jnp.concatenate([map_high, map_low, map_high], axis=0),
                jnp.concatenate([left_high, left_high, left_low], axis=0),
                TN,
            )
            s_m[group] = jnp.where(square_eye, spans[place], 0.0) - jnp.where(same_unit, fade, 0.0)
            shift_high, shift_low = halves(shifts[place])
            key_high, key_low = halves(key_left)
            gained = mm(
                jnp.concatenate(
                    [values[place], values[place], shift_high, shift_low, shift_high], axis=0
                ),
                jnp.concatenate(
                    [key_high, key_low, -left_high, -left_high, -left_low], axis=0
                ),
                TN,
            )
            gained = jnp.where(same_unit, gained, 0.0)
            s_a[group] = (gained[:SPAN] + gained[SPAN : 2 * SPAN]) + (
                gained[2 * SPAN : 3 * SPAN] + gained[3 * SPAN :]
            )
        return carry

    size = min(BATCH, count)
    for index in range(count // size):
        batch(index, 0, size)
        hook()

    def advance(group, state):
        high, low = halves(state)
        step_high, step_low = halves(s_m[group])
        outer = mm(jnp.concatenate([high, low], axis=0), step_high)
        inner = mm(high, step_low)
        following = outer[:SPAN] + (outer[SPAN:] + inner) + s_a[group]
        s_a[group] = state
        return following

    state = states
    for group in range(count):
        state = advance(group, state)
    hook()

    def finish(group, carry):
        maps, shift = s_w[group, :, :QUAD], s_w[group, :, QUAD:]
        dropped, seen_state = quad_dot([maps, s_read[group]], s_a[group], NT)
        dropped = dropped + shift
        out = seen_state + s_local[group] - quad_dot([s_re[group]], dropped)[0]
        s_lin[0, rows_at(group), :] = out[:, :PAIR]
        s_lin[1, rows_at(count - 1 - group), :] = out[:, PAIR:]
        return carry

    def finish_batch(index, carry):
        for k in range(size):
            carry = finish(index * size + k, carry)
        return carry

    lax.fori_loop(0, count // size, finish_batch, 0)
    hook()

    quarter = HD // 4
    back = lax.rem(lane, 2 * quarter) >= quarter
    by_row = lax.rem(lane, HD) < 2 * quarter
    grid = total // GRID_W
    edge = jnp.zeros((WINDOW, PAIR), BF16)
    for ref in (kpad, vpad):
        ref[:WINDOW, :] = edge
        ref[WINDOW + total :, :] = edge

    def turned(value, cosine, sine):
        partner = jnp.where(
            back, pltpu.roll(value, quarter, 1), pltpu.roll(value, PAIR - quarter, 1)
        )
        return value * cosine + partner * sine

    def turn(place, carry):
        rows = rows_at(place)
        cosine, sine = [
            jnp.where(
                by_row,
                table_ref[which, pl.ds(place, 1), :],
                table_ref[which, grid : grid + GRID_W, :],
            )
            for which in range(2)
        ]
        query = proj_ref[rows, 3 * PAIR : 4 * PAIR].astype(F32)
        pair = proj_ref[rows, 4 * PAIR :].astype(F32)
        s_q[rows, :] = turned(query, cosine, sine).astype(BF16)
        key = jnp.where(first, turned(pair, cosine, sine), 0.0)
        value = jnp.where(first, 0.0, pair)
        there = pl.ds(pl.multiple_of(WINDOW + place * SPAN, SPAN), SPAN)
        kpad[there, :] = (key + pltpu.roll(key, HD, 1)).astype(BF16)
        vpad[there, :] = (value + pltpu.roll(value, HD, 1)).astype(BF16)
        return carry

    lax.fori_loop(0, grid, turn, 0)
    reach = ATT_BLOCK + 2 * WINDOW
    ahead_of = lax.broadcasted_iota(jnp.int32, (ATT_BLOCK, reach), 1) - (
        WINDOW + lax.broadcasted_iota(jnp.int32, (ATT_BLOCK, reach), 0)
    )
    near = jnp.abs(ahead_of) <= WINDOW
    key_at = lax.broadcasted_iota(jnp.int32, (ATT_BLOCK, reach), 1) - WINDOW
    mine = lax.broadcasted_iota(jnp.int32, (ATT_BLOCK, PAIR), 1) < HD

    def attend(place, carry):
        start = pl.multiple_of(place * ATT_BLOCK, ATT_BLOCK)
        rows = pl.ds(start, ATT_BLOCK)
        query = s_q[rows, :]
        keys = kpad[pl.ds(start, reach), :]
        held = vpad[pl.ds(start, reach), :]
        allowed = near & (key_at >= -start) & (key_at < total - start)
        mixed = []
        for head in range(2):
            own = jnp.where(mine if head == 0 else jnp.logical_not(mine), query.astype(F32), 0.0)
            scores = mm(own.astype(BF16), keys, NT) * HD ** (-0.5)
            scores = jnp.where(allowed, scores, -jnp.inf)
            top = jnp.maximum(jnp.max(scores, axis=1, keepdims=True), sinks[head])
            raised = jnp.exp(scores - top)
            bottom = jnp.exp(sinks[head] - top) + jnp.sum(raised, axis=1, keepdims=True)
            mixed.append(mm((raised / bottom).astype(BF16), held))
        mix_ref[rows, PAIR:] = jnp.where(mine, mixed[0], mixed[1]).astype(BF16)
        return carry

    lax.fori_loop(0, total // ATT_BLOCK, attend, 0)
    hook()

    def norm(place, carry):
        rows = rows_at(place)
        lin_sum = s_lin[0, rows, :] + s_lin[1, rows, :]
        centred = lin_sum - head_sum(lin_sum) * (1.0 / HD)
        spread = head_sum(centred * centred) * (1.0 / HD)
        mix_ref[rows, :PAIR] = (centred * lax.rsqrt(spread + GROUP_EPS) * gain).astype(BF16)
        return carry

    lax.fori_loop(0, count, norm, 0)


def mix_scratch(total):
    count = total // SPAN
    return [
        pltpu.VMEM((count, SPAN, 2 * QUAD), F32),
        pltpu.VMEM((count, SPAN, QUAD), F32),
        pltpu.VMEM((count, QUAD, QUAD), F32),
        pltpu.VMEM((count, SPAN, QUAD), F32),
        pltpu.VMEM((count, SPAN, QUAD), F32),
        pltpu.VMEM((count, SPAN, QUAD), F32),
        pltpu.VMEM((2, total, PAIR), F32),
        pltpu.VMEM((total + 2 * WINDOW, PAIR), BF16),
        pltpu.VMEM((total + 2 * WINDOW, PAIR), BF16),
        pltpu.VMEM((total, PAIR), BF16),
    ]


def back_kernel(
    lin_ref,
    win_ref,
    init_ref,
    sink_ref,
    proj_ref,
    log_ref,
    learn_ref,
    table_ref,
    gain_ref,
    out_ref,
    owb,
    mbuf,
    mix_ref,
    init,
    local_sem,
    z_send,
    z_recv,
    p_send,
    p_recv,
    f_send,
    f_recv,
    sib_send,
    sib_recv,
    m_send,
    m_recv,
    *scratch,
):
    sp, fs, tp = lax.axis_index("sp"), lax.axis_index("fs"), lax.axis_index("tp")
    depth = lax.axis_size("sp")
    width = lax.axis_size("fs")
    sides = lax.axis_size("tp")
    rows, cols = lin_ref.shape
    share = out_ref.shape[1]
    sibling = {"tp": 1 - tp}
    plane = ({"fs": flipped(fs, 1)}, {"fs": flipped(fs, 2)})

    def remote(src, dst, send, recv, device):
        return pltpu.make_async_remote_copy(
            src_ref=src,
            dst_ref=dst,
            send_sem=send,
            recv_sem=recv,
            device_id=device,
            device_id_type=MESH_IDS,
        )

    def cols_of(z, f, many=1):
        return pl.ds(pl.multiple_of((z * width + f) * cols, cols), many * cols)

    local = [
        pltpu.make_async_copy(
            ref, owb.at[tp, pl.ds(place * rows, rows), cols_of(sp, fs)], local_sem.at[place]
        )
        for place, ref in enumerate((lin_ref, win_ref))
    ]
    head = (tp * depth + sp) * 2
    local.append(pltpu.make_async_copy(init_ref.at[:, pl.ds(head, 2)], init, local_sem.at[2]))
    for copy in local:
        copy.start()
    barrier = pltpu.get_barrier_semaphore()
    pairs = [(k, t) for k in range(depth) for t in range(sides) if k or t]
    peers = [{"sp": flipped(sp, k), "tp": tp + t - 2 * t * tp} for k, t in pairs] + [*plane]
    for peer in peers:
        pl.semaphore_signal(barrier, inc=1, device_id=peer, device_id_type=MESH_IDS)
    pl.semaphore_wait(barrier, len(peers))
    for copy in local:
        copy.wait()

    def z_block(k):
        there = owb.at[tp, :, cols_of(sp, fs)]
        return remote(there, there, z_send.at[k - 1], z_recv.at[k - 1], {"sp": flipped(sp, k)})

    def p_block(k, side):
        there = owb.at[tp, :, cols_of(flipped(sp, k), fs)]
        return remote(there, there, p_send.at[k, side], p_recv.at[k, side], plane[side])

    def f_block(k):
        side = k % 2
        there = owb.at[tp, :, cols_of(flipped(sp, k), flipped(fs, 2 if side == 0 else 1))]
        return remote(there, there, f_send.at[k], f_recv.at[k], plane[side])

    def s_block(k):
        there = owb.at[tp, :, cols_of(flipped(sp, k), 0, width)]
        return remote(there, there, sib_send.at[k], sib_recv.at[k], sibling)

    def w_step(k):
        if k:
            z_block(k).wait_recv()
        for side in range(2):
            p_block(k, side).start()

    def f_step(k):
        for side in range(2):
            p_block(k, side).wait_recv()
        f_block(k).start()

    def s_step(k):
        f_block(k).wait_recv()
        s_block(k).start()

    for k in range(1, depth):
        z_block(k).start()
    w_step(0)
    plan = [
        [(f_step, 0), (w_step, 1)],
        [(s_step, 0), (w_step, 2)],
        [(f_step, 1)],
        [(w_step, 3), (s_step, 1)],
        [(f_step, 2)],
    ]
    queue = iter(plan)

    def hook():
        for step, k in next(queue, ()):
            step(k)

    states = jnp.concatenate([init[d, h] for d in range(2) for h in range(2)], axis=1)
    lanes = pl.ds(pl.multiple_of((tp * depth + sp) * PAIR, PAIR), PAIR)
    mix_body(
        hook,
        proj_ref,
        log_ref,
        learn_ref,
        table_ref,
        gain_ref[:, lanes],
        [sink_ref[0, head], sink_ref[0, head + 1]],
        states,
        mix_ref,
        *scratch,
    )

    def m_block(k, t):
        z, side = flipped(sp, k), tp + t - 2 * t * tp
        start = pl.multiple_of((z * sides + side) * share, share)
        return remote(
            mix_ref.at[pl.ds(start, share)],
            mbuf.at[sp * sides + tp],
            m_send.at[k * sides + t],
            m_recv.at[k * sides + t],
            {"sp": z, "tp": side},
        )

    for k, t in pairs:
        m_block(k, t).start()
    mine = sp * sides + tp
    mbuf[mine] = mix_ref[pl.ds(pl.multiple_of(mine * share, share), share), :]
    f_step(3)
    s_step(2)
    s_step(3)
    for k, t in pairs:
        m_block(k, t).wait_recv()
    lefts = [
        jnp.concatenate(
            [mbuf[z * sides + side, :, :PAIR] for z in range(depth)]
            + [mbuf[z * sides + side, :, PAIR:] for z in range(depth)],
            axis=1,
        )
        for side in range(sides)
    ]
    for k in range(depth):
        s_block(k).wait_recv()
        span = cols_of(flipped(sp, k), 0, width)
        out_ref[0, :, span] = sum(
            jnp.dot(lefts[side], owb[side, :, span], preferred_element_type=F32)
            for side in range(sides)
        ).astype(BF16)
    for k in range(depth):
        if k:
            z_block(k).wait_send()
        for side in range(2):
            p_block(k, side).wait_send()
        f_block(k).wait_send()
        s_block(k).wait_send()
    for k, t in pairs:
        m_block(k, t).wait_send()


def back(proj, logs, learn, gain, sink, init, lin_weight, win_weight):
    depth = lax.axis_size("sp")
    width = lax.axis_size("fs")
    sides = lax.axis_size("tp")
    total = proj.shape[0]
    rows, cols = lin_weight.shape
    share = total // (depth * sides)
    dma = pltpu.SemaphoreType.DMA
    any_spec = pl.BlockSpec(memory_space=pl.ANY)
    vmem_spec = pl.BlockSpec(memory_space=pltpu.VMEM)
    features = cols * depth * width
    return pl.pallas_call(
        back_kernel,
        in_specs=[any_spec] * 3 + [pl.BlockSpec(memory_space=pltpu.SMEM)] + [vmem_spec] * 5,
        out_specs=vmem_spec,
        out_shape=jax.ShapeDtypeStruct((1, share, features), BF16),
        scratch_shapes=[
            pltpu.VMEM((sides, 2 * rows, features), BF16),
            pltpu.VMEM((depth * sides, share, 2 * PAIR), BF16),
            pltpu.VMEM((total, 2 * PAIR), BF16),
            pltpu.VMEM((2, 2, HD, HD), F32),
            dma((3,)),
            dma((depth - 1,)),
            dma((depth - 1,)),
            dma((depth, 2)),
            dma((depth, 2)),
            dma((depth,)),
            dma((depth,)),
            dma((depth,)),
            dma((depth,)),
            dma((depth * sides,)),
            dma((depth * sides,)),
        ]
        + mix_scratch(total),
        compiler_params=pltpu.CompilerParams(
            collective_id=1, has_side_effects=True, vmem_limit_bytes=60 * 2**20
        ),
        name="back",
    )(
        lin_weight,
        win_weight,
        init,
        sink[None, :],
        proj,
        logs,
        learn,
        jnp.asarray(rope_tables(total)),
        gain[None, :],
    )


def by_heads(
    inputs,
    input_norm_gain,
    receptance_weight,
    linear_key_weight,
    linear_value_weight,
    window_query_weight,
    window_key_weight,
    window_value_weight,
    decay_down_weight,
    decay_up_weight,
    decay_offset,
    decay_log_extra,
    erasure_down_weight,
    erasure_up_weight,
    erasure_offset,
    initial_state,
    head_norm_gain,
    query_sink_logit,
    linear_output_weight,
    window_output_weight,
):
    count = window_key_weight.shape[0]
    kv = jnp.concatenate(
        [
            weight.reshape(count, -1, HD)
            for weight in (window_key_weight, window_value_weight)
        ],
        axis=2,
    ).reshape(count, -1)
    proj, logs, learn = front(
        inputs,
        input_norm_gain,
        (receptance_weight, linear_key_weight, linear_value_weight, window_query_weight),
        kv,
        decay_log_extra,
        decay_down_weight,
        decay_up_weight,
        decay_offset,
        erasure_down_weight,
        erasure_up_weight,
        erasure_offset,
    )
    return back(
        proj,
        logs,
        learn,
        head_norm_gain,
        query_sink_logit,
        initial_state,
        linear_output_weight,
        window_output_weight,
    )


def layer(*arrays):
    inputs, recept, keys = arrays[0], arrays[2], arrays[6]
    depth, width, sides = [lax.axis_size(axis) for axis in ("sp", "fs", "tp")]
    fits = (
        recept.shape[1] == arrays[5].shape[1] == depth * PAIR
        and 2 * keys.shape[1] == depth * HD
        and (depth, width, sides) == (4, 4, 2)
        and inputs.shape[1] % WINDOW == 0
        and SPAN == GRID_W
    )
    return (by_heads if fits else local)(*arrays)


def solution(mesh):
    return jax.shard_map(
        layer,
        mesh=mesh,
        in_specs=(
            P("fs", "sp", "tp"),
            P(),
            P(("sp", "fs"), "tp"),
            P(("sp", "fs"), "tp"),
            P(("sp", "fs"), "tp"),
            P(("sp", "fs"), "tp"),
            P(("sp", "fs"), "tp"),
            P(("sp", "fs"), "tp"),
            P(),
            P(),
            P(),
            P("fs", "tp", "sp"),
            P(),
            P(),
            P(),
            P(),
            P(),
            P(),
            P("tp", ("sp", "fs")),
            P("tp", ("sp", "fs")),
        ),
        out_specs=P("fs", ("sp", "tp"), None),
        check_vma=False,
    )
```

```python
import jax
import jax.numpy as jnp
import numpy as np
from jax import lax
from jax.experimental import pallas as pl
from jax.experimental.pallas import tpu as pltpu
from jax.sharding import PartitionSpec as P

HD = 64
WINDOW = 128
GRID_W = 64
ATT_BLOCK = 128


NORM_EPS = 1e-06
GROUP_EPS = 0.00064
ROPE_BASE = 10000.0
HIGHEST = lax.Precision.HIGHEST


def padded(block, sides, width):
    for axis, dim in sides:
        count = lax.axis_size(axis)
        forward = [(i, i + 1) for i in range(count - 1)]
        backward = [(target, source) for source, target in forward]
        low = lax.ppermute(
            lax.slice_in_dim(block, block.shape[dim] - width, None, axis=dim), axis, forward
        )
        high = lax.ppermute(lax.slice_in_dim(block, 0, width, axis=dim), axis, backward)
        block = jnp.concatenate([low, block, high], axis=dim)
    return block


def to_bf16(array):
    return lax.optimization_barrier(array.astype(jnp.bfloat16))


def rope_axial(values, positions):
    quarter = values.shape[-1] // 4
    inverse = ROPE_BASE ** (-jnp.arange(quarter, dtype=jnp.float32) / quarter)
    grid_rows = (positions // GRID_W).astype(jnp.float32)
    grid_cols = (positions % GRID_W).astype(jnp.float32)
    pieces = []
    for which_half, coordinate in ((0, grid_rows), (1, grid_cols)):
        angles = coordinate[:, None] * inverse[None, :]
        cosine = jnp.cos(angles)[:, None, :]
        sine_part = jnp.sin(angles)[:, None, :]
        front_part = values[..., 2 * which_half * quarter : (2 * which_half + 1) * quarter]
        back_part = values[..., (2 * which_half + 1) * quarter : (2 * which_half + 2) * quarter]
        pieces.append(front_part * cosine - back_part * sine_part)
        pieces.append(front_part * sine_part + back_part * cosine)
    return jnp.concatenate(pieces, axis=-1)


CHUNK = 32
PAIR = 2 * HD
F32 = jnp.float32
BF16 = jnp.bfloat16
NN = (((1,), (0,)), ((), ()))
NT = (((1,), (1,)), ((), ()))


def dot1(left, right, dims=NN):
    return lax.dot_general(
        left.astype(jnp.bfloat16), right.astype(jnp.bfloat16), dims, preferred_element_type=F32
    )


def halves(value):
    high = value.astype(jnp.bfloat16)
    return high, (value - high.astype(F32)).astype(jnp.bfloat16)


def dot3(left, right, dims=NN):
    left_high, left_low = halves(left)
    right_high, right_low = halves(right)

    def product(one, other):
        return lax.dot_general(one, other, dims, preferred_element_type=F32)

    return product(left_high, right_high) + (
        product(left_high, right_low) + product(left_low, right_high)
    )


def full_dot(left, right):
    return lax.dot_general(left, right, NN, precision=HIGHEST, preferred_element_type=F32)


def chunk_kernel(read_ref, key_ref, value_ref, log_ref, learn_ref, out_ref, end_ref):
    tokens = read_ref.shape[0]
    read = read_ref[...].astype(F32)
    key = key_ref[...].astype(F32)
    value = value_ref[...].astype(F32)
    first = lax.broadcasted_iota(jnp.int32, (tokens, PAIR), 1) < HD
    pair_i = lax.broadcasted_iota(jnp.int32, (PAIR, PAIR), 0)
    pair_j = lax.broadcasted_iota(jnp.int32, (PAIR, PAIR), 1)
    same_head = jnp.where(pair_i // HD == pair_j // HD, 1.0, 0.0)
    row = lax.broadcasted_iota(jnp.int32, (tokens, tokens), 0)
    col = lax.broadcasted_iota(jnp.int32, (tokens, tokens), 1)
    same_chunk = row // CHUNK == col // CHUNK
    eye = jnp.where(row == col, 1.0, 0.0)
    unit = key * lax.rsqrt(full_dot(key * key, same_head) + NORM_EPS)
    own = (first, jnp.logical_not(first))
    values = (
        jnp.where(first, value, 0.0),
        jnp.where(first, pltpu.roll(value, HD, 1), 0.0),
    )
    all_chunk = jnp.where(same_chunk, 1.0, 0.0)
    for direction in range(2):
        before = (col < row) if direction == 0 else (col > row)
        strict = same_chunk & before
        upto = same_chunk & (before | (col == row))
        log_decay = log_ref[direction]
        erase = unit * learn_ref[direction]
        total_log = full_dot(jnp.where(upto, 1.0, 0.0), log_decay)
        chunk_log = full_dot(all_chunk, log_decay)
        prior_log = total_log - log_decay
        middle = 0.5 * chunk_log
        unit_start = jnp.exp(prior_log) * unit
        unit_mid = jnp.exp(prior_log - middle) * unit
        read_start = jnp.exp(total_log) * read
        read_mid = jnp.exp(total_log - middle) * read
        inverse = jnp.exp(middle - total_log)
        sources = jnp.concatenate([erase * inverse, key * inverse], axis=0)
        rest = jnp.exp(chunk_log - total_log)
        key_rest = key * rest
        erase_rest = erase * rest
        chunk_decay = jnp.exp(chunk_log).T
        solved, offsets, mixes = [], [], []
        for head in range(2):
            readers = jnp.concatenate(
                [jnp.where(own[head], unit_mid, 0.0), jnp.where(own[head], read_mid, 0.0)], axis=0
            )
            meets = dot3(readers, sources, NT)
            erased = jnp.where(strict, meets[:tokens, :tokens], 0.0)
            seen = jnp.where(strict, meets[:tokens, tokens:], 0.0)
            read_erased = jnp.where(upto, meets[tokens:, :tokens], 0.0)
            read_seen = jnp.where(upto, meets[tokens:, tokens:], 0.0)
            solve = eye - jnp.where(row // 2 == col // 2, erased, 0.0)
            size = 2
            while size < CHUNK:
                level = (row // (2 * size) == col // (2 * size)) & (row // size != col // size)
                solve = solve - dot1(dot1(solve, jnp.where(level, erased, 0.0)), solve)
                size *= 2
            solve = solve + dot1(solve, eye - solve - dot3(erased, solve))
            both = dot3(
                solve,
                jnp.concatenate(
                    [jnp.where(own[head], unit_start, 0.0), dot3(seen, values[head])], axis=1
                ),
            )
            solved.append(both[:, :PAIR])
            offsets.append(both[:, PAIR:])
            mixes.append(jnp.concatenate([read_seen, -read_erased], axis=1))
        state = jnp.where(pair_j == HD + pair_i % HD, 1.0, 0.0)
        count = tokens // CHUNK
        drops = [[None] * count, [None] * count]
        reads = [[None] * count, [None] * count]
        for step in range(count):
            place = step if direction == 0 else count - 1 - step
            rows = slice(place * CHUNK, (place + 1) * CHUNK)
            lefts = jnp.concatenate(
                [solved[0][rows], solved[1][rows]]
                + [jnp.where(own[head], read_start, 0.0)[rows] for head in range(2)],
                axis=0,
            )
            seen_state = dot3(lefts, state)
            for head in range(2):
                drops[head][place] = (
                    seen_state[head * CHUNK : (head + 1) * CHUNK] + offsets[head][rows]
                )
                reads[head][place] = seen_state[(2 + head) * CHUNK : (3 + head) * CHUNK]
            adders = jnp.concatenate(
                [jnp.where(own[head], key_rest, 0.0)[rows] for head in range(2)]
                + [jnp.where(own[head], -erase_rest, 0.0)[rows] for head in range(2)],
                axis=0,
            ).T
            added = jnp.concatenate(
                [values[0][rows], values[1][rows], drops[0][place], drops[1][place]], axis=0
            )
            first_col = place * CHUNK
            state = chunk_decay[:, first_col : first_col + 1] * state + dot3(adders, added)
        for head in range(2):
            dropped = jnp.concatenate(drops[head], axis=0)
            out_ref[direction, head] = jnp.concatenate(reads[head], axis=0) + dot3(
                mixes[head], jnp.concatenate([values[head], dropped], axis=0)
            )
        end_ref[direction] = state


def chunked(returned, log_decay, learn, head_width):
    tokens = returned.shape[0]
    pairs = head_width // PAIR

    def role(which):
        return pl.BlockSpec((tokens, PAIR), lambda p: (0, which * pairs + p))

    wide = pl.BlockSpec((2, tokens, PAIR), lambda p: (0, 0, p))
    return pl.pallas_call(
        chunk_kernel,
        grid=(pairs,),
        in_specs=[role(0), role(1), role(2), wide, wide],
        out_specs=[
            pl.BlockSpec((2, 2, tokens, PAIR), lambda p: (0, p, 0, 0)),
            pl.BlockSpec((2, PAIR, PAIR), lambda p: (0, p, 0)),
        ],
        out_shape=[
            jax.ShapeDtypeStruct((2, 2 * pairs, tokens, PAIR), F32),
            jax.ShapeDtypeStruct((2, pairs * PAIR, PAIR), F32),
        ],
        cost_estimate=pl.CostEstimate(
            flops=pairs * 400 * PAIR**3, bytes_accessed=8 * tokens * head_width * 4, transcendentals=0
        ),
        name="chunked_state",
    )(returned, returned, returned, log_decay, learn)


def merge_kernel(local_ref, state_ref, gain_ref, out_ref):
    pair_i = lax.broadcasted_iota(jnp.int32, (PAIR, PAIR), 0)
    pair_j = lax.broadcasted_iota(jnp.int32, (PAIR, PAIR), 1)
    average = jnp.where(pair_i // HD == pair_j // HD, 1.0 / HD, 0.0)
    sums = []
    for head in range(2):
        total = 0.0
        for direction in range(2):
            block = local_ref[direction, head]
            total = total + (
                block[:, :HD] + dot3(block[:, HD:], state_ref[direction, head])
            )
        sums.append(total)
    lin_sum = jnp.concatenate(sums, axis=1)
    centred = lin_sum - full_dot(lin_sum, average)
    normed = centred * lax.rsqrt(full_dot(centred * centred, average) + GROUP_EPS)
    out_ref[...] = (normed * gain_ref[...]).astype(jnp.bfloat16)


def merged(local_out, entry, gain):
    _, head_count, tokens, _ = local_out.shape
    pairs = head_count // 2
    return pl.pallas_call(
        merge_kernel,
        grid=(pairs,),
        in_specs=[
            pl.BlockSpec((2, 2, tokens, PAIR), lambda p: (0, p, 0, 0)),
            pl.BlockSpec((2, 2, HD, HD), lambda p: (0, p, 0, 0)),
            pl.BlockSpec((1, PAIR), lambda p: (0, p)),
        ],
        out_specs=pl.BlockSpec((tokens, PAIR), lambda p: (0, p)),
        out_shape=jax.ShapeDtypeStruct((tokens, head_count * HD), jnp.bfloat16),
        cost_estimate=pl.CostEstimate(
            flops=pairs * 30 * PAIR**3, bytes_accessed=4 * tokens * head_count * PAIR * 4, transcendentals=0
        ),
        name="merged_norm",
    )(local_out, entry, gain[None, :])


def entering_states(ends, initial):
    count = lax.axis_size("sp")
    place = lax.axis_index("sp")
    ups = [(i, i + 1) for i in range(count - 1)]
    downs = [(i + 1, i) for i in range(count - 1)]
    adds, maps = ends[..., :HD], ends[..., HD:]

    def hop(_, states):
        later = jnp.einsum("dhkj,dhjv->dhkv", maps, states, precision=HIGHEST) + adds
        forward = lax.ppermute(later[0], "sp", ups)
        backward = lax.ppermute(later[1], "sp", downs)
        return jnp.stack(
            [
                jnp.where(place == 0, initial[0], forward),
                jnp.where(place == count - 1, initial[1], backward),
            ]
        )

    states = initial
    if count > 8:
        return lax.fori_loop(0, count - 1, hop, states)
    for _ in range(count - 1):
        states = hop(0, states)
    return states


def swapped(block, axis):
    count = lax.axis_size(axis)
    return [block] + [
        lax.ppermute(block, axis, [(i, i ^ flip) for i in range(count)]) for flip in range(1, count)
    ]


def in_order(pieces, axis):
    me = lax.axis_index(axis)
    stacked = jnp.stack(pieces)
    return [
        lax.dynamic_index_in_dim(stacked, me ^ place, 0, False) for place in range(len(pieces))
    ]


def local(
    inputs,
    input_norm_gain,
    receptance_weight,
    linear_key_weight,
    linear_value_weight,
    window_query_weight,
    window_key_weight,
    window_value_weight,
    decay_down_weight,
    decay_up_weight,
    decay_offset,
    decay_log_extra,
    erasure_down_weight,
    erasure_up_weight,
    erasure_offset,
    initial_state,
    head_norm_gain,
    query_sink_logit,
    linear_output_weight,
    window_output_weight,
):
    tokens = inputs.shape[1]
    tp_index = lax.axis_index("tp")
    length = tokens * lax.axis_size("sp")
    offset = lax.axis_index("sp") * tokens
    gathered = lax.all_gather(inputs, "tp", axis=2, tiled=True)[0]
    widened = gathered.astype(jnp.float32)
    hidden = to_bf16(
        widened
        * lax.rsqrt(jnp.mean(widened * widened, axis=-1, keepdims=True) + NORM_EPS)
        * input_norm_gain
    )
    weights = (
        receptance_weight,
        linear_key_weight,
        linear_value_weight,
        window_query_weight,
        window_key_weight,
        window_value_weight,
    )
    widths = [weight.shape[1] for weight in weights]
    joined = jnp.concatenate(weights, axis=1)
    regrouped = lax.all_to_all(joined, "fs", split_axis=1, concat_axis=0, tiled=True)
    every_seq = jnp.concatenate(swapped(hidden, "fs"), axis=0)
    near_cols = jnp.concatenate(in_order(swapped(window_output_weight, "fs"), "fs"), axis=1)
    whole_cols = lax.all_gather(regrouped, "sp", axis=0, tiled=True)
    partial_cols = jnp.dot(every_seq, whole_cols, preferred_element_type=jnp.float32)
    by_seq = to_bf16(partial_cols).reshape(-1, tokens, partial_cols.shape[1])
    outgoing = jnp.concatenate(in_order(list(by_seq), "fs"), axis=0)
    returned = lax.all_to_all(outgoing, "fs", split_axis=0, concat_axis=1, tiled=True)
    bounds = [0]
    for col_width in widths:
        bounds.append(bounds[-1] + col_width)
    projected = [returned[:, bounds[role_idx] : bounds[role_idx + 1]] for role_idx in range(6)]
    recept, lin_keys, lin_values, queries, att_keys, att_values = projected
    head_width = recept.shape[1]
    head_count = head_width // HD
    first_col = tp_index * head_width
    up_decay = lax.dynamic_slice_in_dim(decay_up_weight, first_col, head_width, 2)
    up_learn = lax.dynamic_slice_in_dim(erasure_up_weight, first_col, head_width, 2)
    base_decay = lax.dynamic_slice_in_dim(decay_offset, first_col, head_width, 1)
    base_learn = lax.dynamic_slice_in_dim(erasure_offset, first_col, head_width, 1)
    gain_local = lax.dynamic_slice_in_dim(head_norm_gain, first_col, head_width, 0)
    state_local = lax.dynamic_slice_in_dim(initial_state, tp_index * head_count, head_count, 1)
    spread = (
        jnp.arange(head_count)[:, None] == jnp.arange(head_width)[None, :] // HD
    ).astype(jnp.float32)
    decay_spikes = jnp.einsum("ht,hc->tc", decay_log_extra[0], spread, precision=HIGHEST)
    decay_low = to_bf16(jnp.dot(hidden, decay_down_weight, preferred_element_type=jnp.float32))
    decay_act = to_bf16(jnp.tanh(decay_low.astype(jnp.float32)))
    learn_low = to_bf16(jnp.dot(hidden, erasure_down_weight, preferred_element_type=jnp.float32))
    pre_decay = base_decay[:, None, :] + jnp.einsum(
        "tl,dlc->dtc", decay_act, up_decay, preferred_element_type=jnp.float32
    )
    log_decay = decay_spikes[None] - jnp.exp(-jax.nn.softplus(-pre_decay) - 0.5)
    learn = jax.nn.sigmoid(
        base_learn[:, None, :]
        + jnp.einsum("tl,dlc->dtc", learn_low, up_learn, preferred_element_type=jnp.float32)
    )
    local_out, ends = chunked(returned, log_decay, learn, head_width)
    entry = entering_states(
        ends.reshape(2, head_count, HD, PAIR), jnp.swapaxes(state_local, -1, -2)
    )
    lin_mix = merged(local_out, entry, gain_local)
    positions = offset + jnp.arange(tokens, dtype=jnp.int32)
    query_count = queries.shape[1] // HD
    group_count = att_keys.shape[1] // HD
    group_size = query_count // group_count
    roped_q = rope_axial(
        queries.astype(jnp.float32).reshape(tokens, query_count, HD), positions
    ).astype(jnp.bfloat16)
    roped_k = rope_axial(
        att_keys.astype(jnp.float32).reshape(tokens, group_count, HD), positions
    ).astype(jnp.bfloat16)
    kv_width = group_count * HD
    packed = jnp.concatenate([roped_k.reshape(tokens, kv_width), att_values], axis=1)
    bordered = padded(packed, (("sp", 0),), WINDOW)
    sink_local = lax.dynamic_slice_in_dim(
        query_sink_logit, tp_index * query_count, query_count, 0
    ).reshape(group_count, group_size)[:, :, None, None]
    reach = ATT_BLOCK + 2 * WINDOW
    query_rows = roped_q.reshape(ATT_BLOCK, group_count, group_size, HD)
    key_rows = bordered[:, :kv_width].reshape(reach, group_count, HD)
    value_rows = bordered[:, kv_width:].reshape(reach, group_count, HD)
    scores = jnp.einsum(
        "qgrd,kgd->grqk", query_rows, key_rows, preferred_element_type=jnp.float32
    ) * HD ** (-0.5)
    query_pos = offset + 0 + jnp.arange(ATT_BLOCK, dtype=jnp.int32)
    key_pos = offset + 0 - WINDOW + jnp.arange(reach, dtype=jnp.int32)
    allowed = (
        (jnp.abs(query_pos[:, None] - key_pos[None, :]) <= WINDOW)
        & (key_pos[None, :] >= 0)
        & (key_pos[None, :] < length)
    )
    scores = jnp.where(allowed, scores, -jnp.inf)
    top_score = jnp.maximum(jnp.max(scores, axis=-1, keepdims=True), sink_local)
    raised = jnp.exp(scores - top_score)
    denominator = jnp.exp(sink_local - top_score) + jnp.sum(raised, axis=-1, keepdims=True)
    weights_bf = (raised / denominator).astype(jnp.bfloat16)
    mixed = jnp.einsum("grqk,kgd->qgrd", weights_bf, value_rows, preferred_element_type=jnp.float32)
    outputs = mixed.astype(jnp.bfloat16).reshape(ATT_BLOCK, query_count * HD)
    lin_weight = lax.all_gather(linear_output_weight, ("sp", "fs"), axis=1, tiled=True)
    if lax.axis_size("sp") > 8:
        att_out = jnp.dot(
            outputs,
            lax.all_gather(near_cols, "sp", axis=1, tiled=True),
            preferred_element_type=jnp.float32,
        )
    else:
        att_parts = [
            jnp.dot(outputs, part, preferred_element_type=jnp.float32)
            for part in swapped(near_cols, "sp")
        ]
        att_out = jnp.concatenate(in_order(att_parts, "sp"), axis=1)
    layer_out = lax.psum_scatter(
        jnp.dot(lin_mix, lin_weight, preferred_element_type=jnp.float32) + att_out,
        "tp",
        scatter_dimension=0,
        tiled=True,
    )
    return layer_out.astype(jnp.bfloat16)[None]


SPAN = HD
BATCH = 4
VMEM_GRANT = 67_000_000
QUAD = 4 * HD
TN = (((0,), (0,)), ((), ()))


def mm(left, right, dims=NN):
    return lax.dot_general(left, right, dims, preferred_element_type=F32)


def rope_tables(total):
    quarter = HD // 4
    inverse = ROPE_BASE ** (-np.arange(quarter, dtype=np.float32) / np.float32(quarter))
    inverse = inverse.astype(np.float32)
    lane = np.arange(PAIR) % HD
    rates = inverse[lane % quarter]
    sign = np.where(lane % (2 * quarter) < quarter, -1.0, 1.0)
    coords = np.concatenate([np.arange(total // GRID_W), np.arange(GRID_W)])
    angles = (coords.astype(np.float32)[:, None] * rates[None, :]).astype(np.float64)
    return np.stack([np.cos(angles), np.sin(angles) * sign]).astype(np.float32)


def mix_body(
    hook, proj_ref, log_ref, learn_ref, table_ref, gain, sinks, states, mix_ref, s_w, s_read, s_m, s_a, s_local, s_re, s_lin, kpad, vpad, s_q
):
    total = proj_ref.shape[0]
    count = total // SPAN
    lane = lax.broadcasted_iota(jnp.int32, (SPAN, PAIR), 1)
    first = lane < HD
    ones = (
        jnp.where(first, 1.0, 0.0).astype(BF16),
        jnp.where(first, 0.0, 1.0).astype(BF16),
    )
    nothing = jnp.zeros((SPAN, PAIR), BF16)
    quad_row = lax.broadcasted_iota(jnp.int32, (SPAN, QUAD), 0)
    quad_lane = lax.broadcasted_iota(jnp.int32, (SPAN, QUAD), 1)
    quad_col = lax.rem(quad_lane, HD)
    ahead = quad_lane < PAIR
    before = jnp.where(ahead, quad_col - quad_row, quad_row - quad_col)
    strict, upto = before < 0, before <= 0
    eye = jnp.where(before == 0, 1.0, 0.0)

    def level(size):
        return (lax.div(quad_row, 2 * size) == lax.div(quad_col, 2 * size)) & (
            lax.div(quad_row, size) != lax.div(quad_col, size)
        )

    square_i = lax.broadcasted_iota(jnp.int32, (QUAD, QUAD), 0)
    square_j = lax.broadcasted_iota(jnp.int32, (QUAD, QUAD), 1)
    same_unit = lax.div(square_i, HD) == lax.div(square_j, HD)
    square_eye = square_i == square_j
    tri_i = lax.broadcasted_iota(jnp.int32, (SPAN, SPAN), 0)
    tri_j = lax.broadcasted_iota(jnp.int32, (SPAN, SPAN), 1)
    tri = [
        jnp.where(tri_j <= tri_i, 1.0, 0.0).astype(BF16),
        jnp.where(tri_j >= tri_i, 1.0, 0.0).astype(BF16),
    ]
    tri = [jnp.concatenate([one] * 3, axis=1) for one in tri]

    def diagonal(quad):
        left, right = quad[:, :PAIR], quad[:, PAIR:]
        return jnp.concatenate(
            [jnp.concatenate([left * one, nothing], axis=1) for one in ones]
            + [jnp.concatenate([nothing, right * one], axis=1) for one in ones],
            axis=0,
        )

    def quad_dot(lefts, right, dims=NN):
        highs, lows = zip(*[halves(left) for left in lefts])
        right_high, right_low = halves(right)
        count_left = len(lefts)
        outer = mm(jnp.concatenate(highs + lows, axis=0), diagonal(right_high), dims)
        inner = mm(jnp.concatenate(highs, axis=0), diagonal(right_low), dims)
        return [
            outer[k * SPAN : (k + 1) * SPAN]
            + (
                outer[(count_left + k) * SPAN : (count_left + k + 1) * SPAN]
                + inner[k * SPAN : (k + 1) * SPAN]
            )
            for k in range(count_left)
        ]

    def single(left, right):
        return mm(left.astype(BF16), diagonal(right.astype(BF16)))

    def rows_at(place):
        return pl.ds(pl.multiple_of(place * SPAN, SPAN), SPAN)

    def head_sum(value):
        low = jnp.sum(jnp.where(first, value, 0.0), axis=1, keepdims=True)
        high = jnp.sum(jnp.where(first, 0.0, value), axis=1, keepdims=True)
        return jnp.where(first, low, high)

    def prepare(direction, rows):
        read = proj_ref[rows, :PAIR].astype(F32)
        key = proj_ref[rows, PAIR : 2 * PAIR].astype(F32)
        log_decay = log_ref[direction, rows, :]
        unit = key * lax.rsqrt(head_sum(key * key) + NORM_EPS)
        erase = unit * learn_ref[direction, rows, :]
        high = log_decay.astype(BF16)
        rest = log_decay - high.astype(F32)
        middle_part = rest.astype(BF16)
        low = (rest - middle_part.astype(F32)).astype(BF16)
        total_log = mm(tri[direction], jnp.concatenate([high, middle_part, low], axis=0))
        end = SPAN - 1 if direction == 0 else 0
        span_log = total_log[end : end + 1, :]
        middle = 0.5 * span_log
        prior_log = total_log - log_decay
        inverse = jnp.exp(middle - total_log)
        left = jnp.exp(span_log - total_log)
        readers = jnp.concatenate(
            [jnp.exp(prior_log - middle) * unit, jnp.exp(total_log - middle) * read], axis=0
        )
        sources = jnp.concatenate([erase * inverse, key * inverse], axis=0)
        high_r, low_r = halves(readers)
        high_s, low_s = halves(sources)

        def spread(value):
            top, bottom = value[:SPAN], value[SPAN:]
            return jnp.concatenate([top * one for one in ones] + [bottom * one for one in ones], axis=0)

        high_s, low_s = spread(high_s), spread(low_s)
        meets = mm(
            jnp.concatenate([high_r, low_r, high_r], axis=1),
            jnp.concatenate([high_s, high_s, low_s], axis=1),
            NT,
        )
        return (
            meets,
            jnp.exp(prior_log) * unit,
            jnp.exp(total_log) * read,
            key * left,
            erase * left,
            jnp.exp(span_log),
        )

    def both(one, other):
        return jnp.concatenate([one, other], axis=1)

    def batch(index, carry, size):
        groups = [index * size + k for k in range(size)]
        erased, seens, read_eraseds, starts, lefts, finals, spans, values = [], [], [], [], [], [], [], []
        for group in groups:
            rows = (rows_at(group), rows_at(count - 1 - group))
            parts = [prepare(direction, rows[direction]) for direction in range(2)]
            meets = [part[0] for part in parts]
            value = both(*[proj_ref[row, 2 * PAIR : 3 * PAIR] for row in rows])
            erased.append(
                jnp.where(strict, both(meets[0][:SPAN, :PAIR], meets[1][:SPAN, :PAIR]), 0.0)
            )
            seen = jnp.where(strict, both(meets[0][:SPAN, PAIR:], meets[1][:SPAN, PAIR:]), 0.0)
            s_re[group] = jnp.where(
                upto, both(meets[0][SPAN:, :PAIR], meets[1][SPAN:, :PAIR]), 0.0
            )
            read_seen = jnp.where(upto, both(meets[0][SPAN:, PAIR:], meets[1][SPAN:, PAIR:]), 0.0)
            starts.append(both(parts[0][1], parts[1][1]))
            s_read[group] = both(parts[0][2], parts[1][2])
            lefts.append((both(parts[0][3], parts[1][3]), both(parts[0][4], parts[1][4])))
            spans.append(both(parts[0][5], parts[1][5]))
            values.append(value)
            pieces = jnp.concatenate([*halves(seen), *halves(read_seen)], axis=0)
            met = mm(pieces, diagonal(value))
            seens.append(met[:SPAN] + met[SPAN : 2 * SPAN])
            s_local[group] = met[2 * SPAN : 3 * SPAN] + met[3 * SPAN :]
        solves = [eye - jnp.where(level(1), one, 0.0) for one in erased]
        width = 2
        while width < SPAN:
            at = level(width)
            firsts = [single(solve, jnp.where(at, one, 0.0)) for solve, one in zip(solves, erased)]
            solves = [solve - single(one, solve) for solve, one in zip(solves, firsts)]
            width *= 2
        misses = [
            eye - solve - quad_dot([one], solve)[0] for solve, one in zip(solves, erased)
        ]
        solves = [solve + single(solve, miss) for solve, miss in zip(solves, misses)]
        maps = [quad_dot([solve], start)[0] for solve, start in zip(solves, starts)]
        shifts = [quad_dot([solve], seen)[0] for solve, seen in zip(solves, seens)]
        for place, group in enumerate(groups):
            key_left, erase_left = lefts[place]
            s_w[group] = jnp.concatenate([maps[place], shifts[place]], axis=1)
            map_high, map_low = halves(maps[place])
            left_high, left_low = halves(erase_left)
            fade = mm(
                jnp.concatenate([map_high, map_low, map_high], axis=0),
                jnp.concatenate([left_high, left_high, left_low], axis=0),
                TN,
            )
            s_m[group] = jnp.where(square_eye, spans[place], 0.0) - jnp.where(same_unit, fade, 0.0)
            shift_high, shift_low = halves(shifts[place])
            key_high, key_low = halves(key_left)
            gained = mm(
                jnp.concatenate(
                    [values[place], values[place], shift_high, shift_low, shift_high], axis=0
                ),
                jnp.concatenate(
                    [key_high, key_low, -left_high, -left_high, -left_low], axis=0
                ),
                TN,
            )
            gained = jnp.where(same_unit, gained, 0.0)
            s_a[group] = (gained[:SPAN] + gained[SPAN : 2 * SPAN]) + (
                gained[2 * SPAN : 3 * SPAN] + gained[3 * SPAN :]
            )
        return carry

    size = min(BATCH, count)
    for index in range(count // size):
        batch(index, 0, size)
        hook()

    def advance(group, state):
        high, low = halves(state)
        step_high, step_low = halves(s_m[group])
        outer = mm(jnp.concatenate([high, low], axis=0), step_high)
        inner = mm(high, step_low)
        following = outer[:SPAN] + (outer[SPAN:] + inner) + s_a[group]
        s_a[group] = state
        return following

    state = states
    for group in range(count):
        state = advance(group, state)
    hook()

    def finish(group, carry):
        maps, shift = s_w[group, :, :QUAD], s_w[group, :, QUAD:]
        dropped, seen_state = quad_dot([maps, s_read[group]], s_a[group], NT)
        dropped = dropped + shift
        out = seen_state + s_local[group] - quad_dot([s_re[group]], dropped)[0]
        s_lin[0, rows_at(group), :] = out[:, :PAIR]
        s_lin[1, rows_at(count - 1 - group), :] = out[:, PAIR:]
        return carry

    def finish_batch(index, carry):
        for k in range(size):
            carry = finish(index * size + k, carry)
        return carry

    lax.fori_loop(0, count // size, finish_batch, 0)
    hook()

    quarter = HD // 4
    back = lax.rem(lane, 2 * quarter) >= quarter
    by_row = lax.rem(lane, HD) < 2 * quarter
    grid = total // GRID_W
    edge = jnp.zeros((WINDOW, PAIR), BF16)
    for ref in (kpad, vpad):
        ref[:WINDOW, :] = edge
        ref[WINDOW + total :, :] = edge

    def turned(value, cosine, sine):
        partner = jnp.where(
            back, pltpu.roll(value, quarter, 1), pltpu.roll(value, PAIR - quarter, 1)
        )
        return value * cosine + partner * sine

    def turn(place, carry):
        rows = rows_at(place)
        cosine, sine = [
            jnp.where(
                by_row,
                table_ref[which, pl.ds(place, 1), :],
                table_ref[which, grid : grid + GRID_W, :],
            )
            for which in range(2)
        ]
        query = proj_ref[rows, 3 * PAIR : 4 * PAIR].astype(F32)
        pair = proj_ref[rows, 4 * PAIR :].astype(F32)
        s_q[rows, :] = turned(query, cosine, sine).astype(BF16)
        key = jnp.where(first, turned(pair, cosine, sine), 0.0)
        value = jnp.where(first, 0.0, pair)
        there = pl.ds(pl.multiple_of(WINDOW + place * SPAN, SPAN), SPAN)
        kpad[there, :] = (key + pltpu.roll(key, HD, 1)).astype(BF16)
        vpad[there, :] = (value + pltpu.roll(value, HD, 1)).astype(BF16)
        return carry

    lax.fori_loop(0, grid, turn, 0)
    reach = ATT_BLOCK + 2 * WINDOW
    ahead_of = lax.broadcasted_iota(jnp.int32, (ATT_BLOCK, reach), 1) - (
        WINDOW + lax.broadcasted_iota(jnp.int32, (ATT_BLOCK, reach), 0)
    )
    near = jnp.abs(ahead_of) <= WINDOW
    key_at = lax.broadcasted_iota(jnp.int32, (ATT_BLOCK, reach), 1) - WINDOW
    mine = lax.broadcasted_iota(jnp.int32, (ATT_BLOCK, PAIR), 1) < HD

    def attend(place, carry):
        start = pl.multiple_of(place * ATT_BLOCK, ATT_BLOCK)
        rows = pl.ds(start, ATT_BLOCK)
        query = s_q[rows, :]
        keys = kpad[pl.ds(start, reach), :]
        held = vpad[pl.ds(start, reach), :]
        allowed = near & (key_at >= -start) & (key_at < total - start)
        mixed = []
        for head in range(2):
            own = jnp.where(mine if head == 0 else jnp.logical_not(mine), query.astype(F32), 0.0)
            scores = mm(own.astype(BF16), keys, NT) * HD ** (-0.5)
            scores = jnp.where(allowed, scores, -jnp.inf)
            top = jnp.maximum(jnp.max(scores, axis=1, keepdims=True), sinks[head])
            raised = jnp.exp(scores - top)
            bottom = jnp.exp(sinks[head] - top) + jnp.sum(raised, axis=1, keepdims=True)
            mixed.append(mm((raised / bottom).astype(BF16), held))
        mix_ref[rows, PAIR:] = jnp.where(mine, mixed[0], mixed[1]).astype(BF16)
        return carry

    lax.fori_loop(0, total // ATT_BLOCK, attend, 0)
    hook()

    def norm(place, carry):
        rows = rows_at(place)
        lin_sum = s_lin[0, rows, :] + s_lin[1, rows, :]
        centred = lin_sum - head_sum(lin_sum) * (1.0 / HD)
        spread = head_sum(centred * centred) * (1.0 / HD)
        mix_ref[rows, :PAIR] = (centred * lax.rsqrt(spread + GROUP_EPS) * gain).astype(BF16)
        return carry

    lax.fori_loop(0, count, norm, 0)


def mix_scratch(total):
    count = total // SPAN
    return [
        pltpu.VMEM((count, SPAN, 2 * QUAD), F32),
        pltpu.VMEM((count, SPAN, QUAD), F32),
        pltpu.VMEM((count, QUAD, QUAD), F32),
        pltpu.VMEM((count, SPAN, QUAD), F32),
        pltpu.VMEM((count, SPAN, QUAD), F32),
        pltpu.VMEM((count, SPAN, QUAD), F32),
        pltpu.VMEM((2, total, PAIR), F32),
        pltpu.VMEM((total + 2 * WINDOW, PAIR), BF16),
        pltpu.VMEM((total + 2 * WINDOW, PAIR), BF16),
        pltpu.VMEM((total, PAIR), BF16),
    ]


MESH_IDS = pl.DeviceIdType.MESH


def flipped(index, bits):
    result = index
    for bit in (1, 2):
        if bits & bit:
            result = result + bit - 2 * bit * lax.rem(lax.div(index, bit), 2)
    return result


def remote(src, dst, send, recv, device):
    return pltpu.make_async_remote_copy(
        src_ref=src,
        dst_ref=dst,
        send_sem=send,
        recv_sem=recv,
        device_id=device,
        device_id_type=MESH_IDS,
    )


def layer_kernel(
    x_ref,
    wr_ref,
    wk_ref,
    wv_ref,
    wq_ref,
    extra_ref,
    dup_ref,
    eup_ref,
    lin_ref,
    win_ref,
    init_ref,
    sink_ref,
    ak_ref,
    av_ref,
    gain_ref,
    ddown_ref,
    edown_ref,
    doff_ref,
    eoff_ref,
    table_ref,
    head_gain_ref,
    out_ref,
    xbuf,
    wbuf,
    kvbuf,
    ebuf,
    dup,
    eup,
    proj_ref,
    log_ref,
    learn_ref,
    owb,
    mbuf,
    mix_ref,
    init,
    local_sem,
    wlocal_sem,
    up_send,
    up_recv,
    dn_send,
    dn_recv,
    sib_send,
    sib_recv,
    wz_send,
    wz_recv,
    e_send,
    e_recv,
    p_send,
    p_recv,
    f_send,
    f_recv,
    oz_send,
    oz_recv,
    op_send,
    op_recv,
    of_send,
    of_recv,
    os_send,
    os_recv,
    m_send,
    m_recv,
    *scratch,
):
    sp, fs, tp = lax.axis_index("sp"), lax.axis_index("fs"), lax.axis_index("tp")
    depth, width, sides = [lax.axis_size(axis) for axis in ("sp", "fs", "tp")]
    tokens = x_ref.shape[1]
    rows = wr_ref.shape[0]
    out_rows, out_cols = lin_ref.shape
    share = out_ref.shape[1]
    sibling = {"tp": 1 - tp}
    plane = ({"fs": flipped(fs, 1)}, {"fs": flipped(fs, 2)})
    up_to, dn_to = {"sp": sp + 1}, {"sp": sp - 1}

    def rows_of(z, f):
        return pl.ds(pl.multiple_of((z * width + f) * rows, rows), rows)

    def cols_of(z, f, many=1):
        return pl.ds(pl.multiple_of((z * width + f) * out_cols, out_cols), many * out_cols)

    def pieces(z):
        low = pl.ds(pl.multiple_of(z * PAIR, PAIR), PAIR)
        return [ref.at[:, low] for ref in (wr_ref, wk_ref, wv_ref, wq_ref)]

    def lanes(place):
        return slice(place * PAIR, (place + 1) * PAIR)

    cols = pl.ds(pl.multiple_of((tp * depth + sp) * PAIR, PAIR), PAIR)
    head = (tp * depth + sp) * 2
    own_x = pltpu.make_async_copy(x_ref.at[0], xbuf.at[sp, tp], local_sem.at[0])
    own_w = [
        pltpu.make_async_copy(
            piece, wbuf.at[rows_of(sp, fs), lanes(place)], wlocal_sem.at[place]
        )
        for place, piece in enumerate(pieces(sp))
    ]
    own_o = [
        pltpu.make_async_copy(
            ref,
            owb.at[tp, pl.ds(place * out_rows, out_rows), cols_of(sp, fs)],
            local_sem.at[1 + place],
        )
        for place, ref in enumerate((lin_ref, win_ref))
    ]
    small = [
        pltpu.make_async_copy(extra_ref.at[0], ebuf.at[sp], local_sem.at[3]),
        pltpu.make_async_copy(dup_ref.at[:, :, cols], dup, local_sem.at[4]),
        pltpu.make_async_copy(eup_ref.at[:, :, cols], eup, local_sem.at[5]),
        pltpu.make_async_copy(init_ref.at[:, pl.ds(head, 2)], init, local_sem.at[6]),
    ]
    for copy in [own_x] + own_w + own_o + small:
        copy.start()
    low_lanes = lax.broadcasted_iota(jnp.int32, (rows, PAIR), 1) < HD
    near_key, near_value = ak_ref[...].astype(F32), av_ref[...].astype(F32)
    packs = (
        jnp.where(low_lanes, near_key, pltpu.roll(near_value, HD, 1)).astype(BF16),
        jnp.where(low_lanes, pltpu.roll(near_key, HD, 1), near_value).astype(BF16),
    )
    for place, pack in enumerate(packs):
        kvbuf[place] = pack
    wbuf[rows_of(sp, fs), lanes(4)] = jnp.where(sp >= 2, packs[1], packs[0])

    barrier = pltpu.get_barrier_semaphore()
    pairs = [(k, t) for k in range(depth) for t in range(sides) if k or t]
    peers = [{"sp": flipped(sp, k), "tp": tp + t - 2 * t * tp} for k, t in pairs] + [*plane]
    for peer in peers:
        pl.semaphore_signal(barrier, inc=1, device_id=peer, device_id_type=MESH_IDS)
    pl.semaphore_wait(barrier, len(peers))

    def x_move(src_z, send, recv, device, src=None):
        there = xbuf.at[src_z, tp]
        return remote(there if src is None else src, there, send, recv, device)

    def wz_block(k):
        there = wbuf.at[rows_of(sp, fs)]
        return remote(there, there, wz_send.at[k - 1], wz_recv.at[k - 1], {"sp": flipped(sp, k)})

    def e_block(k):
        return remote(
            extra_ref.at[0],
            ebuf.at[sp],
            e_send.at[k - 1],
            e_recv.at[k - 1],
            {"sp": flipped(sp, k)},
        )

    def p_block(k, side):
        there = wbuf.at[rows_of(flipped(sp, k), fs)]
        return remote(there, there, p_send.at[k, side], p_recv.at[k, side], plane[side])

    def f_block(k):
        side = k % 2
        there = wbuf.at[rows_of(flipped(sp, k), flipped(fs, 2 if side == 0 else 1))]
        return remote(there, there, f_send.at[k], f_recv.at[k], plane[side])

    def oz_block(k):
        there = owb.at[tp, :, cols_of(sp, fs)]
        return remote(there, there, oz_send.at[k - 1], oz_recv.at[k - 1], {"sp": flipped(sp, k)})

    def op_block(k, side):
        there = owb.at[tp, :, cols_of(flipped(sp, k), fs)]
        return remote(there, there, op_send.at[k, side], op_recv.at[k, side], plane[side])

    def of_block(k):
        side = k % 2
        there = owb.at[tp, :, cols_of(flipped(sp, k), flipped(fs, 2 if side == 0 else 1))]
        return remote(there, there, of_send.at[k], of_recv.at[k], plane[side])

    def os_block(k):
        there = owb.at[tp, :, cols_of(flipped(sp, k), 0, width)]
        return remote(there, there, os_send.at[k], os_recv.at[k], sibling)

    def x_step(k):
        @pl.when(sp >= k)
        def _():
            x_move(sp, up_send.at[k - 1], up_recv.at[k - 1], up_to).wait_recv()
            if k < depth - 1:

                @pl.when(sp < depth - 1)
                def _():
                    x_move(sp - k, up_send.at[k], up_recv.at[k], up_to).start()

            x_move(sp - k, sib_send.at[k], sib_recv.at[k], sibling).start()

        @pl.when(sp < depth - k)
        def _():
            x_move(sp, dn_send.at[k - 1], dn_recv.at[k - 1], dn_to).wait_recv()
            if k < depth - 1:

                @pl.when(sp > 0)
                def _():
                    x_move(sp + k, dn_send.at[k], dn_recv.at[k], dn_to).start()

            place = depth + k - 1
            x_move(sp + k, sib_send.at[place], sib_recv.at[place], sibling).start()

    def w_step(k):
        if k:
            wz_block(k).wait_recv()
        for side in range(2):
            p_block(k, side).start()

    def f_step(k):
        for side in range(2):
            p_block(k, side).wait_recv()
        f_block(k).start()

    def oz_start():
        for k in range(1, depth):
            oz_block(k).start()

    def ow_step(k):
        if k:
            oz_block(k).wait_recv()
        for side in range(2):
            op_block(k, side).start()

    def of_step(k):
        for side in range(2):
            op_block(k, side).wait_recv()
        of_block(k).start()

    def os_step(k):
        of_block(k).wait_recv()
        os_block(k).start()

    @pl.when(sp < depth - 1)
    def _():
        x_move(sp, up_send.at[0], up_recv.at[0], up_to, x_ref.at[0]).start()

    @pl.when(sp > 0)
    def _():
        x_move(sp, dn_send.at[0], dn_recv.at[0], dn_to, x_ref.at[0]).start()

    for k in range(1, depth):
        target = flipped(sp, k)
        sources = pieces(target) + [kvbuf.at[lax.div(target, 2)]]
        for place, piece in enumerate(sources):
            remote(
                piece,
                wbuf.at[rows_of(sp, fs), lanes(place)],
                wz_send.at[k - 1],
                wz_recv.at[k - 1],
                {"sp": target},
            ).start()
        e_block(k).start()
    own_x.wait()
    x_move(sp, sib_send.at[0], sib_recv.at[0], sibling).start()
    for copy in own_w:
        copy.wait()

    w_step(0)
    f_step(0)
    x_step(1)
    for copy in own_o:
        copy.wait()
    ow_step(0)
    w_step(1)
    w_step(2)
    f_step(1)
    x_step(2)
    w_step(3)
    f_step(2)
    f_step(3)
    x_step(3)
    oz_start()
    for k in range(depth):
        f_block(k).wait_recv()
    for k in range(1, depth):
        e_block(k).wait_recv()
    x_move(sp, sib_send.at[0], sib_recv.at[0], sibling).wait_recv()
    for k in range(1, depth):

        @pl.when(sp >= k)
        def _():
            x_move(sp, sib_send.at[k], sib_recv.at[k], sibling).wait_recv()

        @pl.when(sp < depth - k)
        def _():
            place = depth + k - 1
            x_move(sp, sib_send.at[place], sib_recv.at[place], sibling).wait_recv()

    for copy in small:
        copy.wait()

    gain = gain_ref[...]
    half = gain.shape[1] // 2
    doff = doff_ref[:, cols]
    eoff = eoff_ref[:, cols]

    def block(z, carry):
        parts = [xbuf[z, side].astype(F32) for side in range(2)]
        total = sum(jnp.sum(part * part, axis=1, keepdims=True) for part in parts)
        scale = lax.rsqrt(total / (2 * half) + NORM_EPS)
        hidden = jnp.concatenate(
            [
                (part * scale * gain[:, side * half : (side + 1) * half]).astype(BF16)
                for side, part in enumerate(parts)
            ],
            axis=1,
        )
        where = pl.ds(pl.multiple_of(z * tokens, tokens), tokens)
        proj_ref[where, :] = mm(hidden, wbuf[...]).astype(BF16)
        decay_low = mm(hidden, ddown_ref[...], NT).astype(BF16)
        decay_act = jnp.tanh(decay_low.astype(F32)).astype(BF16)
        learn_low = mm(hidden, edown_ref[...], NT).astype(BF16)
        spikes = jnp.concatenate(
            [
                jnp.broadcast_to(ebuf[z, pl.ds(2 * sp + place, 1), :], (HD, tokens))
                for place in range(2)
            ],
            axis=0,
        ).T
        for direction in range(2):
            pre = doff[direction : direction + 1] + mm(decay_act, dup[direction])
            softplus = jnp.maximum(-pre, 0.0) + jnp.log1p(jnp.exp(-jnp.abs(pre)))
            log_ref[direction, where, :] = spikes - jnp.exp(-softplus - 0.5)
            learn = eoff[direction : direction + 1] + mm(learn_low, eup[direction])
            learn_ref[direction, where, :] = jax.nn.sigmoid(learn)
        return carry

    lax.fori_loop(0, depth, block, 0)

    plan = [
        [(of_step, 0), (ow_step, 1)],
        [(os_step, 0)],
        [(ow_step, 2)],
        [(of_step, 1)],
        [(ow_step, 3), (os_step, 1), (of_step, 2)],
    ]
    queue = iter(plan)

    def hook():
        for step, k in next(queue, ()):
            step(k)

    states = jnp.concatenate([init[d, h] for d in range(2) for h in range(2)], axis=1)
    mix_body(
        hook,
        proj_ref,
        log_ref,
        learn_ref,
        table_ref,
        head_gain_ref[:, cols],
        [sink_ref[0, head], sink_ref[0, head + 1]],
        states,
        mix_ref,
        *scratch,
    )

    def m_block(k, t):
        z, side = flipped(sp, k), tp + t - 2 * t * tp
        start = pl.multiple_of((z * sides + side) * share, share)
        return remote(
            mix_ref.at[pl.ds(start, share)],
            mbuf.at[sp * sides + tp],
            m_send.at[k * sides + t],
            m_recv.at[k * sides + t],
            {"sp": z, "tp": side},
        )

    for k, t in pairs:
        m_block(k, t).start()
    mine = sp * sides + tp
    mbuf[mine] = mix_ref[pl.ds(pl.multiple_of(mine * share, share), share), :]
    of_step(3)
    os_step(2)
    for k, t in pairs:
        m_block(k, t).wait_recv()
    lefts = [
        jnp.concatenate(
            [mbuf[z * sides + side, :, :PAIR] for z in range(depth)]
            + [mbuf[z * sides + side, :, PAIR:] for z in range(depth)],
            axis=1,
        )
        for side in range(sides)
    ]
    for k in range(depth):
        if k == depth - 1:
            os_step(k)
        os_block(k).wait_recv()
        span = cols_of(flipped(sp, k), 0, width)
        out_ref[0, :, span] = sum(
            mm(lefts[side], owb[side, :, span]) for side in range(sides)
        ).astype(BF16)

    @pl.when(sp < depth - 1)
    def _():
        x_move(sp, up_send.at[0], up_recv.at[0], up_to, x_ref.at[0]).wait_send()

    @pl.when(sp > 0)
    def _():
        x_move(sp, dn_send.at[0], dn_recv.at[0], dn_to, x_ref.at[0]).wait_send()

    x_move(sp, sib_send.at[0], sib_recv.at[0], sibling).wait_send()
    for k in range(1, depth):

        @pl.when(sp >= k)
        def _():
            x_move(sp, sib_send.at[k], sib_recv.at[k], sibling).wait_send()
            if k < depth - 1:

                @pl.when(sp < depth - 1)
                def _():
                    x_move(sp, up_send.at[k], up_recv.at[k], up_to).wait_send()

        @pl.when(sp < depth - k)
        def _():
            place = depth + k - 1
            x_move(sp, sib_send.at[place], sib_recv.at[place], sibling).wait_send()
            if k < depth - 1:

                @pl.when(sp > 0)
                def _():
                    x_move(sp, dn_send.at[k], dn_recv.at[k], dn_to).wait_send()

        wz_block(k).wait_send()
        e_block(k).wait_send()
        oz_block(k).wait_send()
    for k in range(depth):
        for side in range(2):
            p_block(k, side).wait_send()
            op_block(k, side).wait_send()
        f_block(k).wait_send()
        of_block(k).wait_send()
        os_block(k).wait_send()
    for k, t in pairs:
        m_block(k, t).wait_send()


def by_heads(
    inputs,
    input_norm_gain,
    receptance_weight,
    linear_key_weight,
    linear_value_weight,
    window_query_weight,
    window_key_weight,
    window_value_weight,
    decay_down_weight,
    decay_up_weight,
    decay_offset,
    decay_log_extra,
    erasure_down_weight,
    erasure_up_weight,
    erasure_offset,
    initial_state,
    head_norm_gain,
    query_sink_logit,
    linear_output_weight,
    window_output_weight,
):
    depth, width, sides = [lax.axis_size(axis) for axis in ("sp", "fs", "tp")]
    _, tokens, half = inputs.shape
    total = tokens * depth
    rows = receptance_weight.shape[0]
    out_rows, out_cols = linear_output_weight.shape
    features = out_cols * depth * width
    share = tokens // sides
    low = decay_down_weight.shape[1]
    dma = pltpu.SemaphoreType.DMA
    any_spec = pl.BlockSpec(memory_space=pl.ANY)
    vmem_spec = pl.BlockSpec(memory_space=pltpu.VMEM)
    return pl.pallas_call(
        layer_kernel,
        in_specs=[any_spec] * 11 + [pl.BlockSpec(memory_space=pltpu.SMEM)] + [vmem_spec] * 9,
        out_specs=vmem_spec,
        out_shape=jax.ShapeDtypeStruct((1, share, features), BF16),
        scratch_shapes=[
            pltpu.VMEM((depth, 2, tokens, half), BF16),
            pltpu.VMEM((2 * half, 5 * PAIR), BF16),
            pltpu.VMEM((2, rows, PAIR), BF16),
            pltpu.VMEM((depth, decay_log_extra.shape[1], tokens), F32),
            pltpu.VMEM((2, low, PAIR), BF16),
            pltpu.VMEM((2, low, PAIR), BF16),
            pltpu.VMEM((total, 5 * PAIR), BF16),
            pltpu.VMEM((2, total, PAIR), F32),
            pltpu.VMEM((2, total, PAIR), F32),
            pltpu.VMEM((sides, 2 * out_rows, features), BF16),
            pltpu.VMEM((depth * sides, share, 2 * PAIR), BF16),
            pltpu.VMEM((total, 2 * PAIR), BF16),
            pltpu.VMEM((2, 2, HD, HD), F32),
            dma((7,)),
            dma((4,)),
            dma((depth,)),
            dma((depth,)),
            dma((depth,)),
            dma((depth,)),
            dma((2 * depth,)),
            dma((2 * depth,)),
            dma((depth - 1,)),
            dma((depth - 1,)),
            dma((depth - 1,)),
            dma((depth - 1,)),
            dma((width, 2)),
            dma((width, 2)),
            dma((width,)),
            dma((width,)),
            dma((depth - 1,)),
            dma((depth - 1,)),
            dma((depth, 2)),
            dma((depth, 2)),
            dma((depth,)),
            dma((depth,)),
            dma((depth,)),
            dma((depth,)),
            dma((depth * sides,)),
            dma((depth * sides,)),
        ]
        + mix_scratch(total),
        compiler_params=pltpu.CompilerParams(
            collective_id=0, has_side_effects=True, vmem_limit_bytes=VMEM_GRANT
        ),
        name="layer",
    )(
        inputs,
        receptance_weight,
        linear_key_weight,
        linear_value_weight,
        window_query_weight,
        decay_log_extra,
        decay_up_weight,
        erasure_up_weight,
        linear_output_weight,
        window_output_weight,
        initial_state,
        query_sink_logit[None, :],
        window_key_weight,
        window_value_weight,
        input_norm_gain[None, :],
        decay_down_weight.T,
        erasure_down_weight.T,
        decay_offset,
        erasure_offset,
        jnp.asarray(rope_tables(total)),
        head_norm_gain[None, :],
    )


def layer(*arrays):
    inputs, recept, keys = arrays[0], arrays[2], arrays[6]
    depth, width, sides = [lax.axis_size(axis) for axis in ("sp", "fs", "tp")]
    fits = (
        recept.shape[1] == arrays[5].shape[1] == depth * PAIR
        and 2 * keys.shape[1] == depth * HD
        and (depth, width, sides) == (4, 4, 2)
        and inputs.shape[1] % WINDOW == 0
        and SPAN == GRID_W
    )
    return (by_heads if fits else local)(*arrays)


def solution(mesh):
    return jax.shard_map(
        layer,
        mesh=mesh,
        in_specs=(
            P("fs", "sp", "tp"),
            P(),
            P(("sp", "fs"), "tp"),
            P(("sp", "fs"), "tp"),
            P(("sp", "fs"), "tp"),
            P(("sp", "fs"), "tp"),
            P(("sp", "fs"), "tp"),
            P(("sp", "fs"), "tp"),
            P(),
            P(),
            P(),
            P("fs", "tp", "sp"),
            P(),
            P(),
            P(),
            P(),
            P(),
            P(),
            P("tp", ("sp", "fs")),
            P("tp", ("sp", "fs")),
        ),
        out_specs=P("fs", ("sp", "tp"), None),
        check_vma=False,
    )
```

```python
import jax
import jax.numpy as jnp
import numpy as np
from jax import lax
from jax.experimental import pallas as pl
from jax.experimental.pallas import tpu as pltpu
from jax.sharding import PartitionSpec as P

HD = 64
WINDOW = 128
GRID_W = 64
ATT_BLOCK = 128


NORM_EPS = 1e-06
GROUP_EPS = 0.00064
ROPE_BASE = 10000.0
HIGHEST = lax.Precision.HIGHEST


def padded(block, sides, width):
    for axis, dim in sides:
        count = lax.axis_size(axis)
        forward = [(i, i + 1) for i in range(count - 1)]
        backward = [(target, source) for source, target in forward]
        low = lax.ppermute(
            lax.slice_in_dim(block, block.shape[dim] - width, None, axis=dim), axis, forward
        )
        high = lax.ppermute(lax.slice_in_dim(block, 0, width, axis=dim), axis, backward)
        block = jnp.concatenate([low, block, high], axis=dim)
    return block


def to_bf16(array):
    return lax.optimization_barrier(array.astype(jnp.bfloat16))


def rope_axial(values, positions):
    quarter = values.shape[-1] // 4
    inverse = ROPE_BASE ** (-jnp.arange(quarter, dtype=jnp.float32) / quarter)
    grid_rows = (positions // GRID_W).astype(jnp.float32)
    grid_cols = (positions % GRID_W).astype(jnp.float32)
    pieces = []
    for which_half, coordinate in ((0, grid_rows), (1, grid_cols)):
        angles = coordinate[:, None] * inverse[None, :]
        cosine = jnp.cos(angles)[:, None, :]
        sine_part = jnp.sin(angles)[:, None, :]
        front_part = values[..., 2 * which_half * quarter : (2 * which_half + 1) * quarter]
        back_part = values[..., (2 * which_half + 1) * quarter : (2 * which_half + 2) * quarter]
        pieces.append(front_part * cosine - back_part * sine_part)
        pieces.append(front_part * sine_part + back_part * cosine)
    return jnp.concatenate(pieces, axis=-1)


CHUNK = 32
PAIR = 2 * HD
F32 = jnp.float32
BF16 = jnp.bfloat16
NN = (((1,), (0,)), ((), ()))
NT = (((1,), (1,)), ((), ()))


def dot1(left, right, dims=NN):
    return lax.dot_general(
        left.astype(jnp.bfloat16), right.astype(jnp.bfloat16), dims, preferred_element_type=F32
    )


def halves(value):
    high = value.astype(jnp.bfloat16)
    return high, (value - high.astype(F32)).astype(jnp.bfloat16)


def dot3(left, right, dims=NN):
    left_high, left_low = halves(left)
    right_high, right_low = halves(right)

    def product(one, other):
        return lax.dot_general(one, other, dims, preferred_element_type=F32)

    return product(left_high, right_high) + (
        product(left_high, right_low) + product(left_low, right_high)
    )


def full_dot(left, right):
    return lax.dot_general(left, right, NN, precision=HIGHEST, preferred_element_type=F32)


def chunk_kernel(read_ref, key_ref, value_ref, log_ref, learn_ref, out_ref, end_ref):
    tokens = read_ref.shape[0]
    read = read_ref[...].astype(F32)
    key = key_ref[...].astype(F32)
    value = value_ref[...].astype(F32)
    first = lax.broadcasted_iota(jnp.int32, (tokens, PAIR), 1) < HD
    pair_i = lax.broadcasted_iota(jnp.int32, (PAIR, PAIR), 0)
    pair_j = lax.broadcasted_iota(jnp.int32, (PAIR, PAIR), 1)
    same_head = jnp.where(pair_i // HD == pair_j // HD, 1.0, 0.0)
    row = lax.broadcasted_iota(jnp.int32, (tokens, tokens), 0)
    col = lax.broadcasted_iota(jnp.int32, (tokens, tokens), 1)
    same_chunk = row // CHUNK == col // CHUNK
    eye = jnp.where(row == col, 1.0, 0.0)
    unit = key * lax.rsqrt(full_dot(key * key, same_head) + NORM_EPS)
    own = (first, jnp.logical_not(first))
    values = (
        jnp.where(first, value, 0.0),
        jnp.where(first, pltpu.roll(value, HD, 1), 0.0),
    )
    all_chunk = jnp.where(same_chunk, 1.0, 0.0)
    for direction in range(2):
        before = (col < row) if direction == 0 else (col > row)
        strict = same_chunk & before
        upto = same_chunk & (before | (col == row))
        log_decay = log_ref[direction]
        erase = unit * learn_ref[direction]
        total_log = full_dot(jnp.where(upto, 1.0, 0.0), log_decay)
        chunk_log = full_dot(all_chunk, log_decay)
        prior_log = total_log - log_decay
        middle = 0.5 * chunk_log
        unit_start = jnp.exp(prior_log) * unit
        unit_mid = jnp.exp(prior_log - middle) * unit
        read_start = jnp.exp(total_log) * read
        read_mid = jnp.exp(total_log - middle) * read
        inverse = jnp.exp(middle - total_log)
        sources = jnp.concatenate([erase * inverse, key * inverse], axis=0)
        rest = jnp.exp(chunk_log - total_log)
        key_rest = key * rest
        erase_rest = erase * rest
        chunk_decay = jnp.exp(chunk_log).T
        solved, offsets, mixes = [], [], []
        for head in range(2):
            readers = jnp.concatenate(
                [jnp.where(own[head], unit_mid, 0.0), jnp.where(own[head], read_mid, 0.0)], axis=0
            )
            meets = dot3(readers, sources, NT)
            erased = jnp.where(strict, meets[:tokens, :tokens], 0.0)
            seen = jnp.where(strict, meets[:tokens, tokens:], 0.0)
            read_erased = jnp.where(upto, meets[tokens:, :tokens], 0.0)
            read_seen = jnp.where(upto, meets[tokens:, tokens:], 0.0)
            solve = eye - jnp.where(row // 2 == col // 2, erased, 0.0)
            size = 2
            while size < CHUNK:
                level = (row // (2 * size) == col // (2 * size)) & (row // size != col // size)
                solve = solve - dot1(dot1(solve, jnp.where(level, erased, 0.0)), solve)
                size *= 2
            solve = solve + dot1(solve, eye - solve - dot3(erased, solve))
            both = dot3(
                solve,
                jnp.concatenate(
                    [jnp.where(own[head], unit_start, 0.0), dot3(seen, values[head])], axis=1
                ),
            )
            solved.append(both[:, :PAIR])
            offsets.append(both[:, PAIR:])
            mixes.append(jnp.concatenate([read_seen, -read_erased], axis=1))
        state = jnp.where(pair_j == HD + pair_i % HD, 1.0, 0.0)
        count = tokens // CHUNK
        drops = [[None] * count, [None] * count]
        reads = [[None] * count, [None] * count]
        for step in range(count):
            place = step if direction == 0 else count - 1 - step
            rows = slice(place * CHUNK, (place + 1) * CHUNK)
            lefts = jnp.concatenate(
                [solved[0][rows], solved[1][rows]]
                + [jnp.where(own[head], read_start, 0.0)[rows] for head in range(2)],
                axis=0,
            )
            seen_state = dot3(lefts, state)
            for head in range(2):
                drops[head][place] = (
                    seen_state[head * CHUNK : (head + 1) * CHUNK] + offsets[head][rows]
                )
                reads[head][place] = seen_state[(2 + head) * CHUNK : (3 + head) * CHUNK]
            adders = jnp.concatenate(
                [jnp.where(own[head], key_rest, 0.0)[rows] for head in range(2)]
                + [jnp.where(own[head], -erase_rest, 0.0)[rows] for head in range(2)],
                axis=0,
            ).T
            added = jnp.concatenate(
                [values[0][rows], values[1][rows], drops[0][place], drops[1][place]], axis=0
            )
            first_col = place * CHUNK
            state = chunk_decay[:, first_col : first_col + 1] * state + dot3(adders, added)
        for head in range(2):
            dropped = jnp.concatenate(drops[head], axis=0)
            out_ref[direction, head] = jnp.concatenate(reads[head], axis=0) + dot3(
                mixes[head], jnp.concatenate([values[head], dropped], axis=0)
            )
        end_ref[direction] = state


def chunked(returned, log_decay, learn, head_width):
    tokens = returned.shape[0]
    pairs = head_width // PAIR

    def role(which):
        return pl.BlockSpec((tokens, PAIR), lambda p: (0, which * pairs + p))

    wide = pl.BlockSpec((2, tokens, PAIR), lambda p: (0, 0, p))
    return pl.pallas_call(
        chunk_kernel,
        grid=(pairs,),
        in_specs=[role(0), role(1), role(2), wide, wide],
        out_specs=[
            pl.BlockSpec((2, 2, tokens, PAIR), lambda p: (0, p, 0, 0)),
            pl.BlockSpec((2, PAIR, PAIR), lambda p: (0, p, 0)),
        ],
        out_shape=[
            jax.ShapeDtypeStruct((2, 2 * pairs, tokens, PAIR), F32),
            jax.ShapeDtypeStruct((2, pairs * PAIR, PAIR), F32),
        ],
        cost_estimate=pl.CostEstimate(
            flops=pairs * 400 * PAIR**3, bytes_accessed=8 * tokens * head_width * 4, transcendentals=0
        ),
        name="chunked_state",
    )(returned, returned, returned, log_decay, learn)


def merge_kernel(local_ref, state_ref, gain_ref, out_ref):
    pair_i = lax.broadcasted_iota(jnp.int32, (PAIR, PAIR), 0)
    pair_j = lax.broadcasted_iota(jnp.int32, (PAIR, PAIR), 1)
    average = jnp.where(pair_i // HD == pair_j // HD, 1.0 / HD, 0.0)
    sums = []
    for head in range(2):
        total = 0.0
        for direction in range(2):
            block = local_ref[direction, head]
            total = total + (
                block[:, :HD] + dot3(block[:, HD:], state_ref[direction, head])
            )
        sums.append(total)
    lin_sum = jnp.concatenate(sums, axis=1)
    centred = lin_sum - full_dot(lin_sum, average)
    normed = centred * lax.rsqrt(full_dot(centred * centred, average) + GROUP_EPS)
    out_ref[...] = (normed * gain_ref[...]).astype(jnp.bfloat16)


def merged(local_out, entry, gain):
    _, head_count, tokens, _ = local_out.shape
    pairs = head_count // 2
    return pl.pallas_call(
        merge_kernel,
        grid=(pairs,),
        in_specs=[
            pl.BlockSpec((2, 2, tokens, PAIR), lambda p: (0, p, 0, 0)),
            pl.BlockSpec((2, 2, HD, HD), lambda p: (0, p, 0, 0)),
            pl.BlockSpec((1, PAIR), lambda p: (0, p)),
        ],
        out_specs=pl.BlockSpec((tokens, PAIR), lambda p: (0, p)),
        out_shape=jax.ShapeDtypeStruct((tokens, head_count * HD), jnp.bfloat16),
        cost_estimate=pl.CostEstimate(
            flops=pairs * 30 * PAIR**3, bytes_accessed=4 * tokens * head_count * PAIR * 4, transcendentals=0
        ),
        name="merged_norm",
    )(local_out, entry, gain[None, :])


def entering_states(ends, initial):
    count = lax.axis_size("sp")
    place = lax.axis_index("sp")
    ups = [(i, i + 1) for i in range(count - 1)]
    downs = [(i + 1, i) for i in range(count - 1)]
    adds, maps = ends[..., :HD], ends[..., HD:]

    def hop(_, states):
        later = jnp.einsum("dhkj,dhjv->dhkv", maps, states, precision=HIGHEST) + adds
        forward = lax.ppermute(later[0], "sp", ups)
        backward = lax.ppermute(later[1], "sp", downs)
        return jnp.stack(
            [
                jnp.where(place == 0, initial[0], forward),
                jnp.where(place == count - 1, initial[1], backward),
            ]
        )

    states = initial
    if count > 8:
        return lax.fori_loop(0, count - 1, hop, states)
    for _ in range(count - 1):
        states = hop(0, states)
    return states


def swapped(block, axis):
    count = lax.axis_size(axis)
    return [block] + [
        lax.ppermute(block, axis, [(i, i ^ flip) for i in range(count)]) for flip in range(1, count)
    ]


def in_order(pieces, axis):
    me = lax.axis_index(axis)
    stacked = jnp.stack(pieces)
    return [
        lax.dynamic_index_in_dim(stacked, me ^ place, 0, False) for place in range(len(pieces))
    ]


def local(
    inputs,
    input_norm_gain,
    receptance_weight,
    linear_key_weight,
    linear_value_weight,
    window_query_weight,
    window_key_weight,
    window_value_weight,
    decay_down_weight,
    decay_up_weight,
    decay_offset,
    decay_log_extra,
    erasure_down_weight,
    erasure_up_weight,
    erasure_offset,
    initial_state,
    head_norm_gain,
    query_sink_logit,
    linear_output_weight,
    window_output_weight,
):
    tokens = inputs.shape[1]
    tp_index = lax.axis_index("tp")
    length = tokens * lax.axis_size("sp")
    offset = lax.axis_index("sp") * tokens
    gathered = lax.all_gather(inputs, "tp", axis=2, tiled=True)[0]
    widened = gathered.astype(jnp.float32)
    hidden = to_bf16(
        widened
        * lax.rsqrt(jnp.mean(widened * widened, axis=-1, keepdims=True) + NORM_EPS)
        * input_norm_gain
    )
    weights = (
        receptance_weight,
        linear_key_weight,
        linear_value_weight,
        window_query_weight,
        window_key_weight,
        window_value_weight,
    )
    widths = [weight.shape[1] for weight in weights]
    joined = jnp.concatenate(weights, axis=1)
    regrouped = lax.all_to_all(joined, "fs", split_axis=1, concat_axis=0, tiled=True)
    every_seq = jnp.concatenate(swapped(hidden, "fs"), axis=0)
    near_cols = jnp.concatenate(in_order(swapped(window_output_weight, "fs"), "fs"), axis=1)
    whole_cols = lax.all_gather(regrouped, "sp", axis=0, tiled=True)
    partial_cols = jnp.dot(every_seq, whole_cols, preferred_element_type=jnp.float32)
    by_seq = to_bf16(partial_cols).reshape(-1, tokens, partial_cols.shape[1])
    outgoing = jnp.concatenate(in_order(list(by_seq), "fs"), axis=0)
    returned = lax.all_to_all(outgoing, "fs", split_axis=0, concat_axis=1, tiled=True)
    bounds = [0]
    for col_width in widths:
        bounds.append(bounds[-1] + col_width)
    projected = [returned[:, bounds[role_idx] : bounds[role_idx + 1]] for role_idx in range(6)]
    recept, lin_keys, lin_values, queries, att_keys, att_values = projected
    head_width = recept.shape[1]
    head_count = head_width // HD
    first_col = tp_index * head_width
    up_decay = lax.dynamic_slice_in_dim(decay_up_weight, first_col, head_width, 2)
    up_learn = lax.dynamic_slice_in_dim(erasure_up_weight, first_col, head_width, 2)
    base_decay = lax.dynamic_slice_in_dim(decay_offset, first_col, head_width, 1)
    base_learn = lax.dynamic_slice_in_dim(erasure_offset, first_col, head_width, 1)
    gain_local = lax.dynamic_slice_in_dim(head_norm_gain, first_col, head_width, 0)
    state_local = lax.dynamic_slice_in_dim(initial_state, tp_index * head_count, head_count, 1)
    spread = (
        jnp.arange(head_count)[:, None] == jnp.arange(head_width)[None, :] // HD
    ).astype(jnp.float32)
    decay_spikes = jnp.einsum("ht,hc->tc", decay_log_extra[0], spread, precision=HIGHEST)
    decay_low = to_bf16(jnp.dot(hidden, decay_down_weight, preferred_element_type=jnp.float32))
    decay_act = to_bf16(jnp.tanh(decay_low.astype(jnp.float32)))
    learn_low = to_bf16(jnp.dot(hidden, erasure_down_weight, preferred_element_type=jnp.float32))
    pre_decay = base_decay[:, None, :] + jnp.einsum(
        "tl,dlc->dtc", decay_act, up_decay, preferred_element_type=jnp.float32
    )
    log_decay = decay_spikes[None] - jnp.exp(-jax.nn.softplus(-pre_decay) - 0.5)
    learn = jax.nn.sigmoid(
        base_learn[:, None, :]
        + jnp.einsum("tl,dlc->dtc", learn_low, up_learn, preferred_element_type=jnp.float32)
    )
    local_out, ends = chunked(returned, log_decay, learn, head_width)
    entry = entering_states(
        ends.reshape(2, head_count, HD, PAIR), jnp.swapaxes(state_local, -1, -2)
    )
    lin_mix = merged(local_out, entry, gain_local)
    positions = offset + jnp.arange(tokens, dtype=jnp.int32)
    query_count = queries.shape[1] // HD
    group_count = att_keys.shape[1] // HD
    group_size = query_count // group_count
    roped_q = rope_axial(
        queries.astype(jnp.float32).reshape(tokens, query_count, HD), positions
    ).astype(jnp.bfloat16)
    roped_k = rope_axial(
        att_keys.astype(jnp.float32).reshape(tokens, group_count, HD), positions
    ).astype(jnp.bfloat16)
    kv_width = group_count * HD
    packed = jnp.concatenate([roped_k.reshape(tokens, kv_width), att_values], axis=1)
    bordered = padded(packed, (("sp", 0),), WINDOW)
    sink_local = lax.dynamic_slice_in_dim(
        query_sink_logit, tp_index * query_count, query_count, 0
    ).reshape(group_count, group_size)[:, :, None, None]
    reach = ATT_BLOCK + 2 * WINDOW
    query_rows = roped_q.reshape(ATT_BLOCK, group_count, group_size, HD)
    key_rows = bordered[:, :kv_width].reshape(reach, group_count, HD)
    value_rows = bordered[:, kv_width:].reshape(reach, group_count, HD)
    scores = jnp.einsum(
        "qgrd,kgd->grqk", query_rows, key_rows, preferred_element_type=jnp.float32
    ) * HD ** (-0.5)
    query_pos = offset + 0 + jnp.arange(ATT_BLOCK, dtype=jnp.int32)
    key_pos = offset + 0 - WINDOW + jnp.arange(reach, dtype=jnp.int32)
    allowed = (
        (jnp.abs(query_pos[:, None] - key_pos[None, :]) <= WINDOW)
        & (key_pos[None, :] >= 0)
        & (key_pos[None, :] < length)
    )
    scores = jnp.where(allowed, scores, -jnp.inf)
    top_score = jnp.maximum(jnp.max(scores, axis=-1, keepdims=True), sink_local)
    raised = jnp.exp(scores - top_score)
    denominator = jnp.exp(sink_local - top_score) + jnp.sum(raised, axis=-1, keepdims=True)
    weights_bf = (raised / denominator).astype(jnp.bfloat16)
    mixed = jnp.einsum("grqk,kgd->qgrd", weights_bf, value_rows, preferred_element_type=jnp.float32)
    outputs = mixed.astype(jnp.bfloat16).reshape(ATT_BLOCK, query_count * HD)
    lin_weight = lax.all_gather(linear_output_weight, ("sp", "fs"), axis=1, tiled=True)
    if lax.axis_size("sp") > 8:
        att_out = jnp.dot(
            outputs,
            lax.all_gather(near_cols, "sp", axis=1, tiled=True),
            preferred_element_type=jnp.float32,
        )
    else:
        att_parts = [
            jnp.dot(outputs, part, preferred_element_type=jnp.float32)
            for part in swapped(near_cols, "sp")
        ]
        att_out = jnp.concatenate(in_order(att_parts, "sp"), axis=1)
    layer_out = lax.psum_scatter(
        jnp.dot(lin_mix, lin_weight, preferred_element_type=jnp.float32) + att_out,
        "tp",
        scatter_dimension=0,
        tiled=True,
    )
    return layer_out.astype(jnp.bfloat16)[None]


SPAN = HD
PARTS = 2
ORDER = (1, 3, 2)
VMEM_GRANT = 67_000_000
QUAD = 4 * HD
TN = (((0,), (0,)), ((), ()))


def mm(left, right, dims=NN):
    return lax.dot_general(left, right, dims, preferred_element_type=F32)


def rope_tables(total):
    quarter = HD // 4
    inverse = ROPE_BASE ** (-np.arange(quarter, dtype=np.float32) / np.float32(quarter))
    inverse = inverse.astype(np.float32)
    lane = np.arange(PAIR) % HD
    rates = inverse[lane % quarter]
    sign = np.where(lane % (2 * quarter) < quarter, -1.0, 1.0)
    coords = np.concatenate([np.arange(total // GRID_W), np.arange(GRID_W)])
    angles = (coords.astype(np.float32)[:, None] * rates[None, :]).astype(np.float64)
    return np.stack([np.cos(angles), np.sin(angles) * sign]).astype(np.float32)


def mix_body(
    hook, proj_ref, log_ref, learn_ref, table_ref, gain, sinks, states, mix_ref, s_w, s_read, s_m, s_a, s_local, s_re, s_lin, kpad, vpad, s_q
):
    total = proj_ref.shape[0]
    count = total // SPAN
    lane = lax.broadcasted_iota(jnp.int32, (SPAN, PAIR), 1)
    first = lane < HD
    ones = (
        jnp.where(first, 1.0, 0.0).astype(BF16),
        jnp.where(first, 0.0, 1.0).astype(BF16),
    )
    nothing = jnp.zeros((SPAN, PAIR), BF16)
    quad_row = lax.broadcasted_iota(jnp.int32, (SPAN, QUAD), 0)
    quad_lane = lax.broadcasted_iota(jnp.int32, (SPAN, QUAD), 1)
    quad_col = lax.rem(quad_lane, HD)
    ahead = quad_lane < PAIR
    before = jnp.where(ahead, quad_col - quad_row, quad_row - quad_col)
    strict, upto = before < 0, before <= 0
    eye = jnp.where(before == 0, 1.0, 0.0)

    def level(size):
        return (lax.div(quad_row, 2 * size) == lax.div(quad_col, 2 * size)) & (
            lax.div(quad_row, size) != lax.div(quad_col, size)
        )

    square_i = lax.broadcasted_iota(jnp.int32, (QUAD, QUAD), 0)
    square_j = lax.broadcasted_iota(jnp.int32, (QUAD, QUAD), 1)
    same_unit = lax.div(square_i, HD) == lax.div(square_j, HD)
    square_eye = square_i == square_j
    tri_i = lax.broadcasted_iota(jnp.int32, (SPAN, SPAN), 0)
    tri_j = lax.broadcasted_iota(jnp.int32, (SPAN, SPAN), 1)
    tri = [
        jnp.where(tri_j <= tri_i, 1.0, 0.0).astype(BF16),
        jnp.where(tri_j >= tri_i, 1.0, 0.0).astype(BF16),
    ]
    tri = [jnp.concatenate([one] * 3, axis=1) for one in tri]

    def diagonal(quad):
        left, right = quad[:, :PAIR], quad[:, PAIR:]
        return jnp.concatenate(
            [jnp.concatenate([left * one, nothing], axis=1) for one in ones]
            + [jnp.concatenate([nothing, right * one], axis=1) for one in ones],
            axis=0,
        )

    def quad_dot(lefts, right, dims=NN):
        highs, lows = zip(*[halves(left) for left in lefts])
        right_high, right_low = halves(right)
        count_left = len(lefts)
        outer = mm(jnp.concatenate(highs + lows, axis=0), diagonal(right_high), dims)
        inner = mm(jnp.concatenate(highs, axis=0), diagonal(right_low), dims)
        return [
            outer[k * SPAN : (k + 1) * SPAN]
            + (
                outer[(count_left + k) * SPAN : (count_left + k + 1) * SPAN]
                + inner[k * SPAN : (k + 1) * SPAN]
            )
            for k in range(count_left)
        ]

    def single(left, right):
        return mm(left.astype(BF16), diagonal(right.astype(BF16)))

    def rows_at(place):
        return pl.ds(pl.multiple_of(place * SPAN, SPAN), SPAN)

    def head_sum(value):
        low = jnp.sum(jnp.where(first, value, 0.0), axis=1, keepdims=True)
        high = jnp.sum(jnp.where(first, 0.0, value), axis=1, keepdims=True)
        return jnp.where(first, low, high)

    def prepare(direction, rows):
        read = proj_ref[rows, :PAIR].astype(F32)
        key = proj_ref[rows, PAIR : 2 * PAIR].astype(F32)
        log_decay = log_ref[direction, rows, :]
        unit = key * lax.rsqrt(head_sum(key * key) + NORM_EPS)
        erase = unit * learn_ref[direction, rows, :]
        high = log_decay.astype(BF16)
        rest = log_decay - high.astype(F32)
        middle_part = rest.astype(BF16)
        low = (rest - middle_part.astype(F32)).astype(BF16)
        total_log = mm(tri[direction], jnp.concatenate([high, middle_part, low], axis=0))
        end = SPAN - 1 if direction == 0 else 0
        span_log = total_log[end : end + 1, :]
        middle = 0.5 * span_log
        prior_log = total_log - log_decay
        inverse = jnp.exp(middle - total_log)
        left = jnp.exp(span_log - total_log)
        readers = jnp.concatenate(
            [jnp.exp(prior_log - middle) * unit, jnp.exp(total_log - middle) * read], axis=0
        )
        sources = jnp.concatenate([erase * inverse, key * inverse], axis=0)
        high_r, low_r = halves(readers)
        high_s, low_s = halves(sources)

        def spread(value):
            top, bottom = value[:SPAN], value[SPAN:]
            return jnp.concatenate([top * one for one in ones] + [bottom * one for one in ones], axis=0)

        high_s, low_s = spread(high_s), spread(low_s)
        meets = mm(
            jnp.concatenate([high_r, low_r, high_r], axis=1),
            jnp.concatenate([high_s, high_s, low_s], axis=1),
            NT,
        )
        return (
            meets,
            jnp.exp(prior_log) * unit,
            jnp.exp(total_log) * read,
            key * left,
            erase * left,
            jnp.exp(span_log),
        )

    def both(one, other):
        return jnp.concatenate([one, other], axis=1)

    def batch(groups):
        erased, seens, read_eraseds, starts, lefts, finals, spans, values = [], [], [], [], [], [], [], []
        for group in groups:
            rows = (rows_at(group), rows_at(count - 1 - group))
            parts = [prepare(direction, rows[direction]) for direction in range(2)]
            meets = [part[0] for part in parts]
            value = both(*[proj_ref[row, 2 * PAIR : 3 * PAIR] for row in rows])
            erased.append(
                jnp.where(strict, both(meets[0][:SPAN, :PAIR], meets[1][:SPAN, :PAIR]), 0.0)
            )
            seen = jnp.where(strict, both(meets[0][:SPAN, PAIR:], meets[1][:SPAN, PAIR:]), 0.0)
            s_re[group] = jnp.where(
                upto, both(meets[0][SPAN:, :PAIR], meets[1][SPAN:, :PAIR]), 0.0
            )
            read_seen = jnp.where(upto, both(meets[0][SPAN:, PAIR:], meets[1][SPAN:, PAIR:]), 0.0)
            starts.append(both(parts[0][1], parts[1][1]))
            s_read[group] = both(parts[0][2], parts[1][2])
            lefts.append((both(parts[0][3], parts[1][3]), both(parts[0][4], parts[1][4])))
            spans.append(both(parts[0][5], parts[1][5]))
            values.append(value)
            pieces = jnp.concatenate([*halves(seen), *halves(read_seen)], axis=0)
            met = mm(pieces, diagonal(value))
            seens.append(met[:SPAN] + met[SPAN : 2 * SPAN])
            s_local[group] = met[2 * SPAN : 3 * SPAN] + met[3 * SPAN :]
        solves = [eye - jnp.where(level(1), one, 0.0) for one in erased]
        width = 2
        while width < SPAN:
            at = level(width)
            firsts = [single(solve, jnp.where(at, one, 0.0)) for solve, one in zip(solves, erased)]
            solves = [solve - single(one, solve) for solve, one in zip(solves, firsts)]
            width *= 2
        hook()
        misses = [
            eye - solve - quad_dot([one], solve)[0] for solve, one in zip(solves, erased)
        ]
        solves = [solve + single(solve, miss) for solve, miss in zip(solves, misses)]
        maps = [quad_dot([solve], start)[0] for solve, start in zip(solves, starts)]
        shifts = [quad_dot([solve], seen)[0] for solve, seen in zip(solves, seens)]
        for place, group in enumerate(groups):
            key_left, erase_left = lefts[place]
            s_w[group] = jnp.concatenate([maps[place], shifts[place]], axis=1)
            map_high, map_low = halves(maps[place])
            left_high, left_low = halves(erase_left)
            fade = mm(
                jnp.concatenate([map_high, map_low, map_high], axis=0),
                jnp.concatenate([left_high, left_high, left_low], axis=0),
                TN,
            )
            s_m[group] = jnp.where(square_eye, spans[place], 0.0) - jnp.where(same_unit, fade, 0.0)
            shift_high, shift_low = halves(shifts[place])
            key_high, key_low = halves(key_left)
            gained = mm(
                jnp.concatenate(
                    [values[place], values[place], shift_high, shift_low, shift_high], axis=0
                ),
                jnp.concatenate(
                    [key_high, key_low, -left_high, -left_high, -left_low], axis=0
                ),
                TN,
            )
            gained = jnp.where(same_unit, gained, 0.0)
            s_a[group] = (gained[:SPAN] + gained[SPAN : 2 * SPAN]) + (
                gained[2 * SPAN : 3 * SPAN] + gained[3 * SPAN :]
            )

    size = count // 2
    middle = range(count // 4, count - count // 4)
    batch(list(middle))
    hook()
    batch([group for group in range(count) if group not in middle])
    hook()

    def advance(group, state):
        high, low = halves(state)
        step_high, step_low = halves(s_m[group])
        outer = mm(jnp.concatenate([high, low], axis=0), step_high)
        inner = mm(high, step_low)
        following = outer[:SPAN] + (outer[SPAN:] + inner) + s_a[group]
        s_a[group] = state
        return following

    state = states
    for group in range(count):
        state = advance(group, state)
    hook()

    def finish(group, carry):
        maps, shift = s_w[group, :, :QUAD], s_w[group, :, QUAD:]
        dropped, seen_state = quad_dot([maps, s_read[group]], s_a[group], NT)
        dropped = dropped + shift
        out = seen_state + s_local[group] - quad_dot([s_re[group]], dropped)[0]
        s_lin[0, rows_at(group), :] = out[:, :PAIR]
        s_lin[1, rows_at(count - 1 - group), :] = out[:, PAIR:]
        return carry

    def finish_batch(index, carry):
        for k in range(size):
            carry = finish(index * size + k, carry)
        return carry

    for index in range(count // size):
        finish_batch(index, 0)
        hook()

    quarter = HD // 4
    back = lax.rem(lane, 2 * quarter) >= quarter
    by_row = lax.rem(lane, HD) < 2 * quarter
    grid = total // GRID_W
    edge = jnp.zeros((WINDOW, PAIR), BF16)
    for ref in (kpad, vpad):
        ref[:WINDOW, :] = edge
        ref[WINDOW + total :, :] = edge

    def turned(value, cosine, sine):
        partner = jnp.where(
            back, pltpu.roll(value, quarter, 1), pltpu.roll(value, PAIR - quarter, 1)
        )
        return value * cosine + partner * sine

    def turn(place, carry):
        rows = rows_at(place)
        cosine, sine = [
            jnp.where(
                by_row,
                table_ref[which, pl.ds(place, 1), :],
                table_ref[which, grid : grid + GRID_W, :],
            )
            for which in range(2)
        ]
        query = proj_ref[rows, 3 * PAIR : 4 * PAIR].astype(F32)
        pair = proj_ref[rows, 4 * PAIR :].astype(F32)
        s_q[rows, :] = turned(query, cosine, sine).astype(BF16)
        key = jnp.where(first, turned(pair, cosine, sine), 0.0)
        value = jnp.where(first, 0.0, pair)
        there = pl.ds(pl.multiple_of(WINDOW + place * SPAN, SPAN), SPAN)
        kpad[there, :] = (key + pltpu.roll(key, HD, 1)).astype(BF16)
        vpad[there, :] = (value + pltpu.roll(value, HD, 1)).astype(BF16)
        return carry

    lax.fori_loop(0, grid, turn, 0)
    hook()
    reach = ATT_BLOCK + 2 * WINDOW
    ahead_of = lax.broadcasted_iota(jnp.int32, (ATT_BLOCK, reach), 1) - (
        WINDOW + lax.broadcasted_iota(jnp.int32, (ATT_BLOCK, reach), 0)
    )
    near = jnp.abs(ahead_of) <= WINDOW
    key_at = lax.broadcasted_iota(jnp.int32, (ATT_BLOCK, reach), 1) - WINDOW
    mine = lax.broadcasted_iota(jnp.int32, (ATT_BLOCK, PAIR), 1) < HD

    def attend(place, carry):
        start = pl.multiple_of(place * ATT_BLOCK, ATT_BLOCK)
        rows = pl.ds(start, ATT_BLOCK)
        query = s_q[rows, :]
        keys = kpad[pl.ds(start, reach), :]
        held = vpad[pl.ds(start, reach), :]
        allowed = near & (key_at >= -start) & (key_at < total - start)
        mixed = []
        for head in range(2):
            own = jnp.where(mine if head == 0 else jnp.logical_not(mine), query.astype(F32), 0.0)
            scores = mm(own.astype(BF16), keys, NT) * HD ** (-0.5)
            scores = jnp.where(allowed, scores, -jnp.inf)
            top = jnp.maximum(jnp.max(scores, axis=1, keepdims=True), sinks[head])
            raised = jnp.exp(scores - top)
            bottom = jnp.exp(sinks[head] - top) + jnp.sum(raised, axis=1, keepdims=True)
            mixed.append(mm((raised / bottom).astype(BF16), held))
        mix_ref[rows, PAIR:] = jnp.where(mine, mixed[0], mixed[1]).astype(BF16)
        return carry

    blocks = total // ATT_BLOCK
    for part in range(2):
        lax.fori_loop(part * blocks // 2, (part + 1) * blocks // 2, attend, 0)
        hook()

    def norm(place, carry):
        rows = rows_at(place)
        lin_sum = s_lin[0, rows, :] + s_lin[1, rows, :]
        centred = lin_sum - head_sum(lin_sum) * (1.0 / HD)
        spread = head_sum(centred * centred) * (1.0 / HD)
        mix_ref[rows, :PAIR] = (centred * lax.rsqrt(spread + GROUP_EPS) * gain).astype(BF16)
        return carry

    lax.fori_loop(0, count, norm, 0)


def mix_scratch(total):
    count = total // SPAN
    return [
        pltpu.VMEM((count, SPAN, 2 * QUAD), F32),
        pltpu.VMEM((count, SPAN, QUAD), F32),
        pltpu.VMEM((count, QUAD, QUAD), F32),
        pltpu.VMEM((count, SPAN, QUAD), F32),
        pltpu.VMEM((count, SPAN, QUAD), F32),
        pltpu.VMEM((count, SPAN, QUAD), F32),
        pltpu.VMEM((2, total, PAIR), F32),
        pltpu.VMEM((total + 2 * WINDOW, PAIR), BF16),
        pltpu.VMEM((total + 2 * WINDOW, PAIR), BF16),
        pltpu.VMEM((total, PAIR), BF16),
    ]


MESH_IDS = pl.DeviceIdType.MESH


def flipped(index, bits):
    result = index
    for bit in (1, 2):
        if bits & bit:
            result = result + bit - 2 * bit * lax.rem(lax.div(index, bit), 2)
    return result


def remote(src, dst, send, recv, device):
    return pltpu.make_async_remote_copy(
        src_ref=src,
        dst_ref=dst,
        send_sem=send,
        recv_sem=recv,
        device_id=device,
        device_id_type=MESH_IDS,
    )


def layer_kernel(
    x_ref,
    wr_ref,
    wk_ref,
    wv_ref,
    wq_ref,
    extra_ref,
    dup_ref,
    eup_ref,
    lin_ref,
    win_ref,
    init_ref,
    sink_ref,
    ak_ref,
    av_ref,
    gain_ref,
    ddown_ref,
    edown_ref,
    doff_ref,
    eoff_ref,
    table_ref,
    head_gain_ref,
    out_ref,
    xbuf,
    wbuf,
    kvbuf,
    ebuf,
    dup,
    eup,
    proj_ref,
    log_ref,
    learn_ref,
    owb,
    mbuf,
    mix_ref,
    lbuf,
    init,
    local_sem,
    wlocal_sem,
    up_send,
    up_recv,
    dn_send,
    dn_recv,
    sib_send,
    sib_recv,
    wz_send,
    wz_recv,
    e_send,
    e_recv,
    p_send,
    p_recv,
    f_send,
    f_recv,
    ou_send,
    ou_recv,
    od_send,
    od_recv,
    op_send,
    op_recv,
    of_send,
    of_recv,
    os_send,
    os_recv,
    m_send,
    m_recv,
    *scratch,
):
    sp, fs, tp = lax.axis_index("sp"), lax.axis_index("fs"), lax.axis_index("tp")
    depth, width, sides = [lax.axis_size(axis) for axis in ("sp", "fs", "tp")]
    tokens = x_ref.shape[1]
    rows = wr_ref.shape[0]
    out_rows, out_cols = lin_ref.shape
    share = out_ref.shape[1]
    sibling = {"tp": 1 - tp}
    plane = ({"fs": flipped(fs, 1)}, {"fs": flipped(fs, 2)})
    up_to, dn_to = {"sp": sp + 1}, {"sp": sp - 1}

    def rows_of(z, f):
        return pl.ds(pl.multiple_of((z * width + f) * rows, rows), rows)

    def cols_of(z, f, many=1):
        return pl.ds(pl.multiple_of((z * width + f) * out_cols, out_cols), many * out_cols)

    def pieces(z):
        low = pl.ds(pl.multiple_of(z * PAIR, PAIR), PAIR)
        return [ref.at[:, low] for ref in (wr_ref, wk_ref, wv_ref, wq_ref)]

    def lanes(place):
        return slice(place * PAIR, (place + 1) * PAIR)

    cols = pl.ds(pl.multiple_of((tp * depth + sp) * PAIR, PAIR), PAIR)
    head = (tp * depth + sp) * 2
    own_x = pltpu.make_async_copy(x_ref.at[0], xbuf.at[sp, tp], local_sem.at[0])
    own_w = [
        pltpu.make_async_copy(
            piece, wbuf.at[rows_of(sp, fs), lanes(place)], wlocal_sem.at[place]
        )
        for place, piece in enumerate(pieces(sp))
    ]
    own_o = [
        pltpu.make_async_copy(
            ref,
            owb.at[tp, pl.ds(place * out_rows, out_rows), cols_of(sp, fs)],
            local_sem.at[1 + place],
        )
        for place, ref in enumerate((lin_ref, win_ref))
    ]
    small = [
        pltpu.make_async_copy(extra_ref.at[0], ebuf.at[sp], local_sem.at[3]),
        pltpu.make_async_copy(dup_ref.at[:, :, cols], dup, local_sem.at[4]),
        pltpu.make_async_copy(eup_ref.at[:, :, cols], eup, local_sem.at[5]),
        pltpu.make_async_copy(init_ref.at[:, pl.ds(head, 2)], init, local_sem.at[6]),
    ]
    for copy in [own_x] + own_w + own_o + small:
        copy.start()
    low_lanes = lax.broadcasted_iota(jnp.int32, (rows, PAIR), 1) < HD
    near_key, near_value = ak_ref[...].astype(F32), av_ref[...].astype(F32)
    packs = (
        jnp.where(low_lanes, near_key, pltpu.roll(near_value, HD, 1)).astype(BF16),
        jnp.where(low_lanes, pltpu.roll(near_key, HD, 1), near_value).astype(BF16),
    )
    for place, pack in enumerate(packs):
        kvbuf[place] = pack
    wbuf[rows_of(sp, fs), lanes(4)] = jnp.where(sp >= 2, packs[1], packs[0])

    barrier = pltpu.get_barrier_semaphore()
    pairs = [(k, t) for k in range(depth) for t in range(sides) if k or t]
    peers = [{"sp": flipped(sp, k), "tp": tp + t - 2 * t * tp} for k, t in pairs] + [*plane]
    for peer in peers:
        pl.semaphore_signal(barrier, inc=1, device_id=peer, device_id_type=MESH_IDS)
    pl.semaphore_wait(barrier, len(peers))

    up_exists, dn_exists = sp < depth - 1, sp > 0

    def at_distance(k, body):
        if k == 0:
            body(sp)
            return

        def one(j, carry):
            body(sp + (2 * j - 1) * k)
            return carry

        lax.fori_loop(jnp.where(sp >= k, 0, 1), jnp.where(sp < depth - k, 2, 1), one, 0)

    def x_move(z, part, send, recv, device, src=None):
        span = pl.ds(part * (tokens // PARTS), tokens // PARTS)
        there = xbuf.at[z, tp, span]
        return remote(there if src is None else src.at[0, span], there, send, recv, device)

    def x_up(z, k, part, src=None):
        return x_move(z, part, up_send.at[k, part], up_recv.at[k, part], up_to, src)

    def x_dn(z, k, part, src=None):
        return x_move(z, part, dn_send.at[k, part], dn_recv.at[k, part], dn_to, src)

    def sib_move(z):
        there = xbuf.at[z, tp]
        return remote(there, there, sib_send.at[z], sib_recv.at[z], sibling)

    def wz_block(k):
        there = wbuf.at[rows_of(sp, fs)]
        return remote(there, there, wz_send.at[k - 1], wz_recv.at[k - 1], {"sp": flipped(sp, k)})

    def e_block(k):
        return remote(
            extra_ref.at[0],
            ebuf.at[sp],
            e_send.at[k - 1],
            e_recv.at[k - 1],
            {"sp": flipped(sp, k)},
        )

    def p_block(k, side):
        there = wbuf.at[rows_of(flipped(sp, k), fs)]
        return remote(there, there, p_send.at[k, side], p_recv.at[k, side], plane[side])

    def f_block(k):
        side = k % 2
        there = wbuf.at[rows_of(flipped(sp, k), flipped(fs, 2 if side == 0 else 1))]
        return remote(there, there, f_send.at[k], f_recv.at[k], plane[side])

    def o_move(z, send, recv, device):
        there = owb.at[tp, :, cols_of(z, fs)]
        return remote(there, there, send, recv, device)

    def o_up(z, k):
        return o_move(z, ou_send.at[k], ou_recv.at[k], up_to)

    def o_dn(z, k):
        return o_move(z, od_send.at[k], od_recv.at[k], dn_to)

    def op_block(z, side):
        return o_move(z, op_send.at[z, side], op_recv.at[z, side], plane[side])

    def of_block(z):
        odd = lax.rem(z, 2)
        near, far = flipped(fs, 1), flipped(fs, 2)
        there = owb.at[tp, :, cols_of(z, far + odd * (near - far))]
        device = {"fs": near + odd * (far - near)}
        return remote(there, there, of_send.at[z], of_recv.at[z], device)

    def os_block(z):
        there = owb.at[tp, :, cols_of(z, 0, width)]
        return remote(there, there, os_send.at[z], os_recv.at[z], sibling)

    def x_step(k):
        for part in range(PARTS):

            @pl.when(sp >= k)
            def _():
                x_up(sp, k - 1, part).wait_recv()
                if k < depth - 1:

                    @pl.when(up_exists)
                    def _():
                        x_up(sp - k, k, part).start()

            @pl.when(sp < depth - k)
            def _():
                x_dn(sp, k - 1, part).wait_recv()
                if k < depth - 1:

                    @pl.when(dn_exists)
                    def _():
                        x_dn(sp + k, k, part).start()

        at_distance(k, lambda z: sib_move(z).start())
        o_own(k)

    def o_own(k):
        if k < depth - 1:

            @pl.when(sp == k)
            def _():
                o_up(sp, 0).start()

            @pl.when(sp == depth - 1 - k)
            def _():
                o_dn(sp, 0).start()

    def w_step(k):
        if k:
            wz_block(k).wait_recv()
        for side in range(2):
            p_block(k, side).start()

    def f_step(k):
        for side in range(2):
            p_block(k, side).wait_recv()
        f_block(k).start()

    def op_start(z):
        for side in range(2):
            op_block(z, side).start()

    def o_step(k):
        @pl.when(sp >= k)
        def _():
            o_up(sp, k - 1).wait_recv()
            if k < depth - 1:

                @pl.when(up_exists)
                def _():
                    o_up(sp - k, k).start()

        @pl.when(sp < depth - k)
        def _():
            o_dn(sp, k - 1).wait_recv()
            if k < depth - 1:

                @pl.when(dn_exists)
                def _():
                    o_dn(sp + k, k).start()

        at_distance(k, op_start)

    def of_step(k):
        def body(z):
            for side in range(2):
                op_block(z, side).wait_recv()
            of_block(z).start()

        at_distance(k, body)

    def os_step(k):
        def body(z):
            of_block(z).wait_recv()
            os_block(z).start()

        at_distance(k, body)

    for k in ORDER:
        target = flipped(sp, k)
        sources = pieces(target) + [kvbuf.at[lax.div(target, 2)]]
        for place, piece in enumerate(sources):
            remote(
                piece,
                wbuf.at[rows_of(sp, fs), lanes(place)],
                wz_send.at[k - 1],
                wz_recv.at[k - 1],
                {"sp": target},
            ).start()
        e_block(k).start()
    for copy in own_w:
        copy.wait()
    w_step(0)
    for part in range(PARTS):

        @pl.when(up_exists)
        def _():
            x_up(sp, 0, part, x_ref).start()

        @pl.when(dn_exists)
        def _():
            x_dn(sp, 0, part, x_ref).start()

    own_x.wait()
    sib_move(sp).start()
    for copy in own_o:
        copy.wait()
    o_own(0)
    f_step(0)
    for k in ORDER:
        w_step(k)
    f_step(1)
    f_step(3)
    x_step(1)
    f_step(2)
    op_start(sp)
    x_step(2)
    x_step(3)
    of_step(0)
    for k in range(depth):
        f_block(k).wait_recv()
    for k in range(1, depth):
        e_block(k).wait_recv()
    for copy in small:
        copy.wait()

    gain = gain_ref[...]
    half = gain.shape[1] // 2
    doff = doff_ref[:, cols]
    eoff = eoff_ref[:, cols]

    def block(z):
        sib_move(z).wait_recv()
        parts = [xbuf[z, side].astype(F32) for side in range(2)]
        total = sum(jnp.sum(part * part, axis=1, keepdims=True) for part in parts)
        scale = lax.rsqrt(total / (2 * half) + NORM_EPS)
        hidden = jnp.concatenate(
            [
                (part * scale * gain[:, side * half : (side + 1) * half]).astype(BF16)
                for side, part in enumerate(parts)
            ],
            axis=1,
        )
        where = pl.ds(pl.multiple_of(z * tokens, tokens), tokens)
        proj_ref[where, :] = mm(hidden, wbuf[...]).astype(BF16)
        decay_low = mm(hidden, ddown_ref[...], NT).astype(BF16)
        decay_act = jnp.tanh(decay_low.astype(F32)).astype(BF16)
        learn_low = mm(hidden, edown_ref[...], NT).astype(BF16)
        spikes = jnp.concatenate(
            [
                jnp.broadcast_to(ebuf[z, pl.ds(2 * sp + place, 1), :], (HD, tokens))
                for place in range(2)
            ],
            axis=0,
        ).T
        for direction in range(2):
            pre = doff[direction : direction + 1] + mm(decay_act, dup[direction])
            softplus = jnp.maximum(-pre, 0.0) + jnp.log1p(jnp.exp(-jnp.abs(pre)))
            log_ref[direction, where, :] = spikes - jnp.exp(-softplus - 0.5)
            learn = eoff[direction : direction + 1] + mm(learn_low, eup[direction])
            learn_ref[direction, where, :] = jax.nn.sigmoid(learn)

    for k in range(depth):
        at_distance(k, block)
        if k == 1:
            o_step(1)

    plan = [
        [],
        [(os_step, 0), (o_step, 2)],
        [],
        [],
        [],
        [(of_step, 1), (o_step, 3)],
        [],
        [],
        [(of_step, 2)],
        [],
    ]
    queue = iter(plan)

    def hook():
        for step, k in next(queue, ()):
            step(k)

    states = jnp.concatenate([init[d, h] for d in range(2) for h in range(2)], axis=1)
    mix_body(
        hook,
        proj_ref,
        log_ref,
        learn_ref,
        table_ref,
        head_gain_ref[:, cols],
        [sink_ref[0, head], sink_ref[0, head + 1]],
        states,
        mix_ref,
        *scratch,
    )

    def m_block(k, t):
        z, side = flipped(sp, k), tp + t - 2 * t * tp
        start = pl.multiple_of((z * sides + side) * share, share)
        return remote(
            mix_ref.at[pl.ds(start, share)],
            mbuf.at[sp * sides + tp],
            m_send.at[k * sides + t],
            m_recv.at[k * sides + t],
            {"sp": z, "tp": side},
        )

    for k, t in pairs:
        m_block(k, t).start()
    mine = sp * sides + tp
    mbuf[mine] = mix_ref[pl.ds(pl.multiple_of(mine * share, share), share), :]
    os_step(1)
    of_step(3)
    os_step(2)
    for k, t in pairs:
        m_block(k, t).wait_recv()
    lefts = [
        jnp.concatenate(
            [mbuf[z * sides + side, :, :PAIR] for z in range(depth)]
            + [mbuf[z * sides + side, :, PAIR:] for z in range(depth)],
            axis=1,
        )
        for side in range(sides)
    ]
    for side in range(sides):
        lbuf[side] = lefts[side]

    def product(z):
        os_block(z).wait_recv()
        span = cols_of(z, 0, width)
        out_ref[0, :, span] = sum(
            mm(lbuf[side], owb[side, :, span]) for side in range(sides)
        ).astype(BF16)

    at_distance(0, product)
    at_distance(1, product)
    at_distance(2, product)
    os_step(3)
    at_distance(3, product)

    for k in range(depth - 1):

        @pl.when((sp >= k) & up_exists)
        def _():
            for part in range(PARTS):
                x_up(sp, k, part).wait_send()
            o_up(sp, k).wait_send()

        @pl.when((sp < depth - k) & dn_exists)
        def _():
            for part in range(PARTS):
                x_dn(sp, k, part).wait_send()
            o_dn(sp, k).wait_send()

    for k in range(1, depth):
        wz_block(k).wait_send()
        e_block(k).wait_send()
    for k in range(depth):
        for side in range(2):
            p_block(k, side).wait_send()
            op_block(k, side).wait_send()
        f_block(k).wait_send()
        of_block(k).wait_send()
        os_block(k).wait_send()
        sib_move(k).wait_send()
    for k, t in pairs:
        m_block(k, t).wait_send()


def by_heads(
    inputs,
    input_norm_gain,
    receptance_weight,
    linear_key_weight,
    linear_value_weight,
    window_query_weight,
    window_key_weight,
    window_value_weight,
    decay_down_weight,
    decay_up_weight,
    decay_offset,
    decay_log_extra,
    erasure_down_weight,
    erasure_up_weight,
    erasure_offset,
    initial_state,
    head_norm_gain,
    query_sink_logit,
    linear_output_weight,
    window_output_weight,
):
    depth, width, sides = [lax.axis_size(axis) for axis in ("sp", "fs", "tp")]
    _, tokens, half = inputs.shape
    total = tokens * depth
    rows = receptance_weight.shape[0]
    out_rows, out_cols = linear_output_weight.shape
    features = out_cols * depth * width
    share = tokens // sides
    low = decay_down_weight.shape[1]
    dma = pltpu.SemaphoreType.DMA
    any_spec = pl.BlockSpec(memory_space=pl.ANY)
    vmem_spec = pl.BlockSpec(memory_space=pltpu.VMEM)
    return pl.pallas_call(
        layer_kernel,
        in_specs=[any_spec] * 11 + [pl.BlockSpec(memory_space=pltpu.SMEM)] + [vmem_spec] * 9,
        out_specs=vmem_spec,
        out_shape=jax.ShapeDtypeStruct((1, share, features), BF16),
        scratch_shapes=[
            pltpu.VMEM((depth, 2, tokens, half), BF16),
            pltpu.VMEM((2 * half, 5 * PAIR), BF16),
            pltpu.VMEM((2, rows, PAIR), BF16),
            pltpu.VMEM((depth, decay_log_extra.shape[1], tokens), F32),
            pltpu.VMEM((2, low, PAIR), BF16),
            pltpu.VMEM((2, low, PAIR), BF16),
            pltpu.VMEM((total, 5 * PAIR), BF16),
            pltpu.VMEM((2, total, PAIR), F32),
            pltpu.VMEM((2, total, PAIR), F32),
            pltpu.VMEM((sides, 2 * out_rows, features), BF16),
            pltpu.VMEM((depth * sides, share, 2 * PAIR), BF16),
            pltpu.VMEM((total, 2 * PAIR), BF16),
            pltpu.VMEM((sides, share, 2 * out_rows), BF16),
            pltpu.VMEM((2, 2, HD, HD), F32),
            dma((7,)),
            dma((4,)),
            dma((depth, PARTS)),
            dma((depth, PARTS)),
            dma((depth, PARTS)),
            dma((depth, PARTS)),
            dma((depth,)),
            dma((depth,)),
            dma((depth - 1,)),
            dma((depth - 1,)),
            dma((depth - 1,)),
            dma((depth - 1,)),
            dma((width, 2)),
            dma((width, 2)),
            dma((width,)),
            dma((width,)),
            dma((depth - 1,)),
            dma((depth - 1,)),
            dma((depth - 1,)),
            dma((depth - 1,)),
            dma((depth, 2)),
            dma((depth, 2)),
            dma((depth,)),
            dma((depth,)),
            dma((depth,)),
            dma((depth,)),
            dma((depth * sides,)),
            dma((depth * sides,)),
        ]
        + mix_scratch(total),
        compiler_params=pltpu.CompilerParams(
            collective_id=0, has_side_effects=True, vmem_limit_bytes=VMEM_GRANT
        ),
        name="layer",
    )(
        inputs,
        receptance_weight,
        linear_key_weight,
        linear_value_weight,
        window_query_weight,
        decay_log_extra,
        decay_up_weight,
        erasure_up_weight,
        linear_output_weight,
        window_output_weight,
        initial_state,
        query_sink_logit[None, :],
        window_key_weight,
        window_value_weight,
        input_norm_gain[None, :],
        decay_down_weight.T,
        erasure_down_weight.T,
        decay_offset,
        erasure_offset,
        jnp.asarray(rope_tables(total)),
        head_norm_gain[None, :],
    )


def layer(*arrays):
    inputs, recept, keys = arrays[0], arrays[2], arrays[6]
    depth, width, sides = [lax.axis_size(axis) for axis in ("sp", "fs", "tp")]
    fits = (
        recept.shape[1] == arrays[5].shape[1] == depth * PAIR
        and 2 * keys.shape[1] == depth * HD
        and (depth, width, sides) == (4, 4, 2)
        and inputs.shape[1] % WINDOW == 0
        and SPAN == GRID_W
    )
    return (by_heads if fits else local)(*arrays)


def solution(mesh):
    return jax.shard_map(
        layer,
        mesh=mesh,
        in_specs=(
            P("fs", "sp", "tp"),
            P(),
            P(("sp", "fs"), "tp"),
            P(("sp", "fs"), "tp"),
            P(("sp", "fs"), "tp"),
            P(("sp", "fs"), "tp"),
            P(("sp", "fs"), "tp"),
            P(("sp", "fs"), "tp"),
            P(),
            P(),
            P(),
            P("fs", "tp", "sp"),
            P(),
            P(),
            P(),
            P(),
            P(),
            P(),
            P("tp", ("sp", "fs")),
            P("tp", ("sp", "fs")),
        ),
        out_specs=P("fs", ("sp", "tp"), None),
        check_vma=False,
    )
```

```python
import jax
import jax.numpy as jnp
import numpy as np
from jax import lax
from jax.experimental import pallas as pl
from jax.experimental.pallas import tpu as pltpu
from jax.sharding import PartitionSpec as P

HD = 64
WINDOW = 128
GRID_W = 64
ATT_BLOCK = 128


NORM_EPS = 1e-06
GROUP_EPS = 0.00064
ROPE_BASE = 10000.0
HIGHEST = lax.Precision.HIGHEST


def padded(block, sides, width):
    for axis, dim in sides:
        count = lax.axis_size(axis)
        forward = [(i, i + 1) for i in range(count - 1)]
        backward = [(target, source) for source, target in forward]
        low = lax.ppermute(
            lax.slice_in_dim(block, block.shape[dim] - width, None, axis=dim), axis, forward
        )
        high = lax.ppermute(lax.slice_in_dim(block, 0, width, axis=dim), axis, backward)
        block = jnp.concatenate([low, block, high], axis=dim)
    return block


def to_bf16(array):
    return lax.optimization_barrier(array.astype(jnp.bfloat16))


def rope_axial(values, positions):
    quarter = values.shape[-1] // 4
    inverse = ROPE_BASE ** (-jnp.arange(quarter, dtype=jnp.float32) / quarter)
    grid_rows = (positions // GRID_W).astype(jnp.float32)
    grid_cols = (positions % GRID_W).astype(jnp.float32)
    pieces = []
    for which_half, coordinate in ((0, grid_rows), (1, grid_cols)):
        angles = coordinate[:, None] * inverse[None, :]
        cosine = jnp.cos(angles)[:, None, :]
        sine_part = jnp.sin(angles)[:, None, :]
        front_part = values[..., 2 * which_half * quarter : (2 * which_half + 1) * quarter]
        back_part = values[..., (2 * which_half + 1) * quarter : (2 * which_half + 2) * quarter]
        pieces.append(front_part * cosine - back_part * sine_part)
        pieces.append(front_part * sine_part + back_part * cosine)
    return jnp.concatenate(pieces, axis=-1)


CHUNK = 32
PAIR = 2 * HD
F32 = jnp.float32
BF16 = jnp.bfloat16
NN = (((1,), (0,)), ((), ()))
NT = (((1,), (1,)), ((), ()))


def dot1(left, right, dims=NN):
    return lax.dot_general(
        left.astype(jnp.bfloat16), right.astype(jnp.bfloat16), dims, preferred_element_type=F32
    )


def halves(value):
    high = value.astype(jnp.bfloat16)
    return high, (value - high.astype(F32)).astype(jnp.bfloat16)


def dot3(left, right, dims=NN):
    left_high, left_low = halves(left)
    right_high, right_low = halves(right)

    def product(one, other):
        return lax.dot_general(one, other, dims, preferred_element_type=F32)

    return product(left_high, right_high) + (
        product(left_high, right_low) + product(left_low, right_high)
    )


def full_dot(left, right):
    return lax.dot_general(left, right, NN, precision=HIGHEST, preferred_element_type=F32)


def chunk_kernel(read_ref, key_ref, value_ref, log_ref, learn_ref, out_ref, end_ref):
    tokens = read_ref.shape[0]
    read = read_ref[...].astype(F32)
    key = key_ref[...].astype(F32)
    value = value_ref[...].astype(F32)
    first = lax.broadcasted_iota(jnp.int32, (tokens, PAIR), 1) < HD
    pair_i = lax.broadcasted_iota(jnp.int32, (PAIR, PAIR), 0)
    pair_j = lax.broadcasted_iota(jnp.int32, (PAIR, PAIR), 1)
    same_head = jnp.where(pair_i // HD == pair_j // HD, 1.0, 0.0)
    row = lax.broadcasted_iota(jnp.int32, (tokens, tokens), 0)
    col = lax.broadcasted_iota(jnp.int32, (tokens, tokens), 1)
    same_chunk = row // CHUNK == col // CHUNK
    eye = jnp.where(row == col, 1.0, 0.0)
    unit = key * lax.rsqrt(full_dot(key * key, same_head) + NORM_EPS)
    own = (first, jnp.logical_not(first))
    values = (
        jnp.where(first, value, 0.0),
        jnp.where(first, pltpu.roll(value, HD, 1), 0.0),
    )
    all_chunk = jnp.where(same_chunk, 1.0, 0.0)
    for direction in range(2):
        before = (col < row) if direction == 0 else (col > row)
        strict = same_chunk & before
        upto = same_chunk & (before | (col == row))
        log_decay = log_ref[direction]
        erase = unit * learn_ref[direction]
        total_log = full_dot(jnp.where(upto, 1.0, 0.0), log_decay)
        chunk_log = full_dot(all_chunk, log_decay)
        prior_log = total_log - log_decay
        middle = 0.5 * chunk_log
        unit_start = jnp.exp(prior_log) * unit
        unit_mid = jnp.exp(prior_log - middle) * unit
        read_start = jnp.exp(total_log) * read
        read_mid = jnp.exp(total_log - middle) * read
        inverse = jnp.exp(middle - total_log)
        sources = jnp.concatenate([erase * inverse, key * inverse], axis=0)
        rest = jnp.exp(chunk_log - total_log)
        key_rest = key * rest
        erase_rest = erase * rest
        chunk_decay = jnp.exp(chunk_log).T
        solved, offsets, mixes = [], [], []
        for head in range(2):
            readers = jnp.concatenate(
                [jnp.where(own[head], unit_mid, 0.0), jnp.where(own[head], read_mid, 0.0)], axis=0
            )
            meets = dot3(readers, sources, NT)
            erased = jnp.where(strict, meets[:tokens, :tokens], 0.0)
            seen = jnp.where(strict, meets[:tokens, tokens:], 0.0)
            read_erased = jnp.where(upto, meets[tokens:, :tokens], 0.0)
            read_seen = jnp.where(upto, meets[tokens:, tokens:], 0.0)
            solve = eye - jnp.where(row // 2 == col // 2, erased, 0.0)
            size = 2
            while size < CHUNK:
                level = (row // (2 * size) == col // (2 * size)) & (row // size != col // size)
                solve = solve - dot1(dot1(solve, jnp.where(level, erased, 0.0)), solve)
                size *= 2
            solve = solve + dot1(solve, eye - solve - dot3(erased, solve))
            both = dot3(
                solve,
                jnp.concatenate(
                    [jnp.where(own[head], unit_start, 0.0), dot3(seen, values[head])], axis=1
                ),
            )
            solved.append(both[:, :PAIR])
            offsets.append(both[:, PAIR:])
            mixes.append(jnp.concatenate([read_seen, -read_erased], axis=1))
        state = jnp.where(pair_j == HD + pair_i % HD, 1.0, 0.0)
        count = tokens // CHUNK
        drops = [[None] * count, [None] * count]
        reads = [[None] * count, [None] * count]
        for step in range(count):
            place = step if direction == 0 else count - 1 - step
            rows = slice(place * CHUNK, (place + 1) * CHUNK)
            lefts = jnp.concatenate(
                [solved[0][rows], solved[1][rows]]
                + [jnp.where(own[head], read_start, 0.0)[rows] for head in range(2)],
                axis=0,
            )
            seen_state = dot3(lefts, state)
            for head in range(2):
                drops[head][place] = (
                    seen_state[head * CHUNK : (head + 1) * CHUNK] + offsets[head][rows]
                )
                reads[head][place] = seen_state[(2 + head) * CHUNK : (3 + head) * CHUNK]
            adders = jnp.concatenate(
                [jnp.where(own[head], key_rest, 0.0)[rows] for head in range(2)]
                + [jnp.where(own[head], -erase_rest, 0.0)[rows] for head in range(2)],
                axis=0,
            ).T
            added = jnp.concatenate(
                [values[0][rows], values[1][rows], drops[0][place], drops[1][place]], axis=0
            )
            first_col = place * CHUNK
            state = chunk_decay[:, first_col : first_col + 1] * state + dot3(adders, added)
        for head in range(2):
            dropped = jnp.concatenate(drops[head], axis=0)
            out_ref[direction, head] = jnp.concatenate(reads[head], axis=0) + dot3(
                mixes[head], jnp.concatenate([values[head], dropped], axis=0)
            )
        end_ref[direction] = state


def chunked(returned, log_decay, learn, head_width):
    tokens = returned.shape[0]
    pairs = head_width // PAIR

    def role(which):
        return pl.BlockSpec((tokens, PAIR), lambda p: (0, which * pairs + p))

    wide = pl.BlockSpec((2, tokens, PAIR), lambda p: (0, 0, p))
    return pl.pallas_call(
        chunk_kernel,
        grid=(pairs,),
        in_specs=[role(0), role(1), role(2), wide, wide],
        out_specs=[
            pl.BlockSpec((2, 2, tokens, PAIR), lambda p: (0, p, 0, 0)),
            pl.BlockSpec((2, PAIR, PAIR), lambda p: (0, p, 0)),
        ],
        out_shape=[
            jax.ShapeDtypeStruct((2, 2 * pairs, tokens, PAIR), F32),
            jax.ShapeDtypeStruct((2, pairs * PAIR, PAIR), F32),
        ],
        cost_estimate=pl.CostEstimate(
            flops=pairs * 400 * PAIR**3, bytes_accessed=8 * tokens * head_width * 4, transcendentals=0
        ),
        name="chunked_state",
    )(returned, returned, returned, log_decay, learn)


def merge_kernel(local_ref, state_ref, gain_ref, out_ref):
    pair_i = lax.broadcasted_iota(jnp.int32, (PAIR, PAIR), 0)
    pair_j = lax.broadcasted_iota(jnp.int32, (PAIR, PAIR), 1)
    average = jnp.where(pair_i // HD == pair_j // HD, 1.0 / HD, 0.0)
    sums = []
    for head in range(2):
        total = 0.0
        for direction in range(2):
            block = local_ref[direction, head]
            total = total + (
                block[:, :HD] + dot3(block[:, HD:], state_ref[direction, head])
            )
        sums.append(total)
    lin_sum = jnp.concatenate(sums, axis=1)
    centred = lin_sum - full_dot(lin_sum, average)
    normed = centred * lax.rsqrt(full_dot(centred * centred, average) + GROUP_EPS)
    out_ref[...] = (normed * gain_ref[...]).astype(jnp.bfloat16)


def merged(local_out, entry, gain):
    _, head_count, tokens, _ = local_out.shape
    pairs = head_count // 2
    return pl.pallas_call(
        merge_kernel,
        grid=(pairs,),
        in_specs=[
            pl.BlockSpec((2, 2, tokens, PAIR), lambda p: (0, p, 0, 0)),
            pl.BlockSpec((2, 2, HD, HD), lambda p: (0, p, 0, 0)),
            pl.BlockSpec((1, PAIR), lambda p: (0, p)),
        ],
        out_specs=pl.BlockSpec((tokens, PAIR), lambda p: (0, p)),
        out_shape=jax.ShapeDtypeStruct((tokens, head_count * HD), jnp.bfloat16),
        cost_estimate=pl.CostEstimate(
            flops=pairs * 30 * PAIR**3, bytes_accessed=4 * tokens * head_count * PAIR * 4, transcendentals=0
        ),
        name="merged_norm",
    )(local_out, entry, gain[None, :])


def entering_states(ends, initial):
    count = lax.axis_size("sp")
    place = lax.axis_index("sp")
    ups = [(i, i + 1) for i in range(count - 1)]
    downs = [(i + 1, i) for i in range(count - 1)]
    adds, maps = ends[..., :HD], ends[..., HD:]

    def hop(_, states):
        later = jnp.einsum("dhkj,dhjv->dhkv", maps, states, precision=HIGHEST) + adds
        forward = lax.ppermute(later[0], "sp", ups)
        backward = lax.ppermute(later[1], "sp", downs)
        return jnp.stack(
            [
                jnp.where(place == 0, initial[0], forward),
                jnp.where(place == count - 1, initial[1], backward),
            ]
        )

    states = initial
    if count > 8:
        return lax.fori_loop(0, count - 1, hop, states)
    for _ in range(count - 1):
        states = hop(0, states)
    return states


def swapped(block, axis):
    count = lax.axis_size(axis)
    return [block] + [
        lax.ppermute(block, axis, [(i, i ^ flip) for i in range(count)]) for flip in range(1, count)
    ]


def in_order(pieces, axis):
    me = lax.axis_index(axis)
    stacked = jnp.stack(pieces)
    return [
        lax.dynamic_index_in_dim(stacked, me ^ place, 0, False) for place in range(len(pieces))
    ]


def local(
    inputs,
    input_norm_gain,
    receptance_weight,
    linear_key_weight,
    linear_value_weight,
    window_query_weight,
    window_key_weight,
    window_value_weight,
    decay_down_weight,
    decay_up_weight,
    decay_offset,
    decay_log_extra,
    erasure_down_weight,
    erasure_up_weight,
    erasure_offset,
    initial_state,
    head_norm_gain,
    query_sink_logit,
    linear_output_weight,
    window_output_weight,
):
    tokens = inputs.shape[1]
    tp_index = lax.axis_index("tp")
    length = tokens * lax.axis_size("sp")
    offset = lax.axis_index("sp") * tokens
    gathered = lax.all_gather(inputs, "tp", axis=2, tiled=True)[0]
    widened = gathered.astype(jnp.float32)
    hidden = to_bf16(
        widened
        * lax.rsqrt(jnp.mean(widened * widened, axis=-1, keepdims=True) + NORM_EPS)
        * input_norm_gain
    )
    weights = (
        receptance_weight,
        linear_key_weight,
        linear_value_weight,
        window_query_weight,
        window_key_weight,
        window_value_weight,
    )
    widths = [weight.shape[1] for weight in weights]
    joined = jnp.concatenate(weights, axis=1)
    regrouped = lax.all_to_all(joined, "fs", split_axis=1, concat_axis=0, tiled=True)
    every_seq = jnp.concatenate(swapped(hidden, "fs"), axis=0)
    near_cols = jnp.concatenate(in_order(swapped(window_output_weight, "fs"), "fs"), axis=1)
    whole_cols = lax.all_gather(regrouped, "sp", axis=0, tiled=True)
    partial_cols = jnp.dot(every_seq, whole_cols, preferred_element_type=jnp.float32)
    by_seq = to_bf16(partial_cols).reshape(-1, tokens, partial_cols.shape[1])
    outgoing = jnp.concatenate(in_order(list(by_seq), "fs"), axis=0)
    returned = lax.all_to_all(outgoing, "fs", split_axis=0, concat_axis=1, tiled=True)
    bounds = [0]
    for col_width in widths:
        bounds.append(bounds[-1] + col_width)
    projected = [returned[:, bounds[role_idx] : bounds[role_idx + 1]] for role_idx in range(6)]
    recept, lin_keys, lin_values, queries, att_keys, att_values = projected
    head_width = recept.shape[1]
    head_count = head_width // HD
    first_col = tp_index * head_width
    up_decay = lax.dynamic_slice_in_dim(decay_up_weight, first_col, head_width, 2)
    up_learn = lax.dynamic_slice_in_dim(erasure_up_weight, first_col, head_width, 2)
    base_decay = lax.dynamic_slice_in_dim(decay_offset, first_col, head_width, 1)
    base_learn = lax.dynamic_slice_in_dim(erasure_offset, first_col, head_width, 1)
    gain_local = lax.dynamic_slice_in_dim(head_norm_gain, first_col, head_width, 0)
    state_local = lax.dynamic_slice_in_dim(initial_state, tp_index * head_count, head_count, 1)
    spread = (
        jnp.arange(head_count)[:, None] == jnp.arange(head_width)[None, :] // HD
    ).astype(jnp.float32)
    decay_spikes = jnp.einsum("ht,hc->tc", decay_log_extra[0], spread, precision=HIGHEST)
    decay_low = to_bf16(jnp.dot(hidden, decay_down_weight, preferred_element_type=jnp.float32))
    decay_act = to_bf16(jnp.tanh(decay_low.astype(jnp.float32)))
    learn_low = to_bf16(jnp.dot(hidden, erasure_down_weight, preferred_element_type=jnp.float32))
    pre_decay = base_decay[:, None, :] + jnp.einsum(
        "tl,dlc->dtc", decay_act, up_decay, preferred_element_type=jnp.float32
    )
    log_decay = decay_spikes[None] - jnp.exp(-jax.nn.softplus(-pre_decay) - 0.5)
    learn = jax.nn.sigmoid(
        base_learn[:, None, :]
        + jnp.einsum("tl,dlc->dtc", learn_low, up_learn, preferred_element_type=jnp.float32)
    )
    local_out, ends = chunked(returned, log_decay, learn, head_width)
    entry = entering_states(
        ends.reshape(2, head_count, HD, PAIR), jnp.swapaxes(state_local, -1, -2)
    )
    lin_mix = merged(local_out, entry, gain_local)
    positions = offset + jnp.arange(tokens, dtype=jnp.int32)
    query_count = queries.shape[1] // HD
    group_count = att_keys.shape[1] // HD
    group_size = query_count // group_count
    roped_q = rope_axial(
        queries.astype(jnp.float32).reshape(tokens, query_count, HD), positions
    ).astype(jnp.bfloat16)
    roped_k = rope_axial(
        att_keys.astype(jnp.float32).reshape(tokens, group_count, HD), positions
    ).astype(jnp.bfloat16)
    kv_width = group_count * HD
    packed = jnp.concatenate([roped_k.reshape(tokens, kv_width), att_values], axis=1)
    bordered = padded(packed, (("sp", 0),), WINDOW)
    sink_local = lax.dynamic_slice_in_dim(
        query_sink_logit, tp_index * query_count, query_count, 0
    ).reshape(group_count, group_size)[:, :, None, None]
    reach = ATT_BLOCK + 2 * WINDOW
    query_rows = roped_q.reshape(ATT_BLOCK, group_count, group_size, HD)
    key_rows = bordered[:, :kv_width].reshape(reach, group_count, HD)
    value_rows = bordered[:, kv_width:].reshape(reach, group_count, HD)
    scores = jnp.einsum(
        "qgrd,kgd->grqk", query_rows, key_rows, preferred_element_type=jnp.float32
    ) * HD ** (-0.5)
    query_pos = offset + 0 + jnp.arange(ATT_BLOCK, dtype=jnp.int32)
    key_pos = offset + 0 - WINDOW + jnp.arange(reach, dtype=jnp.int32)
    allowed = (
        (jnp.abs(query_pos[:, None] - key_pos[None, :]) <= WINDOW)
        & (key_pos[None, :] >= 0)
        & (key_pos[None, :] < length)
    )
    scores = jnp.where(allowed, scores, -jnp.inf)
    top_score = jnp.maximum(jnp.max(scores, axis=-1, keepdims=True), sink_local)
    raised = jnp.exp(scores - top_score)
    denominator = jnp.exp(sink_local - top_score) + jnp.sum(raised, axis=-1, keepdims=True)
    weights_bf = (raised / denominator).astype(jnp.bfloat16)
    mixed = jnp.einsum("grqk,kgd->qgrd", weights_bf, value_rows, preferred_element_type=jnp.float32)
    outputs = mixed.astype(jnp.bfloat16).reshape(ATT_BLOCK, query_count * HD)
    lin_weight = lax.all_gather(linear_output_weight, ("sp", "fs"), axis=1, tiled=True)
    if lax.axis_size("sp") > 8:
        att_out = jnp.dot(
            outputs,
            lax.all_gather(near_cols, "sp", axis=1, tiled=True),
            preferred_element_type=jnp.float32,
        )
    else:
        att_parts = [
            jnp.dot(outputs, part, preferred_element_type=jnp.float32)
            for part in swapped(near_cols, "sp")
        ]
        att_out = jnp.concatenate(in_order(att_parts, "sp"), axis=1)
    layer_out = lax.psum_scatter(
        jnp.dot(lin_mix, lin_weight, preferred_element_type=jnp.float32) + att_out,
        "tp",
        scatter_dimension=0,
        tiled=True,
    )
    return layer_out.astype(jnp.bfloat16)[None]


SPAN = HD
PARTS = 2
ORDER = (1, 3, 2)
VMEM_GRANT = 67_000_000
QUAD = 4 * HD
TN = (((0,), (0,)), ((), ()))


def mm(left, right, dims=NN):
    return lax.dot_general(left, right, dims, preferred_element_type=F32)


def rope_tables(total):
    quarter = HD // 4
    inverse = ROPE_BASE ** (-np.arange(quarter, dtype=np.float32) / np.float32(quarter))
    inverse = inverse.astype(np.float32)
    lane = np.arange(PAIR) % HD
    rates = inverse[lane % quarter]
    sign = np.where(lane % (2 * quarter) < quarter, -1.0, 1.0)
    coords = np.concatenate([np.arange(total // GRID_W), np.arange(GRID_W)])
    angles = (coords.astype(np.float32)[:, None] * rates[None, :]).astype(np.float64)
    return np.stack([np.cos(angles), np.sin(angles) * sign]).astype(np.float32)


def mix_body(
    hook, proj_ref, log_ref, learn_ref, table_ref, gain, sinks, states, mix_ref, s_w, s_read, s_m, s_a, s_local, s_re, s_lin, kpad, vpad, s_q
):
    total = proj_ref.shape[0]
    count = total // SPAN
    lane = lax.broadcasted_iota(jnp.int32, (SPAN, PAIR), 1)
    first = lane < HD
    ones = (
        jnp.where(first, 1.0, 0.0).astype(BF16),
        jnp.where(first, 0.0, 1.0).astype(BF16),
    )
    nothing = jnp.zeros((SPAN, PAIR), BF16)
    quad_row = lax.broadcasted_iota(jnp.int32, (SPAN, QUAD), 0)
    quad_lane = lax.broadcasted_iota(jnp.int32, (SPAN, QUAD), 1)
    quad_col = lax.rem(quad_lane, HD)
    ahead = quad_lane < PAIR
    before = jnp.where(ahead, quad_col - quad_row, quad_row - quad_col)
    strict, upto = before < 0, before <= 0
    eye = jnp.where(before == 0, 1.0, 0.0)

    def level(size):
        return (lax.div(quad_row, 2 * size) == lax.div(quad_col, 2 * size)) & (
            lax.div(quad_row, size) != lax.div(quad_col, size)
        )

    square_i = lax.broadcasted_iota(jnp.int32, (QUAD, QUAD), 0)
    square_j = lax.broadcasted_iota(jnp.int32, (QUAD, QUAD), 1)
    same_unit = lax.div(square_i, HD) == lax.div(square_j, HD)
    square_eye = square_i == square_j
    tri_i = lax.broadcasted_iota(jnp.int32, (SPAN, SPAN), 0)
    tri_j = lax.broadcasted_iota(jnp.int32, (SPAN, SPAN), 1)
    tri = [
        jnp.where(tri_j <= tri_i, 1.0, 0.0).astype(BF16),
        jnp.where(tri_j >= tri_i, 1.0, 0.0).astype(BF16),
    ]
    tri = [jnp.concatenate([one] * 3, axis=1) for one in tri]

    def diagonal(quad):
        left, right = quad[:, :PAIR], quad[:, PAIR:]
        return jnp.concatenate(
            [jnp.concatenate([left * one, nothing], axis=1) for one in ones]
            + [jnp.concatenate([nothing, right * one], axis=1) for one in ones],
            axis=0,
        )

    def quad_dot(lefts, right, dims=NN):
        highs, lows = zip(*[halves(left) for left in lefts])
        right_high, right_low = halves(right)
        count_left = len(lefts)
        outer = mm(jnp.concatenate(highs + lows, axis=0), diagonal(right_high), dims)
        inner = mm(jnp.concatenate(highs, axis=0), diagonal(right_low), dims)
        return [
            outer[k * SPAN : (k + 1) * SPAN]
            + (
                outer[(count_left + k) * SPAN : (count_left + k + 1) * SPAN]
                + inner[k * SPAN : (k + 1) * SPAN]
            )
            for k in range(count_left)
        ]

    def single(left, right):
        return mm(left.astype(BF16), diagonal(right.astype(BF16)))

    def rows_at(place):
        return pl.ds(pl.multiple_of(place * SPAN, SPAN), SPAN)

    def head_sum(value):
        low = jnp.sum(jnp.where(first, value, 0.0), axis=1, keepdims=True)
        high = jnp.sum(jnp.where(first, 0.0, value), axis=1, keepdims=True)
        return jnp.where(first, low, high)

    def prepare(direction, rows):
        read = proj_ref[rows, :PAIR].astype(F32)
        key = proj_ref[rows, PAIR : 2 * PAIR].astype(F32)
        log_decay = log_ref[direction, rows, :]
        unit = key * lax.rsqrt(head_sum(key * key) + NORM_EPS)
        erase = unit * learn_ref[direction, rows, :]
        high = log_decay.astype(BF16)
        rest = log_decay - high.astype(F32)
        middle_part = rest.astype(BF16)
        low = (rest - middle_part.astype(F32)).astype(BF16)
        total_log = mm(tri[direction], jnp.concatenate([high, middle_part, low], axis=0))
        end = SPAN - 1 if direction == 0 else 0
        span_log = total_log[end : end + 1, :]
        middle = 0.5 * span_log
        prior_log = total_log - log_decay
        inverse = jnp.exp(middle - total_log)
        left = jnp.exp(span_log - total_log)
        readers = jnp.concatenate(
            [jnp.exp(prior_log - middle) * unit, jnp.exp(total_log - middle) * read], axis=0
        )
        sources = jnp.concatenate([erase * inverse, key * inverse], axis=0)
        high_r, low_r = halves(readers)
        high_s, low_s = halves(sources)

        def spread(value):
            top, bottom = value[:SPAN], value[SPAN:]
            return jnp.concatenate([top * one for one in ones] + [bottom * one for one in ones], axis=0)

        high_s, low_s = spread(high_s), spread(low_s)
        meets = mm(
            jnp.concatenate([high_r, low_r, high_r], axis=1),
            jnp.concatenate([high_s, high_s, low_s], axis=1),
            NT,
        )
        return (
            meets,
            jnp.exp(prior_log) * unit,
            jnp.exp(total_log) * read,
            key * left,
            erase * left,
            jnp.exp(span_log),
        )

    def both(one, other):
        return jnp.concatenate([one, other], axis=1)

    def batch(groups):
        erased, seens, read_eraseds, starts, lefts, finals, spans, values = [], [], [], [], [], [], [], []
        for group in groups:
            rows = (rows_at(group), rows_at(count - 1 - group))
            parts = [prepare(direction, rows[direction]) for direction in range(2)]
            meets = [part[0] for part in parts]
            value = both(*[proj_ref[row, 2 * PAIR : 3 * PAIR] for row in rows])
            erased.append(
                jnp.where(strict, both(meets[0][:SPAN, :PAIR], meets[1][:SPAN, :PAIR]), 0.0)
            )
            seen = jnp.where(strict, both(meets[0][:SPAN, PAIR:], meets[1][:SPAN, PAIR:]), 0.0)
            s_re[group] = jnp.where(
                upto, both(meets[0][SPAN:, :PAIR], meets[1][SPAN:, :PAIR]), 0.0
            )
            read_seen = jnp.where(upto, both(meets[0][SPAN:, PAIR:], meets[1][SPAN:, PAIR:]), 0.0)
            starts.append(both(parts[0][1], parts[1][1]))
            s_read[group] = both(parts[0][2], parts[1][2])
            lefts.append((both(parts[0][3], parts[1][3]), both(parts[0][4], parts[1][4])))
            spans.append(both(parts[0][5], parts[1][5]))
            values.append(value)
            pieces = jnp.concatenate([*halves(seen), *halves(read_seen)], axis=0)
            met = mm(pieces, diagonal(value))
            seens.append(met[:SPAN] + met[SPAN : 2 * SPAN])
            s_local[group] = met[2 * SPAN : 3 * SPAN] + met[3 * SPAN :]
        solves = [eye - jnp.where(level(1), one, 0.0) for one in erased]
        width = 2
        while width < SPAN:
            at = level(width)
            firsts = [single(solve, jnp.where(at, one, 0.0)) for solve, one in zip(solves, erased)]
            solves = [solve - single(one, solve) for solve, one in zip(solves, firsts)]
            width *= 2
        hook()
        misses = [
            eye - solve - quad_dot([one], solve)[0] for solve, one in zip(solves, erased)
        ]
        solves = [solve + single(solve, miss) for solve, miss in zip(solves, misses)]
        maps = [quad_dot([solve], start)[0] for solve, start in zip(solves, starts)]
        shifts = [quad_dot([solve], seen)[0] for solve, seen in zip(solves, seens)]
        for place, group in enumerate(groups):
            key_left, erase_left = lefts[place]
            s_w[group] = jnp.concatenate([maps[place], shifts[place]], axis=1)
            map_high, map_low = halves(maps[place])
            left_high, left_low = halves(erase_left)
            fade = mm(
                jnp.concatenate([map_high, map_low, map_high], axis=0),
                jnp.concatenate([left_high, left_high, left_low], axis=0),
                TN,
            )
            s_m[group] = jnp.where(square_eye, spans[place], 0.0) - jnp.where(same_unit, fade, 0.0)
            shift_high, shift_low = halves(shifts[place])
            key_high, key_low = halves(key_left)
            gained = mm(
                jnp.concatenate(
                    [values[place], values[place], shift_high, shift_low, shift_high], axis=0
                ),
                jnp.concatenate(
                    [key_high, key_low, -left_high, -left_high, -left_low], axis=0
                ),
                TN,
            )
            gained = jnp.where(same_unit, gained, 0.0)
            s_a[group] = (gained[:SPAN] + gained[SPAN : 2 * SPAN]) + (
                gained[2 * SPAN : 3 * SPAN] + gained[3 * SPAN :]
            )

    size = count // 2
    middle = range(count // 4, count - count // 4)
    batch(list(middle))
    hook()
    batch([group for group in range(count) if group not in middle])
    hook()

    def advance(group, state):
        high, low = halves(state)
        step_high, step_low = halves(s_m[group])
        outer = mm(jnp.concatenate([high, low], axis=0), step_high)
        inner = mm(high, step_low)
        following = outer[:SPAN] + (outer[SPAN:] + inner) + s_a[group]
        s_a[group] = state
        return following

    state = states
    for group in range(count):
        state = advance(group, state)
    hook()

    def finish(group, carry):
        maps, shift = s_w[group, :, :QUAD], s_w[group, :, QUAD:]
        dropped, seen_state = quad_dot([maps, s_read[group]], s_a[group], NT)
        dropped = dropped + shift
        out = seen_state + s_local[group] - quad_dot([s_re[group]], dropped)[0]
        s_lin[0, rows_at(group), :] = out[:, :PAIR]
        s_lin[1, rows_at(count - 1 - group), :] = out[:, PAIR:]
        return carry

    def finish_batch(index, carry):
        for k in range(size):
            carry = finish(index * size + k, carry)
        return carry

    for index in range(count // size):
        finish_batch(index, 0)
        hook()

    def norm(place, carry):
        rows = rows_at(place)
        lin_sum = s_lin[0, rows, :] + s_lin[1, rows, :]
        centred = lin_sum - head_sum(lin_sum) * (1.0 / HD)
        spread = head_sum(centred * centred) * (1.0 / HD)
        mix_ref[0, rows, :] = (centred * lax.rsqrt(spread + GROUP_EPS) * gain).astype(BF16)
        return carry

    lax.fori_loop(0, count, norm, 0)
    hook()

    quarter = HD // 4
    back = lax.rem(lane, 2 * quarter) >= quarter
    by_row = lax.rem(lane, HD) < 2 * quarter
    grid = total // GRID_W
    edge = jnp.zeros((WINDOW, PAIR), BF16)
    for ref in (kpad, vpad):
        ref[:WINDOW, :] = edge
        ref[WINDOW + total :, :] = edge

    def turned(value, cosine, sine):
        partner = jnp.where(
            back, pltpu.roll(value, quarter, 1), pltpu.roll(value, PAIR - quarter, 1)
        )
        return value * cosine + partner * sine

    def turn(place, carry):
        rows = rows_at(place)
        cosine, sine = [
            jnp.where(
                by_row,
                table_ref[which, pl.ds(place, 1), :],
                table_ref[which, grid : grid + GRID_W, :],
            )
            for which in range(2)
        ]
        query = proj_ref[rows, 3 * PAIR : 4 * PAIR].astype(F32)
        pair = proj_ref[rows, 4 * PAIR :].astype(F32)
        s_q[rows, :] = turned(query, cosine, sine).astype(BF16)
        key = jnp.where(first, turned(pair, cosine, sine), 0.0)
        value = jnp.where(first, 0.0, pair)
        there = pl.ds(pl.multiple_of(WINDOW + place * SPAN, SPAN), SPAN)
        kpad[there, :] = (key + pltpu.roll(key, HD, 1)).astype(BF16)
        vpad[there, :] = (value + pltpu.roll(value, HD, 1)).astype(BF16)
        return carry

    lax.fori_loop(0, grid, turn, 0)
    hook()
    reach = ATT_BLOCK + 2 * WINDOW
    ahead_of = lax.broadcasted_iota(jnp.int32, (ATT_BLOCK, reach), 1) - (
        WINDOW + lax.broadcasted_iota(jnp.int32, (ATT_BLOCK, reach), 0)
    )
    near = jnp.abs(ahead_of) <= WINDOW
    key_at = lax.broadcasted_iota(jnp.int32, (ATT_BLOCK, reach), 1) - WINDOW
    mine = lax.broadcasted_iota(jnp.int32, (ATT_BLOCK, PAIR), 1) < HD

    def attend(place, carry):
        start = pl.multiple_of(place * ATT_BLOCK, ATT_BLOCK)
        rows = pl.ds(start, ATT_BLOCK)
        query = s_q[rows, :]
        keys = kpad[pl.ds(start, reach), :]
        held = vpad[pl.ds(start, reach), :]
        allowed = near & (key_at >= -start) & (key_at < total - start)
        mixed = []
        for head in range(2):
            own = jnp.where(mine if head == 0 else jnp.logical_not(mine), query.astype(F32), 0.0)
            scores = mm(own.astype(BF16), keys, NT) * HD ** (-0.5)
            scores = jnp.where(allowed, scores, -jnp.inf)
            top = jnp.maximum(jnp.max(scores, axis=1, keepdims=True), sinks[head])
            raised = jnp.exp(scores - top)
            bottom = jnp.exp(sinks[head] - top) + jnp.sum(raised, axis=1, keepdims=True)
            mixed.append(mm((raised / bottom).astype(BF16), held))
        mix_ref[1, rows, :] = jnp.where(mine, mixed[0], mixed[1]).astype(BF16)
        return carry

    blocks = total // ATT_BLOCK
    for part in range(2):
        lax.fori_loop(part * blocks // 2, (part + 1) * blocks // 2, attend, 0)
        hook()


def mix_scratch(total):
    count = total // SPAN
    return [
        pltpu.VMEM((count, SPAN, 2 * QUAD), F32),
        pltpu.VMEM((count, SPAN, QUAD), F32),
        pltpu.VMEM((count, QUAD, QUAD), F32),
        pltpu.VMEM((count, SPAN, QUAD), F32),
        pltpu.VMEM((count, SPAN, QUAD), F32),
        pltpu.VMEM((count, SPAN, QUAD), F32),
        pltpu.VMEM((2, total, PAIR), F32),
        pltpu.VMEM((total + 2 * WINDOW, PAIR), BF16),
        pltpu.VMEM((total + 2 * WINDOW, PAIR), BF16),
        pltpu.VMEM((total, PAIR), BF16),
    ]


MESH_IDS = pl.DeviceIdType.MESH


def flipped(index, bits):
    result = index
    for bit in (1, 2):
        if bits & bit:
            result = result + bit - 2 * bit * lax.rem(lax.div(index, bit), 2)
    return result


def remote(src, dst, send, recv, device):
    return pltpu.make_async_remote_copy(
        src_ref=src,
        dst_ref=dst,
        send_sem=send,
        recv_sem=recv,
        device_id=device,
        device_id_type=MESH_IDS,
    )


def layer_kernel(
    x_ref,
    wr_ref,
    wk_ref,
    wv_ref,
    wq_ref,
    extra_ref,
    dup_ref,
    eup_ref,
    lin_ref,
    win_ref,
    init_ref,
    sink_ref,
    ak_ref,
    av_ref,
    gain_ref,
    ddown_ref,
    edown_ref,
    doff_ref,
    eoff_ref,
    table_ref,
    head_gain_ref,
    out_ref,
    xbuf,
    wbuf,
    kvbuf,
    ebuf,
    dup,
    eup,
    proj_ref,
    log_ref,
    learn_ref,
    owb,
    mbuf,
    mix_ref,
    lbuf,
    pbuf,
    rbuf,
    init,
    local_sem,
    wlocal_sem,
    up_send,
    up_recv,
    dn_send,
    dn_recv,
    sib_send,
    sib_recv,
    wz_send,
    wz_recv,
    e_send,
    e_recv,
    p_send,
    p_recv,
    f_send,
    f_recv,
    ou_send,
    ou_recv,
    od_send,
    od_recv,
    op_send,
    op_recv,
    of_send,
    of_recv,
    part_send,
    part_recv,
    m_send,
    m_recv,
    *scratch,
):
    sp, fs, tp = lax.axis_index("sp"), lax.axis_index("fs"), lax.axis_index("tp")
    depth, width, sides = [lax.axis_size(axis) for axis in ("sp", "fs", "tp")]
    tokens = x_ref.shape[1]
    rows = wr_ref.shape[0]
    out_rows, out_cols = lin_ref.shape
    share = out_ref.shape[1]
    sibling = {"tp": 1 - tp}
    plane = ({"fs": flipped(fs, 1)}, {"fs": flipped(fs, 2)})
    up_to, dn_to = {"sp": sp + 1}, {"sp": sp - 1}

    def rows_of(z, f):
        return pl.ds(pl.multiple_of((z * width + f) * rows, rows), rows)

    def cols_of(z, f, many=1):
        return pl.ds(pl.multiple_of((z * width + f) * out_cols, out_cols), many * out_cols)

    def pieces(z):
        low = pl.ds(pl.multiple_of(z * PAIR, PAIR), PAIR)
        return [ref.at[:, low] for ref in (wr_ref, wk_ref, wv_ref, wq_ref)]

    def lanes(place):
        return slice(place * PAIR, (place + 1) * PAIR)

    cols = pl.ds(pl.multiple_of((tp * depth + sp) * PAIR, PAIR), PAIR)
    head = (tp * depth + sp) * 2
    own_x = pltpu.make_async_copy(x_ref.at[0], xbuf.at[sp, tp], local_sem.at[0])
    own_w = [
        pltpu.make_async_copy(
            piece, wbuf.at[rows_of(sp, fs), lanes(place)], wlocal_sem.at[place]
        )
        for place, piece in enumerate(pieces(sp))
    ]
    own_o = [
        pltpu.make_async_copy(
            ref,
            owb.at[pl.ds(place * out_rows, out_rows), cols_of(sp, fs)],
            local_sem.at[1 + place],
        )
        for place, ref in enumerate((lin_ref, win_ref))
    ]
    small = [
        pltpu.make_async_copy(extra_ref.at[0], ebuf.at[sp], local_sem.at[3]),
        pltpu.make_async_copy(dup_ref.at[:, :, cols], dup, local_sem.at[4]),
        pltpu.make_async_copy(eup_ref.at[:, :, cols], eup, local_sem.at[5]),
        pltpu.make_async_copy(init_ref.at[:, pl.ds(head, 2)], init, local_sem.at[6]),
    ]
    for copy in [own_x] + own_w + own_o + small:
        copy.start()
    low_lanes = lax.broadcasted_iota(jnp.int32, (rows, PAIR), 1) < HD
    near_key, near_value = ak_ref[...].astype(F32), av_ref[...].astype(F32)
    packs = (
        jnp.where(low_lanes, near_key, pltpu.roll(near_value, HD, 1)).astype(BF16),
        jnp.where(low_lanes, pltpu.roll(near_key, HD, 1), near_value).astype(BF16),
    )
    for place, pack in enumerate(packs):
        kvbuf[place] = pack
    wbuf[rows_of(sp, fs), lanes(4)] = jnp.where(sp >= 2, packs[1], packs[0])

    barrier = pltpu.get_barrier_semaphore()
    peers = [{"sp": flipped(sp, k)} for k in range(1, depth)] + [sibling, *plane]
    for peer in peers:
        pl.semaphore_signal(barrier, inc=1, device_id=peer, device_id_type=MESH_IDS)
    pl.semaphore_wait(barrier, len(peers))

    up_exists, dn_exists = sp < depth - 1, sp > 0

    def at_distance(k, body):
        if k == 0:
            body(sp)
            return

        def one(j, carry):
            body(sp + (2 * j - 1) * k)
            return carry

        lax.fori_loop(jnp.where(sp >= k, 0, 1), jnp.where(sp < depth - k, 2, 1), one, 0)

    def x_move(z, part, send, recv, device, src=None):
        span = pl.ds(part * (tokens // PARTS), tokens // PARTS)
        there = xbuf.at[z, tp, span]
        return remote(there if src is None else src.at[0, span], there, send, recv, device)

    def x_up(z, k, part, src=None):
        return x_move(z, part, up_send.at[k, part], up_recv.at[k, part], up_to, src)

    def x_dn(z, k, part, src=None):
        return x_move(z, part, dn_send.at[k, part], dn_recv.at[k, part], dn_to, src)

    def sib_move(z):
        there = xbuf.at[z, tp]
        return remote(there, there, sib_send.at[z], sib_recv.at[z], sibling)

    def wz_block(k):
        there = wbuf.at[rows_of(sp, fs)]
        return remote(there, there, wz_send.at[k - 1], wz_recv.at[k - 1], {"sp": flipped(sp, k)})

    def e_block(k):
        return remote(
            extra_ref.at[0],
            ebuf.at[sp],
            e_send.at[k - 1],
            e_recv.at[k - 1],
            {"sp": flipped(sp, k)},
        )

    def p_block(k, side):
        there = wbuf.at[rows_of(flipped(sp, k), fs)]
        return remote(there, there, p_send.at[k, side], p_recv.at[k, side], plane[side])

    def f_block(k):
        side = k % 2
        there = wbuf.at[rows_of(flipped(sp, k), flipped(fs, 2 if side == 0 else 1))]
        return remote(there, there, f_send.at[k], f_recv.at[k], plane[side])

    def o_move(z, send, recv, device):
        there = owb.at[:, cols_of(z, fs)]
        return remote(there, there, send, recv, device)

    def o_up(z, k):
        return o_move(z, ou_send.at[k], ou_recv.at[k], up_to)

    def o_dn(z, k):
        return o_move(z, od_send.at[k], od_recv.at[k], dn_to)

    def op_block(z, side):
        return o_move(z, op_send.at[z, side], op_recv.at[z, side], plane[side])

    def of_block(z):
        odd = lax.rem(z, 2)
        near, far = flipped(fs, 1), flipped(fs, 2)
        there = owb.at[:, cols_of(z, far + odd * (near - far))]
        device = {"fs": near + odd * (far - near)}
        return remote(there, there, of_send.at[z], of_recv.at[z], device)

    def x_step(k):
        for part in range(PARTS):

            @pl.when(sp >= k)
            def _():
                x_up(sp, k - 1, part).wait_recv()
                if k < depth - 1:

                    @pl.when(up_exists)
                    def _():
                        x_up(sp - k, k, part).start()

            @pl.when(sp < depth - k)
            def _():
                x_dn(sp, k - 1, part).wait_recv()
                if k < depth - 1:

                    @pl.when(dn_exists)
                    def _():
                        x_dn(sp + k, k, part).start()

        at_distance(k, lambda z: sib_move(z).start())
        o_own(k)

    def o_own(k):
        if k == 0:
            ups, dns = sp == 0, sp == depth - 1
        else:
            ups, dns = (sp > 0) & up_exists, (sp < depth - 1) & dn_exists
        if k < 2:

            @pl.when(ups)
            def _():
                o_up(sp, 0).start()

            @pl.when(dns)
            def _():
                o_dn(sp, 0).start()

    def w_step(k):
        if k:
            wz_block(k).wait_recv()
        for side in range(2):
            p_block(k, side).start()

    def f_step(k):
        for side in range(2):
            p_block(k, side).wait_recv()
        f_block(k).start()

    def op_start(z):
        for side in range(2):
            op_block(z, side).start()

    inner = (sp > 0) & up_exists
    odd = lax.rem(sp, 2)
    next_z = 1 + odd
    last_z = (depth - 1) * (1 - odd)
    far_z = jnp.where(sp < 2, sp + 2, sp - 2)

    def o_step(z):
        @pl.when(z < sp)
        def _():
            o_up(sp, sp - z - 1).wait_recv()

            @pl.when(up_exists)
            def _():
                o_up(z, sp - z).start()

        @pl.when(z > sp)
        def _():
            o_dn(sp, z - sp - 1).wait_recv()

            @pl.when(dn_exists)
            def _():
                o_dn(z, z - sp).start()

        op_start(z)

    def of_step(z):
        for side in range(2):
            op_block(z, side).wait_recv()
        of_block(z).start()

    def phase(step, stage):
        if stage == 0:

            @pl.when(inner)
            def _():
                step(last_z)

        elif stage == 3:

            @pl.when(jnp.logical_not(inner))
            def _():
                step(last_z)

        else:
            step(next_z if stage == 1 else far_z)

    def inner_only(step, z):
        @pl.when(inner)
        def _():
            step(z)

    def ends_only(step, z):
        @pl.when(jnp.logical_not(inner))
        def _():
            step(z)

    for k in ORDER:
        target = flipped(sp, k)
        sources = pieces(target) + [kvbuf.at[lax.div(target, 2)]]
        for place, piece in enumerate(sources):
            remote(
                piece,
                wbuf.at[rows_of(sp, fs), lanes(place)],
                wz_send.at[k - 1],
                wz_recv.at[k - 1],
                {"sp": target},
            ).start()
        e_block(k).start()
    for copy in own_w:
        copy.wait()
    w_step(0)
    for part in range(PARTS):

        @pl.when(up_exists)
        def _():
            x_up(sp, 0, part, x_ref).start()

        @pl.when(dn_exists)
        def _():
            x_dn(sp, 0, part, x_ref).start()

    own_x.wait()
    sib_move(sp).start()
    for copy in own_o:
        copy.wait()
    o_own(0)
    f_step(0)
    ends_only(op_start, sp)
    for k in ORDER:
        w_step(k)
    f_step(1)
    f_step(3)
    x_step(1)
    f_step(2)
    inner_only(op_start, sp)
    ends_only(of_step, sp)
    x_step(2)
    phase(o_step, 0)
    for k in range(depth):
        f_block(k).wait_recv()
    for k in range(1, depth):
        e_block(k).wait_recv()
    for copy in small:
        copy.wait()

    gain = gain_ref[...]
    half = gain.shape[1] // 2
    doff = doff_ref[:, cols]
    eoff = eoff_ref[:, cols]

    def block(z):
        sib_move(z).wait_recv()
        parts = [xbuf[z, side].astype(F32) for side in range(2)]
        total = sum(jnp.sum(part * part, axis=1, keepdims=True) for part in parts)
        scale = lax.rsqrt(total / (2 * half) + NORM_EPS)
        hidden = jnp.concatenate(
            [
                (part * scale * gain[:, side * half : (side + 1) * half]).astype(BF16)
                for side, part in enumerate(parts)
            ],
            axis=1,
        )
        where = pl.ds(pl.multiple_of(z * tokens, tokens), tokens)
        proj_ref[where, :] = mm(hidden, wbuf[...]).astype(BF16)
        decay_low = mm(hidden, ddown_ref[...], NT).astype(BF16)
        decay_act = jnp.tanh(decay_low.astype(F32)).astype(BF16)
        learn_low = mm(hidden, edown_ref[...], NT).astype(BF16)
        spikes = jnp.concatenate(
            [
                jnp.broadcast_to(ebuf[z, pl.ds(2 * sp + place, 1), :], (HD, tokens))
                for place in range(2)
            ],
            axis=0,
        ).T
        for direction in range(2):
            pre = doff[direction : direction + 1] + mm(decay_act, dup[direction])
            softplus = jnp.maximum(-pre, 0.0) + jnp.log1p(jnp.exp(-jnp.abs(pre)))
            log_ref[direction, where, :] = spikes - jnp.exp(-softplus - 0.5)
            learn = eoff[direction : direction + 1] + mm(learn_low, eup[direction])
            learn_ref[direction, where, :] = jax.nn.sigmoid(learn)

    for k in range(depth - 1):
        at_distance(k, block)
    inner_only(of_step, sp)
    phase(o_step, 1)

    def m_block(part, k):
        z = flipped(sp, k)
        return remote(
            mix_ref.at[part, pl.ds(pl.multiple_of(z * tokens, tokens), tokens)],
            mbuf.at[part, sp],
            m_send.at[part, k - 1],
            m_recv.at[part, k - 1],
            {"sp": z},
        )

    def m_send_part(part):
        for k in range(1, depth):
            m_block(part, k).start()
        mbuf[part, sp] = mix_ref[part, pl.ds(pl.multiple_of(sp * tokens, tokens), tokens), :]

    plan = [
        ((x_step, depth - 1), (inner_only, o_step, far_z), (inner_only, of_step, last_z)),
        ((at_distance, depth - 1, block), (ends_only, of_step, next_z)),
        ((ends_only, o_step, far_z),),
        (),
        (),
        ((inner_only, of_step, next_z),),
        ((ends_only, o_step, last_z),),
        ((m_send_part, 0),),
        ((inner_only, of_step, far_z),),
        ((ends_only, of_step, far_z),),
        (),
    ]
    queue = iter(plan)

    def hook():
        for step, *arguments in next(queue, ()):
            step(*arguments)

    states = jnp.concatenate([init[d, h] for d in range(2) for h in range(2)], axis=1)
    mix_body(
        hook,
        proj_ref,
        log_ref,
        learn_ref,
        table_ref,
        head_gain_ref[:, cols],
        [sink_ref[0, head], sink_ref[0, head + 1]],
        states,
        mix_ref,
        *scratch,
    )

    m_send_part(1)
    ends_only(of_step, last_z)
    for part in range(2):
        for k in range(1, depth):
            m_block(part, k).wait_recv()
    lbuf[...] = jnp.concatenate(
        [mbuf[part, z] for part in range(2) for z in range(depth)], axis=1
    )
    kept = pl.ds(pl.multiple_of(tp * share, share), share)
    given = pl.ds(pl.multiple_of((1 - tp) * share, share), share)

    def part_move(z):
        return remote(
            pbuf.at[z, given], rbuf.at[z], part_send.at[z], part_recv.at[z], sibling
        )

    def product(z):
        pbuf[z] = mm(lbuf[...], owb[:, cols_of(z, 0, width)])
        part_move(z).start()

    def arrived(z):
        of_block(z).wait_recv()
        product(z)

    def total_of(z):
        part_move(z).wait_recv()
        out_ref[0, :, cols_of(z, 0, width)] = (pbuf[z, kept] + rbuf[z]).astype(BF16)

    arrived(sp)
    phase(arrived, 0)
    phase(arrived, 1)
    total_of(sp)
    phase(total_of, 0)
    phase(arrived, 2)
    phase(total_of, 1)
    phase(arrived, 3)
    phase(total_of, 2)
    phase(total_of, 3)

    for k in range(depth - 1):

        @pl.when((sp >= k) & up_exists)
        def _():
            for part in range(PARTS):
                x_up(sp, k, part).wait_send()
            o_up(sp, k).wait_send()

        @pl.when((sp < depth - k) & dn_exists)
        def _():
            for part in range(PARTS):
                x_dn(sp, k, part).wait_send()
            o_dn(sp, k).wait_send()

    for k in range(1, depth):
        wz_block(k).wait_send()
        e_block(k).wait_send()
    for k in range(depth):
        for side in range(2):
            p_block(k, side).wait_send()
            op_block(k, side).wait_send()
        f_block(k).wait_send()
        of_block(k).wait_send()
        part_move(k).wait_send()
        sib_move(k).wait_send()
    for part in range(2):
        for k in range(1, depth):
            m_block(part, k).wait_send()


def by_heads(
    inputs,
    input_norm_gain,
    receptance_weight,
    linear_key_weight,
    linear_value_weight,
    window_query_weight,
    window_key_weight,
    window_value_weight,
    decay_down_weight,
    decay_up_weight,
    decay_offset,
    decay_log_extra,
    erasure_down_weight,
    erasure_up_weight,
    erasure_offset,
    initial_state,
    head_norm_gain,
    query_sink_logit,
    linear_output_weight,
    window_output_weight,
):
    depth, width, sides = [lax.axis_size(axis) for axis in ("sp", "fs", "tp")]
    _, tokens, half = inputs.shape
    total = tokens * depth
    rows = receptance_weight.shape[0]
    out_rows, out_cols = linear_output_weight.shape
    features = out_cols * depth * width
    share = tokens // sides
    low = decay_down_weight.shape[1]
    dma = pltpu.SemaphoreType.DMA
    any_spec = pl.BlockSpec(memory_space=pl.ANY)
    vmem_spec = pl.BlockSpec(memory_space=pltpu.VMEM)
    return pl.pallas_call(
        layer_kernel,
        in_specs=[any_spec] * 11 + [pl.BlockSpec(memory_space=pltpu.SMEM)] + [vmem_spec] * 9,
        out_specs=vmem_spec,
        out_shape=jax.ShapeDtypeStruct((1, share, features), BF16),
        scratch_shapes=[
            pltpu.VMEM((depth, 2, tokens, half), BF16),
            pltpu.VMEM((2 * half, 5 * PAIR), BF16),
            pltpu.VMEM((2, rows, PAIR), BF16),
            pltpu.VMEM((depth, decay_log_extra.shape[1], tokens), F32),
            pltpu.VMEM((2, low, PAIR), BF16),
            pltpu.VMEM((2, low, PAIR), BF16),
            pltpu.VMEM((total, 5 * PAIR), BF16),
            pltpu.VMEM((2, total, PAIR), F32),
            pltpu.VMEM((2, total, PAIR), F32),
            pltpu.VMEM((2 * out_rows, features), BF16),
            pltpu.VMEM((2, depth, tokens, PAIR), BF16),
            pltpu.VMEM((2, total, PAIR), BF16),
            pltpu.VMEM((tokens, 2 * out_rows), BF16),
            pltpu.VMEM((depth, tokens, width * out_cols), F32),
            pltpu.VMEM((depth, share, width * out_cols), F32),
            pltpu.VMEM((2, 2, HD, HD), F32),
            dma((7,)),
            dma((4,)),
            dma((depth, PARTS)),
            dma((depth, PARTS)),
            dma((depth, PARTS)),
            dma((depth, PARTS)),
            dma((depth,)),
            dma((depth,)),
            dma((depth - 1,)),
            dma((depth - 1,)),
            dma((depth - 1,)),
            dma((depth - 1,)),
            dma((width, 2)),
            dma((width, 2)),
            dma((width,)),
            dma((width,)),
            dma((depth - 1,)),
            dma((depth - 1,)),
            dma((depth - 1,)),
            dma((depth - 1,)),
            dma((depth, 2)),
            dma((depth, 2)),
            dma((depth,)),
            dma((depth,)),
            dma((depth,)),
            dma((depth,)),
            dma((2, depth - 1)),
            dma((2, depth - 1)),
        ]
        + mix_scratch(total),
        compiler_params=pltpu.CompilerParams(
            collective_id=0, has_side_effects=True, vmem_limit_bytes=VMEM_GRANT
        ),
        name="layer",
    )(
        inputs,
        receptance_weight,
        linear_key_weight,
        linear_value_weight,
        window_query_weight,
        decay_log_extra,
        decay_up_weight,
        erasure_up_weight,
        linear_output_weight,
        window_output_weight,
        initial_state,
        query_sink_logit[None, :],
        window_key_weight,
        window_value_weight,
        input_norm_gain[None, :],
        decay_down_weight.T,
        erasure_down_weight.T,
        decay_offset,
        erasure_offset,
        jnp.asarray(rope_tables(total)),
        head_norm_gain[None, :],
    )


def layer(*arrays):
    inputs, recept, keys = arrays[0], arrays[2], arrays[6]
    depth, width, sides = [lax.axis_size(axis) for axis in ("sp", "fs", "tp")]
    fits = (
        recept.shape[1] == arrays[5].shape[1] == depth * PAIR
        and 2 * keys.shape[1] == depth * HD
        and (depth, width, sides) == (4, 4, 2)
        and inputs.shape[1] % WINDOW == 0
        and SPAN == GRID_W
    )
    return (by_heads if fits else local)(*arrays)


def solution(mesh):
    return jax.shard_map(
        layer,
        mesh=mesh,
        in_specs=(
            P("fs", "sp", "tp"),
            P(),
            P(("sp", "fs"), "tp"),
            P(("sp", "fs"), "tp"),
            P(("sp", "fs"), "tp"),
            P(("sp", "fs"), "tp"),
            P(("sp", "fs"), "tp"),
            P(("sp", "fs"), "tp"),
            P(),
            P(),
            P(),
            P("fs", "tp", "sp"),
            P(),
            P(),
            P(),
            P(),
            P(),
            P(),
            P("tp", ("sp", "fs")),
            P("tp", ("sp", "fs")),
        ),
        out_specs=P("fs", ("sp", "tp"), None),
        check_vma=False,
    )
```

```python
import jax
import jax.numpy as jnp
import numpy as np
from jax import lax
from jax.experimental import pallas as pl
from jax.experimental.pallas import tpu as pltpu
from jax.sharding import PartitionSpec as P

HD = 64
WINDOW = 128
GRID_W = 64
ATT_BLOCK = 128


NORM_EPS = 1e-06
GROUP_EPS = 0.00064
ROPE_BASE = 10000.0
HIGHEST = lax.Precision.HIGHEST


def padded(block, sides, width):
    for axis, dim in sides:
        count = lax.axis_size(axis)
        forward = [(i, i + 1) for i in range(count - 1)]
        backward = [(target, source) for source, target in forward]
        low = lax.ppermute(
            lax.slice_in_dim(block, block.shape[dim] - width, None, axis=dim), axis, forward
        )
        high = lax.ppermute(lax.slice_in_dim(block, 0, width, axis=dim), axis, backward)
        block = jnp.concatenate([low, block, high], axis=dim)
    return block


def to_bf16(array):
    return lax.optimization_barrier(array.astype(jnp.bfloat16))


def rope_axial(values, positions):
    quarter = values.shape[-1] // 4
    inverse = ROPE_BASE ** (-jnp.arange(quarter, dtype=jnp.float32) / quarter)
    grid_rows = (positions // GRID_W).astype(jnp.float32)
    grid_cols = (positions % GRID_W).astype(jnp.float32)
    pieces = []
    for which_half, coordinate in ((0, grid_rows), (1, grid_cols)):
        angles = coordinate[:, None] * inverse[None, :]
        cosine = jnp.cos(angles)[:, None, :]
        sine_part = jnp.sin(angles)[:, None, :]
        front_part = values[..., 2 * which_half * quarter : (2 * which_half + 1) * quarter]
        back_part = values[..., (2 * which_half + 1) * quarter : (2 * which_half + 2) * quarter]
        pieces.append(front_part * cosine - back_part * sine_part)
        pieces.append(front_part * sine_part + back_part * cosine)
    return jnp.concatenate(pieces, axis=-1)


CHUNK = 32
PAIR = 2 * HD
F32 = jnp.float32
BF16 = jnp.bfloat16
NN = (((1,), (0,)), ((), ()))
NT = (((1,), (1,)), ((), ()))


def dot1(left, right, dims=NN):
    return lax.dot_general(
        left.astype(jnp.bfloat16), right.astype(jnp.bfloat16), dims, preferred_element_type=F32
    )


def halves(value):
    high = value.astype(jnp.bfloat16)
    return high, (value - high.astype(F32)).astype(jnp.bfloat16)


def dot3(left, right, dims=NN):
    left_high, left_low = halves(left)
    right_high, right_low = halves(right)

    def product(one, other):
        return lax.dot_general(one, other, dims, preferred_element_type=F32)

    return product(left_high, right_high) + (
        product(left_high, right_low) + product(left_low, right_high)
    )


def full_dot(left, right):
    return lax.dot_general(left, right, NN, precision=HIGHEST, preferred_element_type=F32)


def chunk_kernel(read_ref, key_ref, value_ref, log_ref, learn_ref, out_ref, end_ref):
    tokens = read_ref.shape[0]
    read = read_ref[...].astype(F32)
    key = key_ref[...].astype(F32)
    value = value_ref[...].astype(F32)
    first = lax.broadcasted_iota(jnp.int32, (tokens, PAIR), 1) < HD
    pair_i = lax.broadcasted_iota(jnp.int32, (PAIR, PAIR), 0)
    pair_j = lax.broadcasted_iota(jnp.int32, (PAIR, PAIR), 1)
    same_head = jnp.where(pair_i // HD == pair_j // HD, 1.0, 0.0)
    row = lax.broadcasted_iota(jnp.int32, (tokens, tokens), 0)
    col = lax.broadcasted_iota(jnp.int32, (tokens, tokens), 1)
    same_chunk = row // CHUNK == col // CHUNK
    eye = jnp.where(row == col, 1.0, 0.0)
    unit = key * lax.rsqrt(full_dot(key * key, same_head) + NORM_EPS)
    own = (first, jnp.logical_not(first))
    values = (
        jnp.where(first, value, 0.0),
        jnp.where(first, pltpu.roll(value, HD, 1), 0.0),
    )
    all_chunk = jnp.where(same_chunk, 1.0, 0.0)
    for direction in range(2):
        before = (col < row) if direction == 0 else (col > row)
        strict = same_chunk & before
        upto = same_chunk & (before | (col == row))
        log_decay = log_ref[direction]
        erase = unit * learn_ref[direction]
        total_log = full_dot(jnp.where(upto, 1.0, 0.0), log_decay)
        chunk_log = full_dot(all_chunk, log_decay)
        prior_log = total_log - log_decay
        middle = 0.5 * chunk_log
        unit_start = jnp.exp(prior_log) * unit
        unit_mid = jnp.exp(prior_log - middle) * unit
        read_start = jnp.exp(total_log) * read
        read_mid = jnp.exp(total_log - middle) * read
        inverse = jnp.exp(middle - total_log)
        sources = jnp.concatenate([erase * inverse, key * inverse], axis=0)
        rest = jnp.exp(chunk_log - total_log)
        key_rest = key * rest
        erase_rest = erase * rest
        chunk_decay = jnp.exp(chunk_log).T
        solved, offsets, mixes = [], [], []
        for head in range(2):
            readers = jnp.concatenate(
                [jnp.where(own[head], unit_mid, 0.0), jnp.where(own[head], read_mid, 0.0)], axis=0
            )
            meets = dot3(readers, sources, NT)
            erased = jnp.where(strict, meets[:tokens, :tokens], 0.0)
            seen = jnp.where(strict, meets[:tokens, tokens:], 0.0)
            read_erased = jnp.where(upto, meets[tokens:, :tokens], 0.0)
            read_seen = jnp.where(upto, meets[tokens:, tokens:], 0.0)
            solve = eye - jnp.where(row // 2 == col // 2, erased, 0.0)
            size = 2
            while size < CHUNK:
                level = (row // (2 * size) == col // (2 * size)) & (row // size != col // size)
                solve = solve - dot1(dot1(solve, jnp.where(level, erased, 0.0)), solve)
                size *= 2
            solve = solve + dot1(solve, eye - solve - dot3(erased, solve))
            both = dot3(
                solve,
                jnp.concatenate(
                    [jnp.where(own[head], unit_start, 0.0), dot3(seen, values[head])], axis=1
                ),
            )
            solved.append(both[:, :PAIR])
            offsets.append(both[:, PAIR:])
            mixes.append(jnp.concatenate([read_seen, -read_erased], axis=1))
        state = jnp.where(pair_j == HD + pair_i % HD, 1.0, 0.0)
        count = tokens // CHUNK
        drops = [[None] * count, [None] * count]
        reads = [[None] * count, [None] * count]
        for step in range(count):
            place = step if direction == 0 else count - 1 - step
            rows = slice(place * CHUNK, (place + 1) * CHUNK)
            lefts = jnp.concatenate(
                [solved[0][rows], solved[1][rows]]
                + [jnp.where(own[head], read_start, 0.0)[rows] for head in range(2)],
                axis=0,
            )
            seen_state = dot3(lefts, state)
            for head in range(2):
                drops[head][place] = (
                    seen_state[head * CHUNK : (head + 1) * CHUNK] + offsets[head][rows]
                )
                reads[head][place] = seen_state[(2 + head) * CHUNK : (3 + head) * CHUNK]
            adders = jnp.concatenate(
                [jnp.where(own[head], key_rest, 0.0)[rows] for head in range(2)]
                + [jnp.where(own[head], -erase_rest, 0.0)[rows] for head in range(2)],
                axis=0,
            ).T
            added = jnp.concatenate(
                [values[0][rows], values[1][rows], drops[0][place], drops[1][place]], axis=0
            )
            first_col = place * CHUNK
            state = chunk_decay[:, first_col : first_col + 1] * state + dot3(adders, added)
        for head in range(2):
            dropped = jnp.concatenate(drops[head], axis=0)
            out_ref[direction, head] = jnp.concatenate(reads[head], axis=0) + dot3(
                mixes[head], jnp.concatenate([values[head], dropped], axis=0)
            )
        end_ref[direction] = state


def chunked(returned, log_decay, learn, head_width):
    tokens = returned.shape[0]
    pairs = head_width // PAIR

    def role(which):
        return pl.BlockSpec((tokens, PAIR), lambda p: (0, which * pairs + p))

    wide = pl.BlockSpec((2, tokens, PAIR), lambda p: (0, 0, p))
    return pl.pallas_call(
        chunk_kernel,
        grid=(pairs,),
        in_specs=[role(0), role(1), role(2), wide, wide],
        out_specs=[
            pl.BlockSpec((2, 2, tokens, PAIR), lambda p: (0, p, 0, 0)),
            pl.BlockSpec((2, PAIR, PAIR), lambda p: (0, p, 0)),
        ],
        out_shape=[
            jax.ShapeDtypeStruct((2, 2 * pairs, tokens, PAIR), F32),
            jax.ShapeDtypeStruct((2, pairs * PAIR, PAIR), F32),
        ],
        cost_estimate=pl.CostEstimate(
            flops=pairs * 400 * PAIR**3, bytes_accessed=8 * tokens * head_width * 4, transcendentals=0
        ),
        name="chunked_state",
    )(returned, returned, returned, log_decay, learn)


def merge_kernel(local_ref, state_ref, gain_ref, out_ref):
    pair_i = lax.broadcasted_iota(jnp.int32, (PAIR, PAIR), 0)
    pair_j = lax.broadcasted_iota(jnp.int32, (PAIR, PAIR), 1)
    average = jnp.where(pair_i // HD == pair_j // HD, 1.0 / HD, 0.0)
    sums = []
    for head in range(2):
        total = 0.0
        for direction in range(2):
            block = local_ref[direction, head]
            total = total + (
                block[:, :HD] + dot3(block[:, HD:], state_ref[direction, head])
            )
        sums.append(total)
    lin_sum = jnp.concatenate(sums, axis=1)
    centred = lin_sum - full_dot(lin_sum, average)
    normed = centred * lax.rsqrt(full_dot(centred * centred, average) + GROUP_EPS)
    out_ref[...] = (normed * gain_ref[...]).astype(jnp.bfloat16)


def merged(local_out, entry, gain):
    _, head_count, tokens, _ = local_out.shape
    pairs = head_count // 2
    return pl.pallas_call(
        merge_kernel,
        grid=(pairs,),
        in_specs=[
            pl.BlockSpec((2, 2, tokens, PAIR), lambda p: (0, p, 0, 0)),
            pl.BlockSpec((2, 2, HD, HD), lambda p: (0, p, 0, 0)),
            pl.BlockSpec((1, PAIR), lambda p: (0, p)),
        ],
        out_specs=pl.BlockSpec((tokens, PAIR), lambda p: (0, p)),
        out_shape=jax.ShapeDtypeStruct((tokens, head_count * HD), jnp.bfloat16),
        cost_estimate=pl.CostEstimate(
            flops=pairs * 30 * PAIR**3, bytes_accessed=4 * tokens * head_count * PAIR * 4, transcendentals=0
        ),
        name="merged_norm",
    )(local_out, entry, gain[None, :])


def entering_states(ends, initial):
    count = lax.axis_size("sp")
    place = lax.axis_index("sp")
    ups = [(i, i + 1) for i in range(count - 1)]
    downs = [(i + 1, i) for i in range(count - 1)]
    adds, maps = ends[..., :HD], ends[..., HD:]

    def hop(_, states):
        later = jnp.einsum("dhkj,dhjv->dhkv", maps, states, precision=HIGHEST) + adds
        forward = lax.ppermute(later[0], "sp", ups)
        backward = lax.ppermute(later[1], "sp", downs)
        return jnp.stack(
            [
                jnp.where(place == 0, initial[0], forward),
                jnp.where(place == count - 1, initial[1], backward),
            ]
        )

    states = initial
    if count > 8:
        return lax.fori_loop(0, count - 1, hop, states)
    for _ in range(count - 1):
        states = hop(0, states)
    return states


def swapped(block, axis):
    count = lax.axis_size(axis)
    return [block] + [
        lax.ppermute(block, axis, [(i, i ^ flip) for i in range(count)]) for flip in range(1, count)
    ]


def in_order(pieces, axis):
    me = lax.axis_index(axis)
    stacked = jnp.stack(pieces)
    return [
        lax.dynamic_index_in_dim(stacked, me ^ place, 0, False) for place in range(len(pieces))
    ]


def local(
    inputs,
    input_norm_gain,
    receptance_weight,
    linear_key_weight,
    linear_value_weight,
    window_query_weight,
    window_key_weight,
    window_value_weight,
    decay_down_weight,
    decay_up_weight,
    decay_offset,
    decay_log_extra,
    erasure_down_weight,
    erasure_up_weight,
    erasure_offset,
    initial_state,
    head_norm_gain,
    query_sink_logit,
    linear_output_weight,
    window_output_weight,
):
    tokens = inputs.shape[1]
    tp_index = lax.axis_index("tp")
    length = tokens * lax.axis_size("sp")
    offset = lax.axis_index("sp") * tokens
    gathered = lax.all_gather(inputs, "tp", axis=2, tiled=True)[0]
    widened = gathered.astype(jnp.float32)
    hidden = to_bf16(
        widened
        * lax.rsqrt(jnp.mean(widened * widened, axis=-1, keepdims=True) + NORM_EPS)
        * input_norm_gain
    )
    weights = (
        receptance_weight,
        linear_key_weight,
        linear_value_weight,
        window_query_weight,
        window_key_weight,
        window_value_weight,
    )
    widths = [weight.shape[1] for weight in weights]
    joined = jnp.concatenate(weights, axis=1)
    regrouped = lax.all_to_all(joined, "fs", split_axis=1, concat_axis=0, tiled=True)
    every_seq = jnp.concatenate(swapped(hidden, "fs"), axis=0)
    near_cols = jnp.concatenate(in_order(swapped(window_output_weight, "fs"), "fs"), axis=1)
    whole_cols = lax.all_gather(regrouped, "sp", axis=0, tiled=True)
    partial_cols = jnp.dot(every_seq, whole_cols, preferred_element_type=jnp.float32)
    by_seq = to_bf16(partial_cols).reshape(-1, tokens, partial_cols.shape[1])
    outgoing = jnp.concatenate(in_order(list(by_seq), "fs"), axis=0)
    returned = lax.all_to_all(outgoing, "fs", split_axis=0, concat_axis=1, tiled=True)
    bounds = [0]
    for col_width in widths:
        bounds.append(bounds[-1] + col_width)
    projected = [returned[:, bounds[role_idx] : bounds[role_idx + 1]] for role_idx in range(6)]
    recept, lin_keys, lin_values, queries, att_keys, att_values = projected
    head_width = recept.shape[1]
    head_count = head_width // HD
    first_col = tp_index * head_width
    up_decay = lax.dynamic_slice_in_dim(decay_up_weight, first_col, head_width, 2)
    up_learn = lax.dynamic_slice_in_dim(erasure_up_weight, first_col, head_width, 2)
    base_decay = lax.dynamic_slice_in_dim(decay_offset, first_col, head_width, 1)
    base_learn = lax.dynamic_slice_in_dim(erasure_offset, first_col, head_width, 1)
    gain_local = lax.dynamic_slice_in_dim(head_norm_gain, first_col, head_width, 0)
    state_local = lax.dynamic_slice_in_dim(initial_state, tp_index * head_count, head_count, 1)
    spread = (
        jnp.arange(head_count)[:, None] == jnp.arange(head_width)[None, :] // HD
    ).astype(jnp.float32)
    decay_spikes = jnp.einsum("ht,hc->tc", decay_log_extra[0], spread, precision=HIGHEST)
    decay_low = to_bf16(jnp.dot(hidden, decay_down_weight, preferred_element_type=jnp.float32))
    decay_act = to_bf16(jnp.tanh(decay_low.astype(jnp.float32)))
    learn_low = to_bf16(jnp.dot(hidden, erasure_down_weight, preferred_element_type=jnp.float32))
    pre_decay = base_decay[:, None, :] + jnp.einsum(
        "tl,dlc->dtc", decay_act, up_decay, preferred_element_type=jnp.float32
    )
    log_decay = decay_spikes[None] - jnp.exp(-jax.nn.softplus(-pre_decay) - 0.5)
    learn = jax.nn.sigmoid(
        base_learn[:, None, :]
        + jnp.einsum("tl,dlc->dtc", learn_low, up_learn, preferred_element_type=jnp.float32)
    )
    local_out, ends = chunked(returned, log_decay, learn, head_width)
    entry = entering_states(
        ends.reshape(2, head_count, HD, PAIR), jnp.swapaxes(state_local, -1, -2)
    )
    lin_mix = merged(local_out, entry, gain_local)
    positions = offset + jnp.arange(tokens, dtype=jnp.int32)
    query_count = queries.shape[1] // HD
    group_count = att_keys.shape[1] // HD
    group_size = query_count // group_count
    roped_q = rope_axial(
        queries.astype(jnp.float32).reshape(tokens, query_count, HD), positions
    ).astype(jnp.bfloat16)
    roped_k = rope_axial(
        att_keys.astype(jnp.float32).reshape(tokens, group_count, HD), positions
    ).astype(jnp.bfloat16)
    kv_width = group_count * HD
    packed = jnp.concatenate([roped_k.reshape(tokens, kv_width), att_values], axis=1)
    bordered = padded(packed, (("sp", 0),), WINDOW)
    sink_local = lax.dynamic_slice_in_dim(
        query_sink_logit, tp_index * query_count, query_count, 0
    ).reshape(group_count, group_size)[:, :, None, None]
    reach = ATT_BLOCK + 2 * WINDOW
    query_rows = roped_q.reshape(ATT_BLOCK, group_count, group_size, HD)
    key_rows = bordered[:, :kv_width].reshape(reach, group_count, HD)
    value_rows = bordered[:, kv_width:].reshape(reach, group_count, HD)
    scores = jnp.einsum(
        "qgrd,kgd->grqk", query_rows, key_rows, preferred_element_type=jnp.float32
    ) * HD ** (-0.5)
    query_pos = offset + 0 + jnp.arange(ATT_BLOCK, dtype=jnp.int32)
    key_pos = offset + 0 - WINDOW + jnp.arange(reach, dtype=jnp.int32)
    allowed = (
        (jnp.abs(query_pos[:, None] - key_pos[None, :]) <= WINDOW)
        & (key_pos[None, :] >= 0)
        & (key_pos[None, :] < length)
    )
    scores = jnp.where(allowed, scores, -jnp.inf)
    top_score = jnp.maximum(jnp.max(scores, axis=-1, keepdims=True), sink_local)
    raised = jnp.exp(scores - top_score)
    denominator = jnp.exp(sink_local - top_score) + jnp.sum(raised, axis=-1, keepdims=True)
    weights_bf = (raised / denominator).astype(jnp.bfloat16)
    mixed = jnp.einsum("grqk,kgd->qgrd", weights_bf, value_rows, preferred_element_type=jnp.float32)
    outputs = mixed.astype(jnp.bfloat16).reshape(ATT_BLOCK, query_count * HD)
    lin_weight = lax.all_gather(linear_output_weight, ("sp", "fs"), axis=1, tiled=True)
    if lax.axis_size("sp") > 8:
        att_out = jnp.dot(
            outputs,
            lax.all_gather(near_cols, "sp", axis=1, tiled=True),
            preferred_element_type=jnp.float32,
        )
    else:
        att_parts = [
            jnp.dot(outputs, part, preferred_element_type=jnp.float32)
            for part in swapped(near_cols, "sp")
        ]
        att_out = jnp.concatenate(in_order(att_parts, "sp"), axis=1)
    layer_out = lax.psum_scatter(
        jnp.dot(lin_mix, lin_weight, preferred_element_type=jnp.float32) + att_out,
        "tp",
        scatter_dimension=0,
        tiled=True,
    )
    return layer_out.astype(jnp.bfloat16)[None]


SPAN = HD
PARTS = 2
ORDER = (1, 3, 2)
VMEM_GRANT = 67_000_000
QUAD = 4 * HD
TN = (((0,), (0,)), ((), ()))


def mm(left, right, dims=NN):
    return lax.dot_general(left, right, dims, preferred_element_type=F32)


def rope_tables(total):
    quarter = HD // 4
    inverse = ROPE_BASE ** (-np.arange(quarter, dtype=np.float32) / np.float32(quarter))
    inverse = inverse.astype(np.float32)
    lane = np.arange(PAIR) % HD
    rates = inverse[lane % quarter]
    sign = np.where(lane % (2 * quarter) < quarter, -1.0, 1.0)
    coords = np.concatenate([np.arange(total // GRID_W), np.arange(GRID_W)])
    angles = (coords.astype(np.float32)[:, None] * rates[None, :]).astype(np.float64)
    return np.stack([np.cos(angles), np.sin(angles) * sign]).astype(np.float32)


def mix_body(
    hook, proj_ref, log_ref, learn_ref, table_ref, gain, sinks, states, mix_ref, s_w, s_read, s_m, s_a, s_local, s_re, s_lin, kpad, vpad, s_q
):
    total = proj_ref.shape[0]
    count = total // SPAN
    lane = lax.broadcasted_iota(jnp.int32, (SPAN, PAIR), 1)
    first = lane < HD
    ones = (
        jnp.where(first, 1.0, 0.0).astype(BF16),
        jnp.where(first, 0.0, 1.0).astype(BF16),
    )
    nothing = jnp.zeros((SPAN, PAIR), BF16)
    quad_row = lax.broadcasted_iota(jnp.int32, (SPAN, QUAD), 0)
    quad_lane = lax.broadcasted_iota(jnp.int32, (SPAN, QUAD), 1)
    quad_col = lax.rem(quad_lane, HD)
    ahead = quad_lane < PAIR
    before = jnp.where(ahead, quad_col - quad_row, quad_row - quad_col)
    strict, upto = before < 0, before <= 0
    eye = jnp.where(before == 0, 1.0, 0.0)

    def level(size):
        return (lax.div(quad_row, 2 * size) == lax.div(quad_col, 2 * size)) & (
            lax.div(quad_row, size) != lax.div(quad_col, size)
        )

    square_i = lax.broadcasted_iota(jnp.int32, (QUAD, QUAD), 0)
    square_j = lax.broadcasted_iota(jnp.int32, (QUAD, QUAD), 1)
    same_unit = lax.div(square_i, HD) == lax.div(square_j, HD)
    square_eye = square_i == square_j
    tri_i = lax.broadcasted_iota(jnp.int32, (SPAN, SPAN), 0)
    tri_j = lax.broadcasted_iota(jnp.int32, (SPAN, SPAN), 1)
    tri = [
        jnp.where(tri_j <= tri_i, 1.0, 0.0).astype(BF16),
        jnp.where(tri_j >= tri_i, 1.0, 0.0).astype(BF16),
    ]
    tri = [jnp.concatenate([one] * 3, axis=1) for one in tri]

    def diagonal(quad):
        left, right = quad[:, :PAIR], quad[:, PAIR:]
        return jnp.concatenate(
            [jnp.concatenate([left * one, nothing], axis=1) for one in ones]
            + [jnp.concatenate([nothing, right * one], axis=1) for one in ones],
            axis=0,
        )

    def quad_dot(lefts, right, dims=NN):
        highs, lows = zip(*[halves(left) for left in lefts])
        right_high, right_low = halves(right)
        count_left = len(lefts)
        outer = mm(jnp.concatenate(highs + lows, axis=0), diagonal(right_high), dims)
        inner = mm(jnp.concatenate(highs, axis=0), diagonal(right_low), dims)
        return [
            outer[k * SPAN : (k + 1) * SPAN]
            + (
                outer[(count_left + k) * SPAN : (count_left + k + 1) * SPAN]
                + inner[k * SPAN : (k + 1) * SPAN]
            )
            for k in range(count_left)
        ]

    def single(left, right):
        return mm(left.astype(BF16), diagonal(right.astype(BF16)))

    def rows_at(place):
        return pl.ds(pl.multiple_of(place * SPAN, SPAN), SPAN)

    def head_sum(value):
        low = jnp.sum(jnp.where(first, value, 0.0), axis=1, keepdims=True)
        high = jnp.sum(jnp.where(first, 0.0, value), axis=1, keepdims=True)
        return jnp.where(first, low, high)

    def prepare(direction, rows):
        read = proj_ref[rows, :PAIR].astype(F32)
        key = proj_ref[rows, PAIR : 2 * PAIR].astype(F32)
        log_decay = log_ref[direction, rows, :]
        unit = key * lax.rsqrt(head_sum(key * key) + NORM_EPS)
        erase = unit * learn_ref[direction, rows, :]
        high = log_decay.astype(BF16)
        rest = log_decay - high.astype(F32)
        middle_part = rest.astype(BF16)
        low = (rest - middle_part.astype(F32)).astype(BF16)
        total_log = mm(tri[direction], jnp.concatenate([high, middle_part, low], axis=0))
        end = SPAN - 1 if direction == 0 else 0
        span_log = total_log[end : end + 1, :]
        middle = 0.5 * span_log
        prior_log = total_log - log_decay
        inverse = jnp.exp(middle - total_log)
        left = jnp.exp(span_log - total_log)
        readers = jnp.concatenate(
            [jnp.exp(prior_log - middle) * unit, jnp.exp(total_log - middle) * read], axis=0
        )
        sources = jnp.concatenate([erase * inverse, key * inverse], axis=0)
        high_r, low_r = halves(readers)
        high_s, low_s = halves(sources)

        def spread(value):
            top, bottom = value[:SPAN], value[SPAN:]
            return jnp.concatenate([top * one for one in ones] + [bottom * one for one in ones], axis=0)

        high_s, low_s = spread(high_s), spread(low_s)
        meets = mm(
            jnp.concatenate([high_r, low_r, high_r], axis=1),
            jnp.concatenate([high_s, high_s, low_s], axis=1),
            NT,
        )
        return (
            meets,
            jnp.exp(prior_log) * unit,
            jnp.exp(total_log) * read,
            key * left,
            erase * left,
            jnp.exp(span_log),
        )

    def both(one, other):
        return jnp.concatenate([one, other], axis=1)

    def batch(groups):
        erased, seens, read_eraseds, starts, lefts, finals, spans, values = [], [], [], [], [], [], [], []
        for group in groups:
            rows = (rows_at(group), rows_at(count - 1 - group))
            parts = [prepare(direction, rows[direction]) for direction in range(2)]
            meets = [part[0] for part in parts]
            value = both(*[proj_ref[row, 2 * PAIR : 3 * PAIR] for row in rows])
            erased.append(
                jnp.where(strict, both(meets[0][:SPAN, :PAIR], meets[1][:SPAN, :PAIR]), 0.0)
            )
            seen = jnp.where(strict, both(meets[0][:SPAN, PAIR:], meets[1][:SPAN, PAIR:]), 0.0)
            s_re[group] = jnp.where(
                upto, both(meets[0][SPAN:, :PAIR], meets[1][SPAN:, :PAIR]), 0.0
            )
            read_seen = jnp.where(upto, both(meets[0][SPAN:, PAIR:], meets[1][SPAN:, PAIR:]), 0.0)
            starts.append(both(parts[0][1], parts[1][1]))
            s_read[group] = both(parts[0][2], parts[1][2])
            lefts.append((both(parts[0][3], parts[1][3]), both(parts[0][4], parts[1][4])))
            spans.append(both(parts[0][5], parts[1][5]))
            values.append(value)
            pieces = jnp.concatenate([*halves(seen), *halves(read_seen)], axis=0)
            met = mm(pieces, diagonal(value))
            seens.append(met[:SPAN] + met[SPAN : 2 * SPAN])
            s_local[group] = met[2 * SPAN : 3 * SPAN] + met[3 * SPAN :]
        solves = [eye - jnp.where(level(1), one, 0.0) for one in erased]
        width = 2
        while width < SPAN:
            at = level(width)
            firsts = [single(solve, jnp.where(at, one, 0.0)) for solve, one in zip(solves, erased)]
            solves = [solve - single(one, solve) for solve, one in zip(solves, firsts)]
            width *= 2
        hook()
        misses = [
            eye - solve - quad_dot([one], solve)[0] for solve, one in zip(solves, erased)
        ]
        solves = [solve + single(solve, miss) for solve, miss in zip(solves, misses)]
        maps = [quad_dot([solve], start)[0] for solve, start in zip(solves, starts)]
        shifts = [quad_dot([solve], seen)[0] for solve, seen in zip(solves, seens)]
        for place, group in enumerate(groups):
            key_left, erase_left = lefts[place]
            s_w[group] = jnp.concatenate([maps[place], shifts[place]], axis=1)
            map_high, map_low = halves(maps[place])
            left_high, left_low = halves(erase_left)
            fade = mm(
                jnp.concatenate([map_high, map_low, map_high], axis=0),
                jnp.concatenate([left_high, left_high, left_low], axis=0),
                TN,
            )
            s_m[group] = jnp.where(square_eye, spans[place], 0.0) - jnp.where(same_unit, fade, 0.0)
            shift_high, shift_low = halves(shifts[place])
            key_high, key_low = halves(key_left)
            gained = mm(
                jnp.concatenate(
                    [values[place], values[place], shift_high, shift_low, shift_high], axis=0
                ),
                jnp.concatenate(
                    [key_high, key_low, -left_high, -left_high, -left_low], axis=0
                ),
                TN,
            )
            gained = jnp.where(same_unit, gained, 0.0)
            s_a[group] = (gained[:SPAN] + gained[SPAN : 2 * SPAN]) + (
                gained[2 * SPAN : 3 * SPAN] + gained[3 * SPAN :]
            )

    size = count // 2
    middle = range(count // 4, count - count // 4)
    batch(list(middle))
    hook()
    batch([group for group in range(count) if group not in middle])
    hook()

    def advance(group, state):
        high, low = halves(state)
        step_high, step_low = halves(s_m[group])
        outer = mm(jnp.concatenate([high, low], axis=0), step_high)
        inner = mm(high, step_low)
        following = outer[:SPAN] + (outer[SPAN:] + inner) + s_a[group]
        s_a[group] = state
        return following

    state = states
    for group in range(count):
        state = advance(group, state)
    hook()

    def finish(group, carry):
        maps, shift = s_w[group, :, :QUAD], s_w[group, :, QUAD:]
        dropped, seen_state = quad_dot([maps, s_read[group]], s_a[group], NT)
        dropped = dropped + shift
        out = seen_state + s_local[group] - quad_dot([s_re[group]], dropped)[0]
        s_lin[0, rows_at(group), :] = out[:, :PAIR]
        s_lin[1, rows_at(count - 1 - group), :] = out[:, PAIR:]
        return carry

    def finish_batch(index, carry):
        for k in range(size):
            carry = finish(index * size + k, carry)
        return carry

    for index in range(count // size):
        finish_batch(index, 0)
        hook()

    def norm(place, carry):
        rows = rows_at(place)
        lin_sum = s_lin[0, rows, :] + s_lin[1, rows, :]
        centred = lin_sum - head_sum(lin_sum) * (1.0 / HD)
        spread = head_sum(centred * centred) * (1.0 / HD)
        mix_ref[0, rows, :] = (centred * lax.rsqrt(spread + GROUP_EPS) * gain).astype(BF16)
        return carry

    lax.fori_loop(0, count, norm, 0)
    hook()

    quarter = HD // 4
    back = lax.rem(lane, 2 * quarter) >= quarter
    by_row = lax.rem(lane, HD) < 2 * quarter
    grid = total // GRID_W
    edge = jnp.zeros((WINDOW, PAIR), BF16)
    for ref in (kpad, vpad):
        ref[:WINDOW, :] = edge
        ref[WINDOW + total :, :] = edge

    def turned(value, cosine, sine):
        partner = jnp.where(
            back, pltpu.roll(value, quarter, 1), pltpu.roll(value, PAIR - quarter, 1)
        )
        return value * cosine + partner * sine

    def turn(place, carry):
        rows = rows_at(place)
        cosine, sine = [
            jnp.where(
                by_row,
                table_ref[which, pl.ds(place, 1), :],
                table_ref[which, grid : grid + GRID_W, :],
            )
            for which in range(2)
        ]
        query = proj_ref[rows, 3 * PAIR : 4 * PAIR].astype(F32)
        pair = proj_ref[rows, 4 * PAIR :].astype(F32)
        s_q[rows, :] = turned(query, cosine, sine).astype(BF16)
        key = jnp.where(first, turned(pair, cosine, sine), 0.0)
        value = jnp.where(first, 0.0, pair)
        there = pl.ds(pl.multiple_of(WINDOW + place * SPAN, SPAN), SPAN)
        kpad[there, :] = (key + pltpu.roll(key, HD, 1)).astype(BF16)
        vpad[there, :] = (value + pltpu.roll(value, HD, 1)).astype(BF16)
        return carry

    lax.fori_loop(0, grid, turn, 0)
    hook()
    reach = ATT_BLOCK + 2 * WINDOW
    ahead_of = lax.broadcasted_iota(jnp.int32, (ATT_BLOCK, reach), 1) - (
        WINDOW + lax.broadcasted_iota(jnp.int32, (ATT_BLOCK, reach), 0)
    )
    near = jnp.abs(ahead_of) <= WINDOW
    key_at = lax.broadcasted_iota(jnp.int32, (ATT_BLOCK, reach), 1) - WINDOW
    mine = lax.broadcasted_iota(jnp.int32, (ATT_BLOCK, PAIR), 1) < HD

    def attend(place, carry):
        start = pl.multiple_of(place * ATT_BLOCK, ATT_BLOCK)
        rows = pl.ds(start, ATT_BLOCK)
        query = s_q[rows, :]
        keys = kpad[pl.ds(start, reach), :]
        held = vpad[pl.ds(start, reach), :]
        allowed = near & (key_at >= -start) & (key_at < total - start)
        mixed = []
        for head in range(2):
            own = jnp.where(mine if head == 0 else jnp.logical_not(mine), query.astype(F32), 0.0)
            scores = mm(own.astype(BF16), keys, NT) * HD ** (-0.5)
            scores = jnp.where(allowed, scores, -jnp.inf)
            top = jnp.maximum(jnp.max(scores, axis=1, keepdims=True), sinks[head])
            raised = jnp.exp(scores - top)
            bottom = jnp.exp(sinks[head] - top) + jnp.sum(raised, axis=1, keepdims=True)
            mixed.append(mm((raised / bottom).astype(BF16), held))
        mix_ref[1, rows, :] = jnp.where(mine, mixed[0], mixed[1]).astype(BF16)
        return carry

    blocks = total // ATT_BLOCK
    for part in range(2):
        lax.fori_loop(part * blocks // 2, (part + 1) * blocks // 2, attend, 0)
        hook()


def mix_scratch(total):
    count = total // SPAN
    return [
        pltpu.VMEM((count, SPAN, 2 * QUAD), F32),
        pltpu.VMEM((count, SPAN, QUAD), F32),
        pltpu.VMEM((count, QUAD, QUAD), F32),
        pltpu.VMEM((count, SPAN, QUAD), F32),
        pltpu.VMEM((count, SPAN, QUAD), F32),
        pltpu.VMEM((count, SPAN, QUAD), F32),
        pltpu.VMEM((2, total, PAIR), F32),
        pltpu.VMEM((total + 2 * WINDOW, PAIR), BF16),
        pltpu.VMEM((total + 2 * WINDOW, PAIR), BF16),
        pltpu.VMEM((total, PAIR), BF16),
    ]


MESH_IDS = pl.DeviceIdType.MESH


def flipped(index, bits):
    result = index
    for bit in (1, 2):
        if bits & bit:
            result = result + bit - 2 * bit * lax.rem(lax.div(index, bit), 2)
    return result


def remote(src, dst, send, recv, device):
    return pltpu.make_async_remote_copy(
        src_ref=src,
        dst_ref=dst,
        send_sem=send,
        recv_sem=recv,
        device_id=device,
        device_id_type=MESH_IDS,
    )


def layer_kernel(
    x_ref,
    wr_ref,
    wk_ref,
    wv_ref,
    wq_ref,
    extra_ref,
    dup_ref,
    eup_ref,
    lin_ref,
    win_ref,
    init_ref,
    sink_ref,
    ak_ref,
    av_ref,
    gain_ref,
    ddown_ref,
    edown_ref,
    doff_ref,
    eoff_ref,
    table_ref,
    head_gain_ref,
    out_ref,
    xbuf,
    wbuf,
    kvbuf,
    ebuf,
    dup,
    eup,
    proj_ref,
    log_ref,
    learn_ref,
    owb,
    mbuf,
    mix_ref,
    lbuf,
    pbuf,
    rbuf,
    init,
    local_sem,
    wlocal_sem,
    up_send,
    up_recv,
    dn_send,
    dn_recv,
    sib_send,
    sib_recv,
    wz_send,
    wz_recv,
    e_send,
    e_recv,
    p_send,
    p_recv,
    f_send,
    f_recv,
    ou_send,
    ou_recv,
    od_send,
    od_recv,
    op_send,
    op_recv,
    of_send,
    of_recv,
    part_send,
    part_recv,
    m_send,
    m_recv,
    *scratch,
):
    sp, fs, tp = lax.axis_index("sp"), lax.axis_index("fs"), lax.axis_index("tp")
    depth, width, sides = [lax.axis_size(axis) for axis in ("sp", "fs", "tp")]
    tokens = x_ref.shape[1]
    rows = wr_ref.shape[0]
    out_rows, out_cols = lin_ref.shape
    share = out_ref.shape[1]
    sibling = {"tp": 1 - tp}
    plane = ({"fs": flipped(fs, 1)}, {"fs": flipped(fs, 2)})
    up_to, dn_to = {"sp": sp + 1}, {"sp": sp - 1}

    def rows_of(z, f):
        return pl.ds(pl.multiple_of((z * width + f) * rows, rows), rows)

    def cols_of(z, f, many=1):
        return pl.ds(pl.multiple_of((z * width + f) * out_cols, out_cols), many * out_cols)

    def pieces(z):
        low = pl.ds(pl.multiple_of(z * PAIR, PAIR), PAIR)
        return [ref.at[:, low] for ref in (wr_ref, wk_ref, wv_ref, wq_ref)]

    def lanes(place):
        return slice(place * PAIR, (place + 1) * PAIR)

    cols = pl.ds(pl.multiple_of((tp * depth + sp) * PAIR, PAIR), PAIR)
    head = (tp * depth + sp) * 2
    own_x = pltpu.make_async_copy(x_ref.at[0], xbuf.at[sp, tp], local_sem.at[0])
    own_w = [
        pltpu.make_async_copy(
            piece, wbuf.at[rows_of(sp, fs), lanes(place)], wlocal_sem.at[place]
        )
        for place, piece in enumerate(pieces(sp))
    ]
    own_o = [
        pltpu.make_async_copy(
            ref,
            owb.at[pl.ds(place * out_rows, out_rows), cols_of(sp, fs)],
            local_sem.at[1 + place],
        )
        for place, ref in enumerate((lin_ref, win_ref))
    ]
    small = [
        pltpu.make_async_copy(extra_ref.at[0], ebuf.at[sp], local_sem.at[3]),
        pltpu.make_async_copy(dup_ref.at[:, :, cols], dup, local_sem.at[4]),
        pltpu.make_async_copy(eup_ref.at[:, :, cols], eup, local_sem.at[5]),
        pltpu.make_async_copy(init_ref.at[:, pl.ds(head, 2)], init, local_sem.at[6]),
    ]
    for copy in [own_x] + own_w + own_o + small:
        copy.start()
    low_lanes = lax.broadcasted_iota(jnp.int32, (rows, PAIR), 1) < HD
    near_key, near_value = ak_ref[...].astype(F32), av_ref[...].astype(F32)
    packs = (
        jnp.where(low_lanes, near_key, pltpu.roll(near_value, HD, 1)).astype(BF16),
        jnp.where(low_lanes, pltpu.roll(near_key, HD, 1), near_value).astype(BF16),
    )
    for place, pack in enumerate(packs):
        kvbuf[place] = pack
    wbuf[rows_of(sp, fs), lanes(4)] = jnp.where(sp >= 2, packs[1], packs[0])

    barrier = pltpu.get_barrier_semaphore()
    peers = [{"sp": flipped(sp, k)} for k in range(1, depth)] + [sibling, *plane]
    for peer in peers:
        pl.semaphore_signal(barrier, inc=1, device_id=peer, device_id_type=MESH_IDS)
    pl.semaphore_wait(barrier, len(peers))

    up_exists, dn_exists = sp < depth - 1, sp > 0

    def at_distance(k, body):
        if k == 0:
            body(sp)
            return

        def one(j, carry):
            body(sp + (2 * j - 1) * k)
            return carry

        lax.fori_loop(jnp.where(sp >= k, 0, 1), jnp.where(sp < depth - k, 2, 1), one, 0)

    def x_move(z, part, send, recv, device, src=None):
        span = pl.ds(part * (tokens // PARTS), tokens // PARTS)
        there = xbuf.at[z, tp, span]
        return remote(there if src is None else src.at[0, span], there, send, recv, device)

    def x_up(z, k, part, src=None):
        return x_move(z, part, up_send.at[k, part], up_recv.at[k, part], up_to, src)

    def x_dn(z, k, part, src=None):
        return x_move(z, part, dn_send.at[k, part], dn_recv.at[k, part], dn_to, src)

    def sib_move(z):
        there = xbuf.at[z, tp]
        return remote(there, there, sib_send.at[z], sib_recv.at[z], sibling)

    def wz_block(k):
        there = wbuf.at[rows_of(sp, fs)]
        return remote(there, there, wz_send.at[k - 1], wz_recv.at[k - 1], {"sp": flipped(sp, k)})

    def e_block(k):
        return remote(
            extra_ref.at[0],
            ebuf.at[sp],
            e_send.at[k - 1],
            e_recv.at[k - 1],
            {"sp": flipped(sp, k)},
        )

    def p_block(k, side):
        there = wbuf.at[rows_of(flipped(sp, k), fs)]
        return remote(there, there, p_send.at[k, side], p_recv.at[k, side], plane[side])

    def f_block(k):
        side = k % 2
        there = wbuf.at[rows_of(flipped(sp, k), flipped(fs, 2 if side == 0 else 1))]
        return remote(there, there, f_send.at[k], f_recv.at[k], plane[side])

    def o_move(z, send, recv, device):
        there = owb.at[:, cols_of(z, fs)]
        return remote(there, there, send, recv, device)

    def o_up(z, k):
        return o_move(z, ou_send.at[k], ou_recv.at[k], up_to)

    def o_dn(z, k):
        return o_move(z, od_send.at[k], od_recv.at[k], dn_to)

    def op_block(z, side):
        return o_move(z, op_send.at[z, side], op_recv.at[z, side], plane[side])

    def of_block(z):
        odd = lax.rem(z, 2)
        near, far = flipped(fs, 1), flipped(fs, 2)
        there = owb.at[:, cols_of(z, far + odd * (near - far))]
        device = {"fs": near + odd * (far - near)}
        return remote(there, there, of_send.at[z], of_recv.at[z], device)

    def x_step(k):
        for part in range(PARTS):

            @pl.when(sp >= k)
            def _():
                x_up(sp, k - 1, part).wait_recv()
                if k < depth - 1:

                    @pl.when(up_exists)
                    def _():
                        x_up(sp - k, k, part).start()

            @pl.when(sp < depth - k)
            def _():
                x_dn(sp, k - 1, part).wait_recv()
                if k < depth - 1:

                    @pl.when(dn_exists)
                    def _():
                        x_dn(sp + k, k, part).start()

        at_distance(k, lambda z: sib_move(z).start())
        o_own(k)

    def o_own(k):
        if k == 0:
            ups, dns = sp == 0, sp == depth - 1
        else:
            ups, dns = (sp > 0) & up_exists, (sp < depth - 1) & dn_exists
        if k < 2:

            @pl.when(ups)
            def _():
                o_up(sp, 0).start()

            @pl.when(dns)
            def _():
                o_dn(sp, 0).start()

    def w_step(k):
        if k:
            wz_block(k).wait_recv()
        for side in range(2):
            p_block(k, side).start()

    def f_step(k):
        for side in range(2):
            p_block(k, side).wait_recv()
        f_block(k).start()

    def op_start(z):
        for side in range(2):
            op_block(z, side).start()

    inner = (sp > 0) & up_exists
    odd = lax.rem(sp, 2)
    next_z = 1 + odd
    last_z = (depth - 1) * (1 - odd)
    far_z = jnp.where(sp < 2, sp + 2, sp - 2)

    def o_step(z):
        @pl.when(z < sp)
        def _():
            o_up(sp, sp - z - 1).wait_recv()

            @pl.when(up_exists)
            def _():
                o_up(z, sp - z).start()

        @pl.when(z > sp)
        def _():
            o_dn(sp, z - sp - 1).wait_recv()

            @pl.when(dn_exists)
            def _():
                o_dn(z, z - sp).start()

        op_start(z)

    def of_step(z):
        for side in range(2):
            op_block(z, side).wait_recv()
        of_block(z).start()

    def phase(step, stage):
        if stage == 0:

            @pl.when(inner)
            def _():
                step(last_z)

        elif stage == 3:

            @pl.when(jnp.logical_not(inner))
            def _():
                step(last_z)

        else:
            step(next_z if stage == 1 else far_z)

    def inner_only(step, z):
        @pl.when(inner)
        def _():
            step(z)

    def ends_only(step, z):
        @pl.when(jnp.logical_not(inner))
        def _():
            step(z)

    for k in ORDER:
        target = flipped(sp, k)
        sources = pieces(target) + [kvbuf.at[lax.div(target, 2)]]
        for place, piece in enumerate(sources):
            remote(
                piece,
                wbuf.at[rows_of(sp, fs), lanes(place)],
                wz_send.at[k - 1],
                wz_recv.at[k - 1],
                {"sp": target},
            ).start()
        e_block(k).start()
    for copy in own_w:
        copy.wait()
    w_step(0)
    for part in range(PARTS):

        @pl.when(up_exists)
        def _():
            x_up(sp, 0, part, x_ref).start()

        @pl.when(dn_exists)
        def _():
            x_dn(sp, 0, part, x_ref).start()

    own_x.wait()
    sib_move(sp).start()
    for copy in own_o:
        copy.wait()
    o_own(0)
    f_step(0)
    ends_only(op_start, sp)
    for k in ORDER:
        w_step(k)
    f_step(1)
    f_step(3)
    x_step(1)
    f_step(2)
    inner_only(op_start, sp)
    ends_only(of_step, sp)
    x_step(2)
    phase(o_step, 0)
    for k in range(depth):
        f_block(k).wait_recv()
    for k in range(1, depth):
        e_block(k).wait_recv()
    for copy in small:
        copy.wait()

    gain = gain_ref[...]
    half = gain.shape[1] // 2
    doff = doff_ref[:, cols]
    eoff = eoff_ref[:, cols]

    def block(z):
        sib_move(z).wait_recv()
        parts = [xbuf[z, side].astype(F32) for side in range(2)]
        total = sum(jnp.sum(part * part, axis=1, keepdims=True) for part in parts)
        scale = lax.rsqrt(total / (2 * half) + NORM_EPS)
        hidden = jnp.concatenate(
            [
                (part * scale * gain[:, side * half : (side + 1) * half]).astype(BF16)
                for side, part in enumerate(parts)
            ],
            axis=1,
        )
        where = pl.ds(pl.multiple_of(z * tokens, tokens), tokens)
        proj_ref[where, :] = mm(hidden, wbuf[...]).astype(BF16)
        decay_low = mm(hidden, ddown_ref[...], NT).astype(BF16)
        decay_act = jnp.tanh(decay_low.astype(F32)).astype(BF16)
        learn_low = mm(hidden, edown_ref[...], NT).astype(BF16)
        spikes = jnp.concatenate(
            [
                jnp.broadcast_to(ebuf[z, pl.ds(2 * sp + place, 1), :], (HD, tokens))
                for place in range(2)
            ],
            axis=0,
        ).T
        for direction in range(2):
            pre = doff[direction : direction + 1] + mm(decay_act, dup[direction])
            softplus = jnp.maximum(-pre, 0.0) + jnp.log1p(jnp.exp(-jnp.abs(pre)))
            log_ref[direction, where, :] = spikes - jnp.exp(-softplus - 0.5)
            learn = eoff[direction : direction + 1] + mm(learn_low, eup[direction])
            learn_ref[direction, where, :] = jax.nn.sigmoid(learn)

    for k in range(depth - 1):
        at_distance(k, block)
        if k == 0:
            ends_only(o_step, next_z)
    inner_only(of_step, sp)
    inner_only(o_step, next_z)

    def m_block(part, k):
        z = flipped(sp, k)
        return remote(
            mix_ref.at[part, pl.ds(pl.multiple_of(z * tokens, tokens), tokens)],
            mbuf.at[part, sp],
            m_send.at[part, k - 1],
            m_recv.at[part, k - 1],
            {"sp": z},
        )

    def m_send_part(part):
        for k in range(1, depth):
            m_block(part, k).start()
        mbuf[part, sp] = mix_ref[part, pl.ds(pl.multiple_of(sp * tokens, tokens), tokens), :]

    plan = [
        ((x_step, depth - 1), (inner_only, o_step, far_z), (inner_only, of_step, last_z)),
        ((at_distance, depth - 1, block), (ends_only, of_step, next_z)),
        ((ends_only, o_step, far_z),),
        (),
        (),
        ((inner_only, of_step, next_z),),
        ((ends_only, o_step, last_z),),
        ((m_send_part, 0),),
        ((inner_only, of_step, far_z),),
        ((ends_only, of_step, far_z),),
        (),
    ]
    queue = iter(plan)

    def hook():
        for step, *arguments in next(queue, ()):
            step(*arguments)

    states = jnp.concatenate([init[d, h] for d in range(2) for h in range(2)], axis=1)
    mix_body(
        hook,
        proj_ref,
        log_ref,
        learn_ref,
        table_ref,
        head_gain_ref[:, cols],
        [sink_ref[0, head], sink_ref[0, head + 1]],
        states,
        mix_ref,
        *scratch,
    )

    m_send_part(1)
    ends_only(of_step, last_z)
    for part in range(2):
        for k in range(1, depth):
            m_block(part, k).wait_recv()
    lbuf[...] = jnp.concatenate(
        [mbuf[part, z] for part in range(2) for z in range(depth)], axis=1
    )
    kept = pl.ds(pl.multiple_of(tp * share, share), share)
    given = pl.ds(pl.multiple_of((1 - tp) * share, share), share)

    def part_move(z):
        return remote(
            pbuf.at[z, given], rbuf.at[z], part_send.at[z], part_recv.at[z], sibling
        )

    def product(z):
        pbuf[z] = mm(lbuf[...], owb[:, cols_of(z, 0, width)])
        part_move(z).start()

    def arrived(z):
        of_block(z).wait_recv()
        product(z)

    def total_of(z):
        part_move(z).wait_recv()
        out_ref[0, :, cols_of(z, 0, width)] = (pbuf[z, kept] + rbuf[z]).astype(BF16)

    arrived(sp)
    phase(arrived, 0)
    phase(arrived, 1)
    total_of(sp)
    phase(total_of, 0)
    phase(arrived, 2)
    phase(total_of, 1)
    phase(arrived, 3)
    phase(total_of, 2)
    phase(total_of, 3)

    for k in range(depth - 1):

        @pl.when((sp >= k) & up_exists)
        def _():
            for part in range(PARTS):
                x_up(sp, k, part).wait_send()
            o_up(sp, k).wait_send()

        @pl.when((sp < depth - k) & dn_exists)
        def _():
            for part in range(PARTS):
                x_dn(sp, k, part).wait_send()
            o_dn(sp, k).wait_send()

    for k in range(1, depth):
        wz_block(k).wait_send()
        e_block(k).wait_send()
    for k in range(depth):
        for side in range(2):
            p_block(k, side).wait_send()
            op_block(k, side).wait_send()
        f_block(k).wait_send()
        of_block(k).wait_send()
        part_move(k).wait_send()
        sib_move(k).wait_send()
    for part in range(2):
        for k in range(1, depth):
            m_block(part, k).wait_send()


def by_heads(
    inputs,
    input_norm_gain,
    receptance_weight,
    linear_key_weight,
    linear_value_weight,
    window_query_weight,
    window_key_weight,
    window_value_weight,
    decay_down_weight,
    decay_up_weight,
    decay_offset,
    decay_log_extra,
    erasure_down_weight,
    erasure_up_weight,
    erasure_offset,
    initial_state,
    head_norm_gain,
    query_sink_logit,
    linear_output_weight,
    window_output_weight,
):
    depth, width, sides = [lax.axis_size(axis) for axis in ("sp", "fs", "tp")]
    _, tokens, half = inputs.shape
    total = tokens * depth
    rows = receptance_weight.shape[0]
    out_rows, out_cols = linear_output_weight.shape
    features = out_cols * depth * width
    share = tokens // sides
    low = decay_down_weight.shape[1]
    dma = pltpu.SemaphoreType.DMA
    any_spec = pl.BlockSpec(memory_space=pl.ANY)
    vmem_spec = pl.BlockSpec(memory_space=pltpu.VMEM)
    return pl.pallas_call(
        layer_kernel,
        in_specs=[any_spec] * 11 + [pl.BlockSpec(memory_space=pltpu.SMEM)] + [vmem_spec] * 9,
        out_specs=vmem_spec,
        out_shape=jax.ShapeDtypeStruct((1, share, features), BF16),
        scratch_shapes=[
            pltpu.VMEM((depth, 2, tokens, half), BF16),
            pltpu.VMEM((2 * half, 5 * PAIR), BF16),
            pltpu.VMEM((2, rows, PAIR), BF16),
            pltpu.VMEM((depth, decay_log_extra.shape[1], tokens), F32),
            pltpu.VMEM((2, low, PAIR), BF16),
            pltpu.VMEM((2, low, PAIR), BF16),
            pltpu.VMEM((total, 5 * PAIR), BF16),
            pltpu.VMEM((2, total, PAIR), F32),
            pltpu.VMEM((2, total, PAIR), F32),
            pltpu.VMEM((2 * out_rows, features), BF16),
            pltpu.VMEM((2, depth, tokens, PAIR), BF16),
            pltpu.VMEM((2, total, PAIR), BF16),
            pltpu.VMEM((tokens, 2 * out_rows), BF16),
            pltpu.VMEM((depth, tokens, width * out_cols), F32),
            pltpu.VMEM((depth, share, width * out_cols), F32),
            pltpu.VMEM((2, 2, HD, HD), F32),
            dma((7,)),
            dma((4,)),
            dma((depth, PARTS)),
            dma((depth, PARTS)),
            dma((depth, PARTS)),
            dma((depth, PARTS)),
            dma((depth,)),
            dma((depth,)),
            dma((depth - 1,)),
            dma((depth - 1,)),
            dma((depth - 1,)),
            dma((depth - 1,)),
            dma((width, 2)),
            dma((width, 2)),
            dma((width,)),
            dma((width,)),
            dma((depth - 1,)),
            dma((depth - 1,)),
            dma((depth - 1,)),
            dma((depth - 1,)),
            dma((depth, 2)),
            dma((depth, 2)),
            dma((depth,)),
            dma((depth,)),
            dma((depth,)),
            dma((depth,)),
            dma((2, depth - 1)),
            dma((2, depth - 1)),
        ]
        + mix_scratch(total),
        compiler_params=pltpu.CompilerParams(
            collective_id=0, has_side_effects=True, vmem_limit_bytes=VMEM_GRANT
        ),
        name="layer",
    )(
        inputs,
        receptance_weight,
        linear_key_weight,
        linear_value_weight,
        window_query_weight,
        decay_log_extra,
        decay_up_weight,
        erasure_up_weight,
        linear_output_weight,
        window_output_weight,
        initial_state,
        query_sink_logit[None, :],
        window_key_weight,
        window_value_weight,
        input_norm_gain[None, :],
        decay_down_weight.T,
        erasure_down_weight.T,
        decay_offset,
        erasure_offset,
        jnp.asarray(rope_tables(total)),
        head_norm_gain[None, :],
    )


def layer(*arrays):
    inputs, recept, keys = arrays[0], arrays[2], arrays[6]
    depth, width, sides = [lax.axis_size(axis) for axis in ("sp", "fs", "tp")]
    fits = (
        recept.shape[1] == arrays[5].shape[1] == depth * PAIR
        and 2 * keys.shape[1] == depth * HD
        and (depth, width, sides) == (4, 4, 2)
        and inputs.shape[1] % WINDOW == 0
        and SPAN == GRID_W
    )
    return (by_heads if fits else local)(*arrays)


def solution(mesh):
    return jax.shard_map(
        layer,
        mesh=mesh,
        in_specs=(
            P("fs", "sp", "tp"),
            P(),
            P(("sp", "fs"), "tp"),
            P(("sp", "fs"), "tp"),
            P(("sp", "fs"), "tp"),
            P(("sp", "fs"), "tp"),
            P(("sp", "fs"), "tp"),
            P(("sp", "fs"), "tp"),
            P(),
            P(),
            P(),
            P("fs", "tp", "sp"),
            P(),
            P(),
            P(),
            P(),
            P(),
            P(),
            P("tp", ("sp", "fs")),
            P("tp", ("sp", "fs")),
        ),
        out_specs=P("fs", ("sp", "tp"), None),
        check_vma=False,
    )
```
